32 devices in a mesh: sp: 16 (over z, y, core), tp: 2 (over x).
Axes of the slice: x: 2, y: 2, z: 4, core: 2. Of those that a mesh axis runs over, the one named last changes fastest.
Arguments:
- inputs: bfloat16 [4096, 4096], P('sp', 'tp'), may hold values from -20 to 20
- norm_gain: float32 [3, 4096], replicated, may hold values from 0.1 to 1.9
- in_weight: bfloat16 [3, 4096, 1024], P(None, 'tp', 'sp'), may hold values from -0.09375 to 0.09375
- pool_scale: float32 [3, 1024], replicated, may hold values from 0.1 to 1.9
- out_weight: bfloat16 [3, 1024, 4096], P(None, 'sp', 'tp'), may hold values from -0.1875 to 0.1875
Outputs:
- final_state: bfloat16 [4096, 4096], P('sp', 'tp')
The draws below stay inside these ranges and needn't reach their ends.
All inputs are finite; a program needn't handle non-finite values.
Results may differ from the reference program's by a relative error of at most 0.017.
Values may be sent and summed in bfloat16 or wider, within the bound.
A program may use at most 64 MiB of HBM per device.

```python
import jax
import jax.numpy as jnp
from jax import lax

D = 4096
P_SIZE = 1024
LAYERS = 3
TOKENS = 4096


def draw_inputs(key, part):
    column = lax.broadcasted_iota(jnp.float32, (1, D), 1) / D
    rough = jax.random.uniform(jax.random.fold_in(key, 2), (1, D), jnp.float32, 0.6, 1.4)
    column_scale = 0.35 * jnp.exp(jnp.log(10.0) * column) * rough
    base = jnp.clip(jax.random.normal(jax.random.fold_in(key, 1), (TOKENS, D), jnp.float32), -4.0, 4.0)
    return jnp.clip(base * column_scale, -20.0, 20.0).astype(jnp.bfloat16)


def levels(own_key, shape, split, least, largest):
    level = 1.0
    for dim, shards_of in split:
        heights = jax.random.uniform(jax.random.fold_in(jax.random.fold_in(own_key, 6), dim), (shards_of,), jnp.float32, least / len(split), largest / len(split))
        level = level * jnp.repeat(jnp.exp(heights), shape[dim] // shards_of).reshape((-1,) + (1,) * (len(shape) - 1 - dim))
    return level


def centred(own_key, extent, deviation, reach, pieces=(), dtype=jnp.bfloat16):
    values = jax.random.normal(own_key, extent, jnp.float32) * deviation
    if len(pieces) > 0:
        values = levels(own_key, extent, pieces, -0.22, 0.18) * values
    return jnp.clip(values, min=-reach, max=reach).astype(dtype)


def setup_inputs(seed: int = 0) -> dict:
    keys = jax.random.split(jax.random.key(seed), 6)
    inputs = draw_inputs(jax.random.fold_in(keys[5], 71), 0)
    norm_gain = jnp.clip(1.0 + 0.18 * jax.random.normal(keys[1], (LAYERS, D), jnp.float32), 0.1, 1.9)
    in_weight = centred(keys[2], (LAYERS, D, P_SIZE), D ** -0.5, 0.09375, ((1, 2), (2, 16)))
    pool_scale = jnp.clip(1.0 + 0.18 * jax.random.normal(keys[3], (LAYERS, P_SIZE), jnp.float32), 0.1, 1.9)
    out_weight = centred(keys[4], (LAYERS, P_SIZE, D), P_SIZE ** -0.5, 0.1875, ((1, 16), (2, 2)))
    return {"inputs": inputs, "norm_gain": norm_gain, "in_weight": in_weight, "pool_scale": pool_scale, "out_weight": out_weight}


epsilon = 1e-06
halo_rows = 16
group_count = 4

def window_means(extended, row_count, first_channel, first_pos, pool_total):
    width = extended.shape[1]
    channel = first_channel + lax.broadcasted_iota(jnp.int32, (1, width), 1)
    group_index = channel // (pool_total // group_count)
    window_len = jnp.left_shift(jnp.int32(2), group_index)
    running = jnp.zeros((row_count, width), jnp.float32)
    for offset in range(halo_rows):
        shifted = extended[halo_rows - offset:halo_rows - offset + row_count]
        running = running + jnp.where(offset < window_len, shifted, 0.0)
    position = first_pos + lax.broadcasted_iota(jnp.int32, (row_count, 1), 0)
    divisor = jnp.minimum(position + 1, window_len).astype(jnp.float32)
    return running / divisor - extended[halo_rows:]

def reference(inputs, norm_gain, in_weight, pool_scale, out_weight):
    current = inputs
    for layer_index in range(LAYERS):
        widened = current.astype(jnp.float32)
        inv_rms = lax.rsqrt(lax.optimization_barrier(jnp.mean(widened * widened, axis=1, keepdims=True)) + epsilon)
        normed = (widened * inv_rms * norm_gain[layer_index]).astype(jnp.bfloat16)
        pool_in = jnp.dot(normed, in_weight[layer_index], preferred_element_type=jnp.float32).astype(jnp.bfloat16)
        extended = jnp.concatenate([jnp.zeros((halo_rows, P_SIZE), jnp.float32), pool_in.astype(jnp.float32)], 0)
        means = window_means(extended, TOKENS, 0, 0, P_SIZE)
        mixed = (means * pool_scale[layer_index]).astype(jnp.bfloat16)
        branch = jnp.dot(mixed, out_weight[layer_index], preferred_element_type=jnp.float32)
        current = (widened + branch).astype(jnp.bfloat16)
    return current
```

```python
import functools

import jax
import jax.numpy as jnp
from jax import lax
from jax.experimental import pallas as pl
from jax.experimental.pallas import tpu as pltpu
from jax.sharding import PartitionSpec as P

EPS = 1e-06
REACH = 16
GROUPS = 4
MESH_ID = pl.DeviceIdType.MESH


def shift_sp(value):
    count = lax.axis_size("sp")
    return lax.ppermute(value, "sp", [(i, i + 1) for i in range(count - 1)])


def window_means(extended, row_count, first_channel, first_pos, pool_total):
    width = extended.shape[1]
    channel = first_channel + lax.broadcasted_iota(jnp.int32, (1, width), 1)
    window_len = jnp.left_shift(jnp.int32(2), channel // (pool_total // GROUPS))
    running = jnp.zeros((row_count, width), jnp.float32)
    for offset in range(REACH):
        shifted = extended[REACH - offset : REACH - offset + row_count]
        running = running + jnp.where(offset < window_len, shifted, 0.0)
    position = first_pos + lax.broadcasted_iota(jnp.int32, (row_count, 1), 0)
    divisor = jnp.minimum(position + 1, window_len).astype(jnp.float32)
    return running / divisor - extended[REACH:]


def plain_body(inputs, norm_gain, in_weight, pool_scale, out_weight):
    rows, feats = inputs.shape
    layers, features = norm_gain.shape
    pools = pool_scale.shape[1]
    part = pools // lax.axis_size("tp")
    t = lax.axis_index("tp")
    s = lax.axis_index("sp")
    current = inputs
    for layer in range(layers):
        in_all = lax.all_gather(in_weight[layer], "sp", axis=1, tiled=True)
        out_all = lax.all_gather(out_weight[layer], "sp", axis=0, tiled=True)
        wide = current.astype(jnp.float32)
        squares = lax.psum(jnp.sum(wide * wide, axis=1), "tp")
        inv_rms = lax.rsqrt(squares / features + EPS)[:, None]
        gain = lax.dynamic_slice_in_dim(norm_gain[layer], t * feats, feats)
        normed = (wide * inv_rms * gain).astype(jnp.bfloat16)
        partial = jnp.dot(normed, in_all, preferred_element_type=jnp.float32)
        pool_in = lax.psum_scatter(
            partial.astype(jnp.bfloat16), "tp", scatter_dimension=1, tiled=True
        )
        edge = shift_sp(pool_in[rows - REACH :])
        extended = jnp.concatenate([edge, pool_in], 0).astype(jnp.float32)
        means = window_means(extended, rows, t * part, s * rows, pools)
        scale = lax.dynamic_slice_in_dim(pool_scale[layer], t * part, part)
        mixed = (means * scale).astype(jnp.bfloat16)
        pooled = lax.all_gather(mixed, "tp", axis=1, tiled=True)
        branch = jnp.dot(pooled, out_all, preferred_element_type=jnp.float32)
        current = (current.astype(jnp.float32) + branch).astype(jnp.bfloat16)
    return current


PIECES = 4
STATE_CHUNKS = 4


def phase_table(layers, feats):
    table = []
    for layer in range(layers):
        table.append((2 * layer, 0, feats))
        count = PIECES if layer == layers - 1 else 1
        width = feats // count
        table += [(2 * layer + 1, k * width, width) for k in range(count)]
    return table


def kernel(
    n_z, layers, halo,
    x_ref, gain_ref, wi_ref, scale_ref, wo_ref, o_ref,
    held, state, xg, edge, p_send, p_recv, mix, stage, part_sq, inv_col, sq_send, sq_recv,
    w_send, w_recv, local_sem, e_send, e_recv, s_send, s_recv, a_send, a_recv, f_send, f_recv,
):
    rows, feats = x_ref.shape
    total = rows + halo
    blocks, depth = held.shape[1], held.shape[2]
    pools = scale_ref.shape[1]
    chunk = pools // n_z
    last = layers - 1
    table = phase_table(layers, feats)
    phases = len(table)
    lanes = 128
    sq_tiles = part_sq.shape[1] // lanes
    s = lax.axis_index("sp")
    t = lax.axis_index("tp")
    core = s % 2
    y = (s // 2) % 2
    z = s // 4
    side = z // 2

    def block_of(zz, yy, cc):
        return zz * 4 + yy * 2 + cc

    z_in, z_end = 1 + side, 3 * side
    z_over, z_far = 2 - side, 3 - 3 * side
    is_end = z == z_end
    s_end, s_in = block_of(z_end, y, core), block_of(z_in, y, core)

    y_mate = (block_of(z, 1 - y, core), t)
    c_mate = (block_of(z, y, 1 - core), t)
    x_mate = (s, 1 - t)
    opposite = (block_of(z_over, y, core), t)
    inner = (s_in, t)
    outer = (s_end, t)
    after = (s + 1) % blocks
    after_z = after // 4
    after_holder = (block_of(1 + after_z // 2, (after // 2) % 2, after % 2), t)
    after_slot = jnp.where((after_z == 0) | (after_z == n_z - 1), 1, 0)
    before = [((s_in + blocks - 1) % blocks, t), ((s_end + blocks - 1) % blocks, t)]

    barrier = pltpu.get_barrier_semaphore()

    def greet(peers):
        for peer in peers:
            pl.semaphore_signal(barrier, inc=1, device_id=peer, device_id_type=MESH_ID)

    sent = []

    def send(src, dst, send_sem, recv_sem, to):
        copy = pltpu.make_async_remote_copy(
            src_ref=src, dst_ref=dst, send_sem=send_sem, recv_sem=recv_sem,
            device_id=to, device_id_type=MESH_ID,
        )
        copy.start()
        sent.append(copy)

    def arrived(ref, sem):
        pltpu.make_async_remote_copy(
            src_ref=ref, dst_ref=ref, send_sem=sem, recv_sem=sem,
            device_id=c_mate, device_id_type=MESH_ID,
        ).wait_recv()

    whole, first, second = pl.ds(0, depth), pl.ds(0, depth // 2), pl.ds(depth // 2, depth // 2)
    count = [0] * phases

    def own(ph):
        buf, start, width = table[ph]
        return (wi_ref if buf % 2 == 0 else wo_ref).at[buf // 2, :, pl.ds(start, width)]

    def slot(ph, block, piece=whole):
        buf, start, width = table[ph]
        return held.at[buf, block, piece, pl.ds(start, width)]

    def recv_sem(ph, block, piece=whole):
        return w_recv.at[ph, block, 1 if piece is second else 0]

    def next_send(ph):
        count[ph] += 1
        return w_send.at[ph, count[ph] - 1]

    def send_own(ph, to):
        send(own(ph), slot(ph, s), next_send(ph), recv_sem(ph, s), to)

    def forward(ph, block, to, piece=whole):
        ref = slot(ph, block, piece)
        send(ref, ref, next_send(ph), recv_sem(ph, block, piece), to)

    def wait_block(ph, block, piece=whole):
        arrived(slot(ph, block, piece), recv_sem(ph, block, piece))

    state_rows = rows // STATE_CHUNKS
    final_cols = feats // PIECES

    def send_edge():
        send(
            x_ref.at[pl.ds(rows - halo, halo)], edge.at[after_slot],
            e_send.at[0], e_recv.at[after_slot], after_holder,
        )

    def end_program():
        greet([inner, y_mate])
        pl.semaphore_wait(barrier, 3)
        mate = block_of(z, 1 - y, core)

        def ship(k):
            at = pl.ds(k * state_rows, state_rows)
            send(
                x_ref.at[at], state.at[1, pl.ds(halo + k * state_rows, state_rows)],
                s_send.at[k], s_recv.at[k], inner,
            )

        send_own(0, y_mate)
        send_own(0, inner)
        send_edge()
        send_own(1, y_mate)
        wait_block(0, mate)
        forward(0, mate, inner)
        for k in range(STATE_CHUNKS):
            ship(k)
        for ph in range(1, phases):
            send_own(ph, inner)
            if ph + 1 < phases:
                send_own(ph + 1, y_mate)
            wait_block(ph, mate)
            forward(ph, mate, inner)
        for k in range(PIECES):
            at = pl.ds(k * final_cols, final_cols)
            arrived(o_ref.at[:, at], f_recv.at[k])
        for copy in sent:
            copy.wait_send()
        sent.clear()

    def inner_program():
        greet([opposite, y_mate, c_mate, x_mate, outer] + before)
        pl.semaphore_wait(barrier, 6)
        locals_ = {}
        chunk_z = [z_in, z_end, z_over, z_far]

        def issue(ph):
            if ph >= phases:
                return
            send_own(ph, opposite)
            send_own(ph, y_mate)
            send_own(ph, c_mate)
            copy = pltpu.make_async_copy(own(ph), slot(ph, s), local_sem.at[ph])
            copy.start()
            locals_[ph] = copy

        def take_end(ph):
            block = block_of(z_end, y, core)
            wait_block(ph, block)
            forward(ph, block, opposite)
            forward(ph, block, c_mate)

        def take_over(ph):
            block = block_of(z_over, y, core)
            wait_block(ph, block)
            forward(ph, block, y_mate, first)
            forward(ph, block, c_mate)

        def take_mate(ph):
            block = block_of(z_in, 1 - y, core)
            wait_block(ph, block)
            forward(ph, block, opposite, second)
            forward(ph, block, c_mate)

        def take_far(ph):
            block = block_of(z_far, y, core)
            wait_block(ph, block)
            forward(ph, block, y_mate)
            forward(ph, block, c_mate)

        def take_mate_end(ph):
            block = block_of(z_end, 1 - y, core)
            wait_block(ph, block)
            forward(ph, block, c_mate)

        def take_mate_over(ph):
            block = block_of(z_over, 1 - y, core)
            wait_block(ph, block, first)
            wait_block(ph, block, second)
            forward(ph, block, c_mate)

        def take_mate_far(ph):
            block = block_of(z_far, 1 - y, core)
            wait_block(ph, block)
            forward(ph, block, c_mate)

        def plane(ph, k):
            if k == 0:
                locals_[ph].wait()
            for yy in range(2):
                wait_block(ph, block_of(chunk_z[k], yy, 1 - core))

        def first_row(layer):
            return REACH * layer

        def from_row(start):
            return pl.ds(start, total - start)

        def gain_of(layer, start, width):
            at = pl.multiple_of(t * feats + start, lanes)
            return gain_ref[pl.ds(layer, 1), pl.ds(at, width)]

        def pack_squares(g, layer):
            for k in range(sq_tiles):
                block = part_sq[g, pl.ds(k * lanes, lanes)].T
                value = jnp.sum(block, axis=0, keepdims=True)
                sq_send[layer, g, k] = jnp.broadcast_to(value, (8, lanes))
            exchange(sq_send.at[layer, g], sq_recv.at[layer, g], layer, g, n_z)

        def exchange(src, dst, layer, g, k):
            send(src, dst, a_send.at[layer, g, k], a_recv.at[layer, g, k], x_mate)

        def take_edge(g):
            arrived(edge.at[g], e_recv.at[g])
            keep = ((s_in if g == 0 else s_end) > 0).astype(jnp.float32)

            @pl.loop(0, halo // REACH)
            def _(i):
                at = pl.ds(i * REACH, REACH)
                state[g, at] = (edge[g, at].astype(jnp.float32) * keep).astype(jnp.bfloat16)

        def own_state():
            @pl.loop(0, rows // REACH)
            def _(i):
                state[0, pl.ds(halo + i * REACH, REACH)] = x_ref[pl.ds(i * REACH, REACH)]

        def take_state(k):
            arrived(state.at[1, pl.ds(halo + k * state_rows, state_rows)], s_recv.at[k])

        def squares(g, start, stop):
            @pl.loop(start // REACH, stop // REACH)
            def _(i):
                at = pl.ds(i * REACH, REACH)
                sums = jnp.zeros((REACH, lanes), jnp.float32)
                for j in range(feats // lanes):
                    cols = pl.ds(j * lanes, lanes)
                    wide = state[g, at, cols].astype(jnp.float32)
                    sums = sums + wide * wide
                    xg[g, at, cols] = (wide * gain_of(0, j * lanes, lanes)).astype(jnp.bfloat16)
                part_sq[g, at] = sums

        def project(layer, g, k):
            at = from_row(first_row(layer))
            weight = held[2 * layer, pl.ds(chunk_z[k] * 4, 4)].reshape(chunk, feats)
            value = lax.dot_general(
                xg[g, at], weight, (((1,), (1,)), ((), ())),
                preferred_element_type=jnp.float32,
            )
            p_send[layer, g, k, at] = value.astype(jnp.bfloat16)
            exchange(p_send.at[layer, g, k, at], p_recv.at[layer, g, k, at], layer, g, k)

        def inverse(layer, g):
            arrived(sq_recv.at[layer, g], a_recv.at[layer, g, n_z])
            for k in range(sq_tiles):
                mean = (sq_send[layer, g, k] + sq_recv[layer, g, k]) / (2 * feats)
                inv = lax.rsqrt(mean + EPS)
                inv_col[g, pl.ds(k * lanes, lanes)] = jnp.broadcast_to(inv[0:1], (lanes, lanes)).T

        def pool(layer, g, k):
            start = first_row(layer)
            at = from_row(start)
            arrived(p_recv.at[layer, g, k, at], a_recv.at[layer, g, k])
            group = chunk_z[k]
            row = lax.broadcasted_iota(jnp.int32, (total - start, lanes), 0)
            position = (s_in if g == 0 else s_end) * rows - halo + start + row
            span = jnp.left_shift(jnp.int32(2), group)
            divisor = jnp.maximum(jnp.minimum(position + 1, span), 1).astype(jnp.float32)
            share = 1.0 / divisor
            inv = inv_col[g, at]
            for j in range(chunk // lanes):
                cols = pl.ds(j * lanes, lanes)
                joined = p_send[layer, g, k, at, cols].astype(jnp.float32)
                joined = joined + p_recv[layer, g, k, at, cols].astype(jnp.float32)
                base = (joined * inv).astype(jnp.bfloat16).astype(jnp.float32)
                running = base
                width = 1
                picked = None
                for step in range(GROUPS):
                    running = running + pltpu.roll(running, width, 0)
                    width *= 2
                    picked = running if picked is None else jnp.where(group >= step, running, picked)
                lane = pl.multiple_of(group * chunk + j * lanes, lanes)
                scale = scale_ref[pl.ds(layer, 1), pl.ds(lane, lanes)]
                mix[g, group, at, cols] = ((picked * share - base) * scale).astype(jnp.bfloat16)

        def expand(layer, g, start, stop):
            width = 256
            at = from_row(first_row(layer + 1))
            buf = 2 * layer + 1

            @pl.loop(start // width, stop // width)
            def _(n):
                col = pl.multiple_of(n * width, width)
                cols = pl.ds(col, width)
                mixed = jnp.concatenate([mix[g, c, at] for c in range(n_z)], axis=1)
                weight = held[buf, :, :, cols].reshape(pools, width)
                branch = jnp.dot(mixed, weight, preferred_element_type=jnp.float32)
                new = (state[g, at, cols].astype(jnp.float32) + branch).astype(jnp.bfloat16)
                if layer == last:
                    if g == 0:
                        o_ref[:, cols] = new
                    else:
                        stage[:, cols] = new
                else:
                    state[g, at, cols] = new
                    wide = new.astype(jnp.float32)
                    xg[g, at, cols] = (wide * gain_of(layer + 1, col, width)).astype(jnp.bfloat16)
                    square = wide * wide
                    sums = square[:, :lanes]
                    for j in range(1, width // lanes):
                        sums = sums + square[:, j * lanes:(j + 1) * lanes]
                    part_sq[g, at] = part_sq[g, at] + sums

        def clear(g):
            part_sq[g] = jnp.zeros(part_sq.shape[1:], jnp.float32)

        def return_final(k):
            cols = pl.ds(k * final_cols, final_cols)
            send(stage.at[:, cols], o_ref.at[:, cols], f_send.at[k], f_recv.at[k], outer)

        def early(ph):
            take_end(ph)
            take_over(ph)
            take_mate(ph)

        def middle(ph):
            take_far(ph)
            take_mate_end(ph)

        def late(ph):
            take_mate_over(ph)
            take_mate_far(ph)

        def planes(ph):
            for k in range(n_z):
                plane(ph, k)

        a_of = [i for i, row in enumerate(table) if row[0] % 2 == 0]
        b_of = [[i for i, row in enumerate(table) if row[0] == 2 * l + 1] for l in range(layers)]

        send_edge()
        issue(0)
        issue(1)
        clear(0)
        clear(1)
        own_state()
        take_edge(0)
        squares(0, 0, total)
        pack_squares(0, 0)
        early(0)
        plane(0, 0)
        project(0, 0, 0)
        middle(0)
        plane(0, 1)
        project(0, 0, 1)
        issue(2)
        early(1)
        late(0)
        plane(0, 2)
        project(0, 0, 2)
        plane(0, 3)
        project(0, 0, 3)
        inverse(0, 0)
        pool(0, 0, 0)
        take_edge(1)
        squares(1, 0, halo)
        middle(1)
        for k in range(2):
            take_state(k)
            squares(1, halo + k * state_rows, halo + (k + 1) * state_rows)
        pool(0, 0, 1)
        issue(3)
        late(1)
        pool(0, 0, 2)
        for k in range(2, STATE_CHUNKS):
            take_state(k)
            squares(1, halo + k * state_rows, halo + (k + 1) * state_rows)
        pack_squares(1, 0)
        project(0, 1, 0)
        project(0, 1, 1)
        early(2)
        project(0, 1, 2)
        project(0, 1, 3)
        pool(0, 0, 3)
        clear(0)
        planes(1)
        expand(0, 0, 0, feats)
        pack_squares(0, 1)
        middle(2)
        issue(4)
        plane(2, 0)
        project(1, 0, 0)
        plane(2, 1)
        project(1, 0, 1)
        early(3)
        late(2)
        plane(2, 2)
        project(1, 0, 2)
        inverse(0, 1)
        pool(0, 1, 0)
        plane(2, 3)
        project(1, 0, 3)
        for k in range(1, n_z):
            pool(0, 1, k)
        clear(1)
        middle(3)
        expand(0, 1, 0, feats)
        pack_squares(1, 1)
        issue(5)
        for k in range(n_z):
            project(1, 1, k)
        late(3)
        early(4)
        inverse(1, 0)
        for k in range(n_z):
            pool(1, 0, k)
        planes(3)
        clear(0)
        middle(4)
        issue(6)
        expand(1, 0, 0, feats)
        pack_squares(0, 2)
        plane(4, 0)
        project(2, 0, 0)
        plane(4, 1)
        project(2, 0, 1)
        early(5)
        inverse(1, 1)
        for k in range(n_z):
            pool(1, 1, k)
        clear(1)
        expand(1, 1, 0, feats)
        pack_squares(1, 2)
        project(2, 1, 0)
        project(2, 1, 1)
        late(4)
        plane(4, 2)
        project(2, 0, 2)
        project(2, 1, 2)
        plane(4, 3)
        project(2, 1, 3)
        project(2, 0, 3)
        middle(5)
        issue(7)
        early(6)
        inverse(2, 1)
        pool(2, 1, 0)
        late(5)
        pool(2, 1, 1)
        middle(6)
        issue(8)
        pool(2, 1, 2)
        early(7)
        late(6)
        pool(2, 1, 3)
        for piece in range(PIECES):
            ph = b_of[last][piece]
            planes(ph)
            expand(last, 1, piece * final_cols, (piece + 1) * final_cols)
            return_final(piece)
            if piece == 0:
                inverse(2, 0)
                pool(2, 0, 0)
                pool(2, 0, 1)
                middle(7)
                early(8)
                late(7)
            if piece == 1:
                pool(2, 0, 2)
                pool(2, 0, 3)
                middle(8)
                late(8)
        expand(last, 0, 0, feats)
        for copy in sent:
            copy.wait_send()
        sent.clear()

    pl.when(is_end)(end_program)
    for ph in range(phases):
        count[ph] = 0
    pl.when(jnp.logical_not(is_end))(inner_program)


def fused_body(inputs, norm_gain, in_weight, pool_scale, out_weight):
    rows, feats = inputs.shape
    layers = norm_gain.shape[0]
    pools = pool_scale.shape[1]
    blocks = lax.axis_size("sp")
    n_z = blocks // 4
    depth = out_weight.shape[1]
    halo = REACH * layers
    total = rows + halo
    sq_tiles = -(-total // 128)
    chunk = pools // n_z
    phases = len(phase_table(layers, feats))
    bf, f32 = jnp.bfloat16, jnp.float32
    vmem = pl.BlockSpec(memory_space=pltpu.VMEM)
    dma = pltpu.SemaphoreType.DMA
    return pl.pallas_call(
        functools.partial(kernel, n_z, layers, halo),
        out_shape=jax.ShapeDtypeStruct((rows, feats), bf),
        in_specs=[vmem] * 5,
        out_specs=vmem,
        scratch_shapes=[
            pltpu.VMEM((2 * layers, blocks, depth, feats), bf),
            pltpu.VMEM((2, total, feats), bf),
            pltpu.VMEM((2, total, feats), bf),
            pltpu.VMEM((2, halo, feats), bf),
            pltpu.VMEM((layers, 2, n_z, total, chunk), bf),
            pltpu.VMEM((layers, 2, n_z, total, chunk), bf),
            pltpu.VMEM((2, n_z, total, chunk), bf),
            pltpu.VMEM((rows, feats), bf),
            pltpu.VMEM((2, sq_tiles * 128, 128), f32),
            pltpu.VMEM((2, sq_tiles * 128, 128), f32),
            pltpu.VMEM((layers, 2, sq_tiles, 8, 128), f32),
            pltpu.VMEM((layers, 2, sq_tiles, 8, 128), f32),
            dma((phases, 14)),
            dma((phases, blocks, 2)),
            dma((phases,)),
            dma((1,)),
            dma((2,)),
            dma((STATE_CHUNKS,)),
            dma((STATE_CHUNKS,)),
            dma((layers, 2, n_z + 1)),
            dma((layers, 2, n_z + 1)),
            dma((PIECES,)),
            dma((PIECES,)),
        ],
        compiler_params=pltpu.CompilerParams(
            collective_id=0, has_side_effects=True, vmem_limit_bytes=60 * 1024 * 1024
        ),
    )(inputs, norm_gain, jnp.swapaxes(in_weight, 1, 2), pool_scale, out_weight)


def solution(mesh):
    n_sp, n_tp = mesh.shape["sp"], mesh.shape["tp"]
    fused = n_tp == 2 and n_sp == 16
    placed = (P("sp", "tp"), P(), P(None, "tp", "sp"), P(), P(None, "sp", "tp"))
    return jax.shard_map(
        fused_body if fused else plain_body,
        mesh=mesh, in_specs=placed, out_specs=P("sp", "tp"), check_vma=False,
    )
```

```python
import functools

import jax
import jax.numpy as jnp
from jax import lax
from jax.experimental import pallas as pl
from jax.experimental.pallas import tpu as pltpu
from jax.sharding import PartitionSpec as P

EPS = 1e-06
REACH = 16
GROUPS = 4
MESH_ID = pl.DeviceIdType.MESH


def shift_sp(value):
    count = lax.axis_size("sp")
    return lax.ppermute(value, "sp", [(i, i + 1) for i in range(count - 1)])


def window_means(extended, row_count, first_channel, first_pos, pool_total):
    width = extended.shape[1]
    channel = first_channel + lax.broadcasted_iota(jnp.int32, (1, width), 1)
    window_len = jnp.left_shift(jnp.int32(2), channel // (pool_total // GROUPS))
    running = jnp.zeros((row_count, width), jnp.float32)
    for offset in range(REACH):
        shifted = extended[REACH - offset : REACH - offset + row_count]
        running = running + jnp.where(offset < window_len, shifted, 0.0)
    position = first_pos + lax.broadcasted_iota(jnp.int32, (row_count, 1), 0)
    divisor = jnp.minimum(position + 1, window_len).astype(jnp.float32)
    return running / divisor - extended[REACH:]


def plain_body(inputs, norm_gain, in_weight, pool_scale, out_weight):
    rows, feats = inputs.shape
    layers, features = norm_gain.shape
    pools = pool_scale.shape[1]
    part = pools // lax.axis_size("tp")
    t = lax.axis_index("tp")
    s = lax.axis_index("sp")
    current = inputs
    for layer in range(layers):
        in_all = lax.all_gather(in_weight[layer], "sp", axis=1, tiled=True)
        out_all = lax.all_gather(out_weight[layer], "sp", axis=0, tiled=True)
        wide = current.astype(jnp.float32)
        squares = lax.psum(jnp.sum(wide * wide, axis=1), "tp")
        inv_rms = lax.rsqrt(squares / features + EPS)[:, None]
        gain = lax.dynamic_slice_in_dim(norm_gain[layer], t * feats, feats)
        normed = (wide * inv_rms * gain).astype(jnp.bfloat16)
        partial = jnp.dot(normed, in_all, preferred_element_type=jnp.float32)
        pool_in = lax.psum_scatter(
            partial.astype(jnp.bfloat16), "tp", scatter_dimension=1, tiled=True
        )
        edge = shift_sp(pool_in[rows - REACH :])
        extended = jnp.concatenate([edge, pool_in], 0).astype(jnp.float32)
        means = window_means(extended, rows, t * part, s * rows, pools)
        scale = lax.dynamic_slice_in_dim(pool_scale[layer], t * part, part)
        mixed = (means * scale).astype(jnp.bfloat16)
        pooled = lax.all_gather(mixed, "tp", axis=1, tiled=True)
        branch = jnp.dot(pooled, out_all, preferred_element_type=jnp.float32)
        current = (current.astype(jnp.float32) + branch).astype(jnp.bfloat16)
    return current


PIECES = (2, 2, 2, 2, 2, 4)
EDGE_BY_MATE = (True, True, False, False, False, False)
OVER_BY_MATE = (0.5, 0, 0.5, 1, 0, 0.5)
INNER_ORDER = [
    ("init",), ("issue", 0), ("issue", 1), ("issue", 2), ("sq", 0), ("M", 0), ("O", 0), ("E", 0), ("inv", 0, 0),
    ("O", 1), ("M", 1), ("plane", 0, 0), ("P", 0, 0, 0), ("st", 0), ("M", 2), ("O", 2), ("OM", 0), ("E", 1),
    ("F", 0), ("EM", 0), ("issue", 3), ("Q", 0, 0, 0), ("OM", 1), ("plane", 0, 2), ("P", 0, 0, 2), ("st", 1),
    ("EM", 1), ("OM", 2), ("plane", 0, 1), ("P", 0, 0, 1), ("FM", 0), ("F", 1), ("issue", 4), ("Q", 0, 0, 2),
    ("st", 2), ("M", 3), ("O", 3), ("plane", 1, 0), ("Q", 0, 0, 1), ("E", 2), ("FM", 1), ("O", 4), ("plane", 0, 3),
    ("P", 0, 0, 3), ("E", 3), ("OM", 3), ("M", 4), ("plane", 1, 2), ("EM", 2), ("F", 2), ("issue", 5),
    ("Q", 0, 0, 3), ("st", 3), ("sq", 1), ("F", 3), ("issue", 6), ("P", 0, 1, 2), ("P", 0, 1, 1), ("EM", 3),
    ("OM", 4), ("P", 0, 1, 3), ("E", 4), ("P", 0, 1, 0), ("plane", 1, 1), ("inv", 0, 1), ("O", 5), ("FM", 2),
    ("EM", 4), ("Q", 0, 1, 2), ("O", 6), ("M", 5), ("E", 5), ("plane", 2, 0), ("Q", 0, 1, 1), ("FM", 3), ("F", 4),
    ("issue", 7), ("EM", 5), ("plane", 1, 3), ("X", 0, 0, 0, 2), ("M", 6), ("plane", 2, 1), ("X", 0, 0, 2, 3),
    ("Q", 0, 1, 3), ("X", 0, 0, 3, 4), ("E", 6), ("F", 5), ("issue", 8), ("OM", 5), ("P", 1, 0, 0), ("P", 1, 0, 1),
    ("Q", 0, 1, 0), ("plane", 2, 2), ("mx", 0), ("P", 1, 0, 2), ("O", 7), ("OM", 6), ("EM", 6), ("inv", 1, 0),
    ("X", 0, 1, 0, 3), ("E", 7), ("F", 6), ("issue", 9), ("FM", 4), ("X", 0, 1, 3, 4), ("P", 1, 1, 2),
    ("Q", 1, 0, 0), ("P", 1, 1, 1), ("EM", 7), ("P", 1, 1, 0), ("O", 8), ("M", 7), ("Q", 1, 0, 1), ("plane", 3, 1),
    ("plane", 3, 0), ("E", 8), ("F", 7), ("FM", 5), ("issue", 10), ("Q", 1, 0, 2), ("plane", 2, 3), ("P", 1, 1, 3),
    ("inv", 1, 1), ("P", 1, 0, 3), ("M", 8), ("EM", 8), ("O", 9), ("Q", 1, 1, 2), ("E", 9), ("OM", 7), ("F", 8),
    ("issue", 11), ("O", 10), ("plane", 3, 2), ("Q", 1, 1, 1), ("EM", 9), ("FM", 6), ("plane", 4, 1), ("E", 10),
    ("OM", 8), ("EM", 10), ("Q", 1, 1, 0), ("M", 9), ("E", 11), ("F", 9), ("issue", 12), ("plane", 4, 0), ("EM", 11),
    ("O", 11), ("FM", 7), ("Q", 1, 1, 3), ("mx", 1), ("E", 12), ("F", 10), ("M", 10), ("issue", 13), ("plane", 3, 3),
    ("X", 1, 1, 0, 2), ("EM", 12), ("X", 1, 1, 2, 3), ("Q", 1, 0, 3), ("X", 1, 1, 3, 4), ("FM", 8), ("E", 13),
    ("OM", 9), ("P", 2, 1, 0), ("P", 2, 1, 1), ("M", 11), ("EM", 13), ("F", 11), ("X", 1, 0, 0, 1), ("plane", 4, 2),
    ("X", 1, 0, 1, 2), ("O", 12), ("P", 2, 1, 2), ("inv", 2, 1), ("F", 12), ("X", 1, 0, 2, 3), ("OM", 10), ("FM", 9),
    ("X", 1, 0, 3, 4), ("P", 2, 0, 1), ("M", 12), ("O", 13), ("plane", 4, 3), ("P", 2, 1, 3), ("P", 2, 0, 3),
    ("F", 13), ("P", 2, 0, 0), ("OM", 11), ("FM", 10), ("H", 0), ("inv", 2, 0), ("P", 2, 0, 2), ("M", 13),
    ("bplane", 10), ("FM", 11), ("Q", 2, 0, 1), ("OM", 12), ("bplane", 11), ("FM", 12), ("OM", 13), ("H", 1),
    ("bplane", 12), ("FM", 13), ("bplane", 13), ("Q", 2, 0, 3), ("Q", 2, 0, 0), ("Q", 2, 0, 2), ("X", 2, 0, 0, 4),
]
END_ORDER = [
    ("ey", 0), ("eown", 0), ("eM", 0), ("st", 0), ("ey", 1), ("eown", 1), ("eM", 1), ("st", 1), ("st", 2), ("ey", 2),
    ("ey", 3), ("eown", 2), ("ey", 4), ("eM", 2), ("eown", 3), ("ey", 5), ("eI", 2), ("eM", 3), ("st", 3),
    ("eown", 4), ("ey", 6), ("eM", 4), ("eown", 5), ("ey", 7), ("eM", 5), ("eown", 6), ("ey", 8), ("eO", 2),
    ("eIM", 2), ("eM", 6), ("eown", 7), ("ey", 9), ("eI", 3), ("eM", 7), ("eown", 8), ("ey", 10), ("eM", 8),
    ("eown", 9), ("ey", 11), ("eOM", 2), ("eO", 3), ("eM", 9), ("eown", 10), ("ey", 12), ("eIM", 3), ("eM", 10),
    ("eown", 11), ("ey", 13), ("eM", 11), ("eown", 12), ("eF", 2), ("eOM", 3), ("eM", 12), ("eown", 13), ("eF", 3),
    ("eM", 13), ("eI", 6), ("eFM", 2), ("epl", 2), ("eFM", 3), ("eO", 6), ("epl", 3), ("eIM", 6), ("eI", 7),
    ("eOM", 6), ("eIM", 7), ("emx", 0, 0), ("emx", 0, 1), ("emy", 0, 0), ("eO", 7), ("emy", 0, 1), ("eX", 0, 0, 2),
    ("eF", 6), ("eX", 0, 2, 4), ("eOM", 7), ("eF", 7), ("eI", 10), ("eFM", 6), ("eI", 11), ("epl", 6), ("eO", 10),
    ("eFM", 7), ("epl", 7), ("eIM", 10), ("eIM", 11), ("eI", 12), ("eOM", 10), ("eO", 11), ("eIM", 12),
    ("emx", 1, 0), ("eOM", 11), ("emx", 1, 1), ("eF", 10), ("emy", 1, 0), ("eI", 13), ("eF", 11), ("emy", 1, 1),
    ("eX", 1, 0, 1), ("eFM", 10), ("eX", 1, 1, 2), ("eO", 12), ("eX", 1, 2, 3), ("eIM", 13), ("epl", 10),
    ("eX", 1, 3, 4), ("eF", 12), ("eFM", 11), ("eO", 13), ("epl", 11), ("eOM", 12), ("eF", 13), ("eFM", 12),
    ("epl", 12), ("eOM", 13), ("emx", 2, 0), ("eFM", 13), ("epl", 13), ("emx", 2, 1), ("emy", 2, 0), ("emy", 2, 1),
    ("eX", 2, 0, 4),
]


def phase_table(feats):
    table = []
    for buf, count in enumerate(PIECES):
        width = feats // count
        table += [(buf, k * width, width) for k in range(count)]
    return table


def kernel(
    n_z, layers, halo,
    x_ref, gain_ref, wi_ref, scale_ref, wo_ref, o_ref,
    held, state, xg, edge, p_send, p_recv, mix, mix_in, part_sq, inv_col, sq_send, sq_recv,
    w_send, w_recv, local_sem, e_send, e_recv, s_send, s_recv, a_send, a_recv, m_send, m_recv,
):
    rows, feats = x_ref.shape
    total = rows + halo
    blocks, depth = held.shape[1], held.shape[2]
    pools = scale_ref.shape[1]
    chunk = pools // n_z
    last = layers - 1
    table = phase_table(feats)
    phases = len(table)
    lanes = 128
    quarter = feats // 4
    state_chunks = s_send.shape[0]
    sq_tiles = part_sq.shape[1] // lanes
    s = lax.axis_index("sp")
    t = lax.axis_index("tp")
    core = s % 2
    y = (s // 2) % 2
    z = s // 4
    side = z // 2

    def block_of(zz, yy, cc):
        return zz * 4 + yy * 2 + cc

    z_in, z_end = 1 + side, 3 * side
    z_over, z_far = 2 - side, 3 - 3 * side
    is_end = z == z_end
    s_end, s_in = block_of(z_end, y, core), block_of(z_in, y, core)

    y_mate = (block_of(z, 1 - y, core), t)
    c_mate = (block_of(z, y, 1 - core), t)
    x_mate = (s, 1 - t)
    opposite = (block_of(z_over, y, core), t)
    inner = (s_in, t)
    outer = (s_end, t)
    after = (s + 1) % blocks
    after_z = after // 4
    after_holder = (block_of(1 + after_z // 2, (after // 2) % 2, after % 2), t)
    after_slot = jnp.where((after_z == 0) | (after_z == n_z - 1), 1, 0)
    before = [((s_in + blocks - 1) % blocks, t), ((s_end + blocks - 1) % blocks, t)]

    barrier = pltpu.get_barrier_semaphore()

    def greet(peers):
        for peer in peers:
            pl.semaphore_signal(barrier, inc=1, device_id=peer, device_id_type=MESH_ID)

    sent = []

    def send(src, dst, send_sem, recv_sem, to, when=None):
        copy = pltpu.make_async_remote_copy(
            src_ref=src, dst_ref=dst, send_sem=send_sem, recv_sem=recv_sem,
            device_id=to, device_id_type=MESH_ID,
        )
        if when is None:
            copy.start()
        else:
            pl.when(when)(copy.start)
        sent.append((copy, when))

    def drain():
        for copy, when in sent:
            if when is None:
                copy.wait_send()
            else:
                pl.when(when)(copy.wait_send)
        sent.clear()

    def arrived(ref, sem):
        pltpu.make_async_remote_copy(
            src_ref=ref, dst_ref=ref, send_sem=sem, recv_sem=sem,
            device_id=c_mate, device_id_type=MESH_ID,
        ).wait_recv()

    whole, first, second = pl.ds(0, depth), pl.ds(0, depth // 2), pl.ds(depth // 2, depth // 2)
    count = [0] * phases

    def own(ph):
        buf, start, width = table[ph]
        return (wi_ref if buf % 2 == 0 else wo_ref).at[buf // 2, :, pl.ds(start, width)]

    def slot(ph, block, piece=whole):
        buf, start, width = table[ph]
        return held.at[buf, block, piece, pl.ds(start, width)]

    def recv_sem(ph, block, piece=whole):
        return w_recv.at[ph, block, 1 if piece is second else 0]

    def next_send(ph):
        count[ph] += 1
        return w_send.at[ph, count[ph] - 1]

    def send_own(ph, to):
        send(own(ph), slot(ph, s), next_send(ph), recv_sem(ph, s), to)

    def forward(ph, block, to, piece=whole):
        ref = slot(ph, block, piece)
        send(ref, ref, next_send(ph), recv_sem(ph, block, piece), to)

    def wait_block(ph, block, piece=whole):
        arrived(slot(ph, block, piece), recv_sem(ph, block, piece))

    state_rows = rows // state_chunks
    locals_ = {}

    def parts_of(buf):
        return [ph for ph in range(phases) if table[ph][0] == buf]

    def is_out(ph):
        return table[ph][0] % 2 == 1

    def keep_own(ph):
        copy = pltpu.make_async_copy(own(ph), slot(ph, s), local_sem.at[ph])
        copy.start()
        locals_[ph] = copy

    def from_core_mate(ph, zz):
        for yy in range(2):
            wait_block(ph, block_of(zz, yy, 1 - core))

    def send_edge():
        send(
            x_ref.at[pl.ds(rows - halo, halo)], edge.at[after_slot],
            e_send.at[0], e_recv.at[after_slot], after_holder,
        )

    def run(table_of_steps, order):
        for name, *args in order:
            with jax.named_scope("_".join([name] + [str(a) for a in args])):
                table_of_steps[name](*args)

    def end_program():
        greet([inner, y_mate, c_mate, x_mate])
        pl.semaphore_wait(barrier, 5)
        send_edge()
        mate = block_of(z_end, 1 - y, core)
        columns = [z_in, z_over, z_far]

        def own_aside(ph):
            if is_out(ph) or not EDGE_BY_MATE[table[ph][0]]:
                send_own(ph, y_mate)
            if is_out(ph):
                send_own(ph, c_mate)
                keep_own(ph)

        def own_inward(ph):
            send_own(ph, inner)

        def mate_inward(ph):
            direct = not EDGE_BY_MATE[table[ph][0]]
            if is_out(ph) or direct:
                wait_block(ph, mate)
            if direct:
                forward(ph, mate, inner)
            if is_out(ph):
                forward(ph, mate, c_mate)

        def ship_state(k):
            at = pl.ds(k * state_rows, state_rows)
            send(
                x_ref.at[at], state.at[1, pl.ds(halo + k * state_rows, state_rows)],
                s_send.at[k], s_recv.at[k], inner,
            )

        def take_column(which, ph):
            block = block_of(columns[which], y, core)
            wait_block(ph, block)
            forward(ph, block, y_mate)
            forward(ph, block, c_mate)

        def take_mate_column(which, ph):
            block = block_of(columns[which], 1 - y, core)
            wait_block(ph, block)
            forward(ph, block, c_mate)

        def gathered(ph):
            locals_[ph].wait()
            for zz in range(n_z):
                from_core_mate(ph, zz)

        def take_mix(layer, j):
            zz = 2 * t + j
            ref, sem = mix_in.at[layer, zz], m_recv.at[layer, zz]
            arrived(ref, sem)
            send(ref, ref, m_send.at[layer, j], sem, x_mate)

        def take_mate_mix(layer, j):
            zz = 2 * (1 - t) + j
            arrived(mix_in.at[layer, zz], m_recv.at[layer, zz])

        def end_expand(layer, begin, end):
            width = 256
            at = pl.ds(halo, rows)

            @pl.loop(begin * quarter // width, end * quarter // width)
            def _(n):
                cols = pl.ds(pl.multiple_of(n * width, width), width)
                mixed = jnp.concatenate([mix_in[layer, c] for c in range(n_z)], axis=1)
                weight = held[2 * layer + 1, :, :, cols].reshape(pools, width)
                branch = jnp.dot(mixed, weight, preferred_element_type=jnp.float32)
                old = x_ref[:, cols] if layer == 0 else state[1, at, cols]
                new = (old.astype(jnp.float32) + branch).astype(jnp.bfloat16)
                if layer == last:
                    o_ref[:, cols] = new
                else:
                    state[1, at, cols] = new

        part = functools.partial
        run({
            "ey": own_aside, "eown": own_inward, "eM": mate_inward, "st": ship_state,
            "eI": part(take_column, 0), "eO": part(take_column, 1), "eF": part(take_column, 2),
            "eIM": part(take_mate_column, 0), "eOM": part(take_mate_column, 1),
            "eFM": part(take_mate_column, 2), "epl": gathered,
            "emx": take_mix, "emy": take_mate_mix, "eX": end_expand,
        }, END_ORDER)
        drain()

    def inner_program():
        greet([opposite, y_mate, c_mate, x_mate, outer] + before)
        pl.semaphore_wait(barrier, 6)
        send_edge()
        chunk_z = [z_in, z_end, z_over, z_far]

        def issue(ph):
            send_own(ph, opposite)
            send_own(ph, y_mate)
            send_own(ph, c_mate)
            if is_out(ph):
                send_own(ph, outer)
            keep_own(ph)

        def over_pieces(ph):
            share = OVER_BY_MATE[table[ph][0]]
            by_mate = None if share == 0 else whole if share == 1 else first
            direct = None if share == 1 else whole if share == 0 else second
            return by_mate, direct

        def take_end(ph):
            block = block_of(z_end, y, core)
            wait_block(ph, block)
            forward(ph, block, opposite)
            if EDGE_BY_MATE[table[ph][0]]:
                forward(ph, block, y_mate)
            forward(ph, block, c_mate)

        def take_over(ph):
            block = block_of(z_over, y, core)
            wait_block(ph, block)
            by_mate, _ = over_pieces(ph)
            if by_mate is not None:
                forward(ph, block, y_mate, by_mate)
            forward(ph, block, c_mate)
            if is_out(ph):
                forward(ph, block, outer)

        def take_mate(ph):
            block = block_of(z_in, 1 - y, core)
            wait_block(ph, block)
            _, direct = over_pieces(ph)
            if direct is not None:
                forward(ph, block, opposite, direct)
            forward(ph, block, c_mate)

        def take_far(ph):
            block = block_of(z_far, y, core)
            wait_block(ph, block)
            forward(ph, block, y_mate)
            forward(ph, block, c_mate)
            if is_out(ph):
                forward(ph, block, outer)

        def take_mate_end(ph):
            block = block_of(z_end, 1 - y, core)
            wait_block(ph, block)
            forward(ph, block, c_mate)

        def take_mate_over(ph):
            block = block_of(z_over, 1 - y, core)
            for piece in over_pieces(ph):
                if piece is not None:
                    wait_block(ph, block, piece)
            forward(ph, block, c_mate)

        def take_mate_far(ph):
            block = block_of(z_far, 1 - y, core)
            wait_block(ph, block)
            forward(ph, block, c_mate)

        def plane(ph, k):
            if k == 0:
                locals_[ph].wait()
            from_core_mate(ph, chunk_z[k])

        def planes_of(buf, k):
            for ph in parts_of(buf):
                plane(ph, k)

        def all_planes(ph):
            for k in range(n_z):
                plane(ph, k)

        def first_row(layer):
            return REACH * layer

        def from_row(start):
            return pl.ds(start, total - start)

        def gain_of(layer, start, width):
            at = pl.multiple_of(t * feats + start, lanes)
            return gain_ref[pl.ds(layer, 1), pl.ds(at, width)]

        def pack_squares(g, layer):
            for k in range(sq_tiles):
                block = part_sq[g, pl.ds(k * lanes, lanes)].T
                value = jnp.sum(block, axis=0, keepdims=True)
                sq_send[layer, g, k] = jnp.broadcast_to(value, (8, lanes))
            exchange(sq_send.at[layer, g], sq_recv.at[layer, g], layer, g, n_z)

        def exchange(src, dst, layer, g, k, when=None):
            send(src, dst, a_send.at[layer, g, k], a_recv.at[layer, g, k], x_mate, when)

        def halved(layer, g):
            return layer == last and g == 1

        def mix_slot(layer, g):
            return 0 if g == 0 else 1 + layer

        def take_edge(g):
            arrived(edge.at[g], e_recv.at[g])
            keep = ((s_in if g == 0 else s_end) > 0).astype(jnp.float32)

            @pl.loop(0, halo // REACH)
            def _(i):
                at = pl.ds(i * REACH, REACH)
                state[g, at] = (edge[g, at].astype(jnp.float32) * keep).astype(jnp.bfloat16)

        def own_state():
            @pl.loop(0, rows // REACH)
            def _(i):
                state[0, pl.ds(halo + i * REACH, REACH)] = x_ref[pl.ds(i * REACH, REACH)]

        def take_state(k):
            arrived(state.at[1, pl.ds(halo + k * state_rows, state_rows)], s_recv.at[k])

        def squares(g, start, stop):
            @pl.loop(start // REACH, stop // REACH)
            def _(i):
                at = pl.ds(i * REACH, REACH)
                sums = jnp.zeros((REACH, lanes), jnp.float32)
                for j in range(feats // lanes):
                    cols = pl.ds(j * lanes, lanes)
                    wide = state[g, at, cols].astype(jnp.float32)
                    sums = sums + wide * wide
                    xg[g, at, cols] = (wide * gain_of(0, j * lanes, lanes)).astype(jnp.bfloat16)
                part_sq[g, at] = sums

        def project(layer, g, k):
            at = from_row(first_row(layer))
            zz = chunk_z[k]
            weight = held[2 * layer, pl.ds(zz * 4, 4)].reshape(chunk, feats)
            value = lax.dot_general(
                xg[g, at], weight, (((1,), (1,)), ((), ())),
                preferred_element_type=jnp.float32,
            )
            p_send[layer, g, zz, at] = value.astype(jnp.bfloat16)
            when = (zz // 2 != t) if halved(layer, g) else None
            exchange(p_send.at[layer, g, zz, at], p_recv.at[layer, g, zz, at], layer, g, zz, when)

        def inverse(layer, g):
            arrived(sq_recv.at[layer, g], a_recv.at[layer, g, n_z])
            for k in range(sq_tiles):
                mean = (sq_send[layer, g, k] + sq_recv[layer, g, k]) / (2 * feats)
                inv = lax.rsqrt(mean + EPS)
                inv_col[g, pl.ds(k * lanes, lanes)] = jnp.broadcast_to(inv[0:1], (lanes, lanes)).T

        def pool(layer, g, k):
            pool_plane(layer, g, chunk_z[k])

        def pool_half(j):
            pool_plane(last, 1, 2 * t + j)
            ship_mix(last, j)

        def ship_mix(layer, j):
            zz = 2 * t + j
            send(
                mix.at[mix_slot(layer, 1), zz, pl.ds(halo, rows)], mix_in.at[layer, zz],
                m_send.at[layer, j], m_recv.at[layer, zz], outer,
            )

        def ship_mixes(layer):
            for j in range(2):
                ship_mix(layer, j)

        def pool_plane(layer, g, group):
            start = first_row(layer)
            at = from_row(start)
            arrived(p_recv.at[layer, g, group, at], a_recv.at[layer, g, group])
            row = lax.broadcasted_iota(jnp.int32, (total - start, lanes), 0)
            position = (s_in if g == 0 else s_end) * rows - halo + start + row
            span = jnp.left_shift(jnp.int32(2), group)
            divisor = jnp.maximum(jnp.minimum(position + 1, span), 1).astype(jnp.float32)
            share = 1.0 / divisor
            inv = inv_col[g, at]
            for j in range(chunk // lanes):
                cols = pl.ds(j * lanes, lanes)
                joined = p_send[layer, g, group, at, cols].astype(jnp.float32)
                joined = joined + p_recv[layer, g, group, at, cols].astype(jnp.float32)
                base = (joined * inv).astype(jnp.bfloat16).astype(jnp.float32)
                running = base
                width = 1
                picked = None
                for step in range(GROUPS):
                    running = running + pltpu.roll(running, width, 0)
                    width *= 2
                    picked = running if picked is None else jnp.where(group >= step, running, picked)
                lane = pl.multiple_of(group * chunk + j * lanes, lanes)
                scale = scale_ref[pl.ds(layer, 1), pl.ds(lane, lanes)]
                mix[mix_slot(layer, g), group, at, cols] = ((picked * share - base) * scale).astype(jnp.bfloat16)

        def expand(layer, g, begin, end):
            width = 256
            at = from_row(first_row(layer + 1))
            buf = 2 * layer + 1
            if layer < last and begin == 0:
                part_sq[g] = jnp.zeros(part_sq.shape[1:], jnp.float32)

            @pl.loop(begin * quarter // width, end * quarter // width)
            def _(n):
                col = pl.multiple_of(n * width, width)
                cols = pl.ds(col, width)
                mixed = jnp.concatenate([mix[mix_slot(layer, g), c, at] for c in range(n_z)], axis=1)
                weight = held[buf, :, :, cols].reshape(pools, width)
                branch = jnp.dot(mixed, weight, preferred_element_type=jnp.float32)
                new = (state[g, at, cols].astype(jnp.float32) + branch).astype(jnp.bfloat16)
                if layer == last:
                    o_ref[:, cols] = new
                else:
                    state[g, at, cols] = new
                    wide = new.astype(jnp.float32)
                    xg[g, at, cols] = (wide * gain_of(layer + 1, col, width)).astype(jnp.bfloat16)
                    square = wide * wide
                    sums = square[:, :lanes]
                    for j in range(1, width // lanes):
                        sums = sums + square[:, j * lanes:(j + 1) * lanes]
                    part_sq[g, at] = part_sq[g, at] + sums

            if layer < last and end == 4:
                pack_squares(g, layer + 1)

        def prepare():
            for g in range(2):
                part_sq[g] = jnp.zeros(part_sq.shape[1:], jnp.float32)
            own_state()

        def first_squares(g):
            take_edge(g)
            squares(g, 0, total if g == 0 else halo)
            pack_squares(g, 0)

        def shipped_squares(k):
            take_state(k)
            squares(1, halo + k * state_rows, halo + (k + 1) * state_rows)

        run({
            "issue": issue, "E": take_end, "O": take_over, "M": take_mate, "F": take_far,
            "EM": take_mate_end, "OM": take_mate_over, "FM": take_mate_far,
            "plane": planes_of, "bplane": all_planes, "init": prepare, "sq": first_squares,
            "st": shipped_squares, "P": project, "Q": pool, "inv": inverse, "H": pool_half,
            "mx": ship_mixes, "X": expand,
        }, INNER_ORDER)
        drain()

    pl.when(is_end)(end_program)
    for ph in range(phases):
        count[ph] = 0
    locals_.clear()
    pl.when(jnp.logical_not(is_end))(inner_program)


def fused_body(inputs, norm_gain, in_weight, pool_scale, out_weight):
    rows, feats = inputs.shape
    layers = norm_gain.shape[0]
    pools = pool_scale.shape[1]
    blocks = lax.axis_size("sp")
    n_z = blocks // 4
    depth = out_weight.shape[1]
    halo = REACH * layers
    total = rows + halo
    sq_tiles = -(-total // 128)
    chunk = pools // n_z
    phases = len(phase_table(feats))
    state_chunks = len([row for row in END_ORDER if row[0] == "st"])
    bf, f32 = jnp.bfloat16, jnp.float32
    vmem = pl.BlockSpec(memory_space=pltpu.VMEM)
    dma = pltpu.SemaphoreType.DMA
    return pl.pallas_call(
        functools.partial(kernel, n_z, layers, halo),
        out_shape=jax.ShapeDtypeStruct((rows, feats), bf),
        in_specs=[vmem] * 5,
        out_specs=vmem,
        scratch_shapes=[
            pltpu.VMEM((2 * layers, blocks, depth, feats), bf),
            pltpu.VMEM((2, total, feats), bf),
            pltpu.VMEM((2, total, feats), bf),
            pltpu.VMEM((2, halo, feats), bf),
            pltpu.VMEM((layers, 2, n_z, total, chunk), bf),
            pltpu.VMEM((layers, 2, n_z, total, chunk), bf),
            pltpu.VMEM((1 + layers, n_z, total, chunk), bf),
            pltpu.VMEM((layers, n_z, rows, chunk), bf),
            pltpu.VMEM((2, sq_tiles * 128, 128), f32),
            pltpu.VMEM((2, sq_tiles * 128, 128), f32),
            pltpu.VMEM((layers, 2, sq_tiles, 8, 128), f32),
            pltpu.VMEM((layers, 2, sq_tiles, 8, 128), f32),
            dma((phases, 18)),
            dma((phases, blocks, 2)),
            dma((phases,)),
            dma((1,)),
            dma((2,)),
            dma((state_chunks,)),
            dma((state_chunks,)),
            dma((layers, 2, n_z + 1)),
            dma((layers, 2, n_z + 1)),
            dma((layers, 2)),
            dma((layers, n_z)),
        ],
        compiler_params=pltpu.CompilerParams(
            collective_id=0, has_side_effects=True, vmem_limit_bytes=60 * 1024 * 1024
        ),
    )(inputs, norm_gain, jnp.swapaxes(in_weight, 1, 2), pool_scale, out_weight)


def solution(mesh):
    n_sp, n_tp = mesh.shape["sp"], mesh.shape["tp"]
    fused = n_tp == 2 and n_sp == 16
    placed = (P("sp", "tp"), P(), P(None, "tp", "sp"), P(), P(None, "sp", "tp"))
    return jax.shard_map(
        fused_body if fused else plain_body,
        mesh=mesh, in_specs=placed, out_specs=P("sp", "tp"), check_vma=False,
    )
```

```python
import functools

import jax
import jax.numpy as jnp
from jax import lax
from jax.experimental import pallas as pl
from jax.experimental.pallas import tpu as pltpu
from jax.sharding import PartitionSpec as P

EPS = 1e-06
REACH = 16
GROUPS = 4
MESH_ID = pl.DeviceIdType.MESH


def shift_sp(value):
    count = lax.axis_size("sp")
    return lax.ppermute(value, "sp", [(i, i + 1) for i in range(count - 1)])


def window_means(extended, row_count, first_channel, first_pos, pool_total):
    width = extended.shape[1]
    channel = first_channel + lax.broadcasted_iota(jnp.int32, (1, width), 1)
    window_len = jnp.left_shift(jnp.int32(2), channel // (pool_total // GROUPS))
    running = jnp.zeros((row_count, width), jnp.float32)
    for offset in range(REACH):
        shifted = extended[REACH - offset : REACH - offset + row_count]
        running = running + jnp.where(offset < window_len, shifted, 0.0)
    position = first_pos + lax.broadcasted_iota(jnp.int32, (row_count, 1), 0)
    divisor = jnp.minimum(position + 1, window_len).astype(jnp.float32)
    return running / divisor - extended[REACH:]


def plain_body(inputs, norm_gain, in_weight, pool_scale, out_weight):
    rows, feats = inputs.shape
    layers, features = norm_gain.shape
    pools = pool_scale.shape[1]
    part = pools // lax.axis_size("tp")
    t = lax.axis_index("tp")
    s = lax.axis_index("sp")
    current = inputs
    for layer in range(layers):
        in_all = lax.all_gather(in_weight[layer], "sp", axis=1, tiled=True)
        out_all = lax.all_gather(out_weight[layer], "sp", axis=0, tiled=True)
        wide = current.astype(jnp.float32)
        squares = lax.psum(jnp.sum(wide * wide, axis=1), "tp")
        inv_rms = lax.rsqrt(squares / features + EPS)[:, None]
        gain = lax.dynamic_slice_in_dim(norm_gain[layer], t * feats, feats)
        normed = (wide * inv_rms * gain).astype(jnp.bfloat16)
        partial = jnp.dot(normed, in_all, preferred_element_type=jnp.float32)
        pool_in = lax.psum_scatter(
            partial.astype(jnp.bfloat16), "tp", scatter_dimension=1, tiled=True
        )
        edge = shift_sp(pool_in[rows - REACH :])
        extended = jnp.concatenate([edge, pool_in], 0).astype(jnp.float32)
        means = window_means(extended, rows, t * part, s * rows, pools)
        scale = lax.dynamic_slice_in_dim(pool_scale[layer], t * part, part)
        mixed = (means * scale).astype(jnp.bfloat16)
        pooled = lax.all_gather(mixed, "tp", axis=1, tiled=True)
        branch = jnp.dot(pooled, out_all, preferred_element_type=jnp.float32)
        current = (current.astype(jnp.float32) + branch).astype(jnp.bfloat16)
    return current


E, O, M, F, EM, OM1, OM2, FM = range(8)
PIECES = (2, 2, 2, 2, 2, 2)
EDGE_BY_MATE = (True, True, False, False, False, False)
OVER_BY_MATE = (0.5, 0, 0, 1, 0, 0)
INNER_ORDER = [
    ("issue", 0), ("issue", 1), ("edge",), ("issue", 2), ("init",), ("O", 0), ("M", 0), ("E", 0), ("M", 1), ("O", 1),
    ("plane", 0, 0), ("sq", 0), ("P", 0, 0, 0), ("O", 2), ("M", 2), ("inv", 0, 0), ("st", 0), ("OM", 0), ("F", 0),
    ("issue", 3), ("E", 1), ("EM", 0), ("Q", 0, 0, 0), ("OM", 1), ("plane", 0, 2), ("P", 0, 0, 2), ("OM", 2),
    ("E", 2), ("FM", 0), ("O", 3), ("M", 3), ("F", 1), ("issue", 4), ("Q", 0, 0, 2), ("st", 1), ("EM", 1),
    ("plane", 0, 1), ("P", 0, 0, 1), ("F", 2), ("issue", 5), ("E", 3), ("EM", 2), ("OM", 3), ("FM", 1),
    ("plane", 0, 3), ("P", 0, 0, 3), ("O", 4), ("Q", 0, 0, 1), ("st", 2), ("M", 4), ("O", 5), ("FM", 2), ("F", 3),
    ("issue", 6), ("Q", 0, 0, 3), ("st", 3), ("sq", 1), ("P", 0, 1, 3), ("M", 5), ("P", 0, 1, 1), ("P", 0, 1, 0),
    ("E", 4), ("OM", 4), ("plane", 2, 0), ("inv", 0, 1), ("P", 0, 1, 2), ("EM", 3), ("O", 6), ("EM", 4), ("FM", 3),
    ("Q", 0, 1, 3), ("all", 1), ("X", 0, 0, 0, 1), ("OM", 5), ("X", 0, 0, 1, 2), ("E", 5), ("X", 0, 0, 2, 3),
    ("M", 6), ("plane", 2, 2), ("X", 0, 0, 3, 4), ("P", 1, 0, 2), ("F", 4), ("issue", 7), ("EM", 5), ("P", 1, 0, 0),
    ("OM", 6), ("Q", 0, 1, 1), ("plane", 2, 1), ("P", 1, 0, 1), ("F", 5), ("issue", 8), ("Q", 0, 1, 0), ("E", 6),
    ("FM", 4), ("Q", 0, 1, 2), ("O", 7), ("inv", 1, 0), ("EM", 6), ("mx", 0), ("X", 0, 1, 0, 3), ("M", 7),
    ("X", 0, 1, 3, 4), ("O", 8), ("E", 7), ("P", 1, 1, 1), ("P", 1, 1, 0), ("Q", 1, 0, 2), ("FM", 5), ("P", 1, 1, 2),
    ("F", 6), ("issue", 9), ("EM", 7), ("plane", 2, 3), ("P", 1, 1, 3), ("P", 1, 0, 3), ("M", 8), ("Q", 1, 0, 0),
    ("F", 7), ("issue", 10), ("E", 8), ("Q", 1, 0, 1), ("inv", 1, 1), ("OM", 7), ("O", 9), ("EM", 8), ("Q", 1, 1, 1),
    ("FM", 6), ("OM", 8), ("E", 9), ("M", 9), ("Q", 1, 1, 0), ("O", 10), ("EM", 9), ("plane", 4, 0), ("plane", 4, 1),
    ("FM", 7), ("Q", 1, 1, 2), ("F", 8), ("issue", 11), ("E", 10), ("M", 10), ("F", 9), ("Q", 1, 1, 3), ("EM", 10),
    ("mx", 1), ("all", 3), ("X", 1, 1, 0, 3), ("FM", 8), ("X", 1, 1, 3, 4), ("E", 11), ("OM", 9), ("Q", 1, 0, 3),
    ("P", 2, 1, 0), ("P", 2, 1, 1), ("M", 11), ("plane", 4, 2), ("P", 2, 1, 2), ("O", 11), ("inv", 2, 1), ("EM", 11),
    ("X", 1, 0, 0, 3), ("FM", 9), ("X", 1, 0, 3, 4), ("F", 10), ("P", 2, 0, 2), ("plane", 4, 3), ("P", 2, 1, 3),
    ("P", 2, 0, 1), ("H", 0), ("OM", 10), ("inv", 2, 0), ("P", 2, 0, 0), ("P", 2, 0, 3), ("FM", 10), ("F", 11),
    ("Q", 2, 0, 2), ("bplane", 10), ("OM", 11), ("H", 1), ("FM", 11), ("bplane", 11), ("Q", 2, 0, 1), ("Q", 2, 0, 0),
    ("Q", 2, 0, 3), ("X", 2, 0, 0, 4),
]
END_ORDER = [
    ("ey", 0), ("ey", 1), ("eown", 0), ("eM", 0), ("edge", 1), ("st", 0), ("eown", 1), ("edge", 0), ("eM", 1),
    ("ey", 2), ("eown", 2), ("ey", 3), ("ey", 4), ("eI", 2), ("eM", 2), ("st", 1), ("eown", 3), ("ey", 5), ("eM", 3),
    ("st", 2), ("st", 3), ("eown", 4), ("ey", 6), ("eM", 4), ("eown", 5), ("ey", 7), ("eIM", 2), ("eO", 2),
    ("eM", 5), ("eown", 6), ("ey", 8), ("eI", 3), ("eM", 6), ("eown", 7), ("ey", 9), ("eM", 7), ("eown", 8),
    ("ey", 10), ("eOM", 2), ("eO", 3), ("eM", 8), ("eown", 9), ("ey", 11), ("eIM", 3), ("eF", 2), ("eM", 9),
    ("eown", 10), ("eM", 10), ("eown", 11), ("eOM", 3), ("eM", 11), ("eF", 3), ("eFM", 2), ("eI", 6), ("eFM", 3),
    ("eO", 6), ("eIM", 6), ("eOM", 6), ("eI", 7), ("eIM", 7), ("eO", 7), ("emx", 0, 0), ("eOM", 7), ("emx", 0, 1),
    ("emy", 0, 0), ("eF", 6), ("emy", 0, 1), ("eall", 1), ("eX", 0, 0, 2), ("eF", 7), ("eX", 0, 2, 4), ("eFM", 6),
    ("eI", 10), ("eFM", 7), ("eO", 10), ("eIM", 10), ("eI", 11), ("eOM", 10), ("emx", 1, 0), ("eIM", 11),
    ("emx", 1, 1), ("emy", 1, 0), ("eO", 11), ("emy", 1, 1), ("eall", 3), ("eX", 1, 0, 2), ("eF", 10),
    ("eX", 1, 2, 4), ("eOM", 11), ("emx", 2, 0), ("eFM", 10), ("eF", 11), ("epl", 10), ("emy", 2, 0), ("emx", 2, 1),
    ("eFM", 11), ("epl", 11), ("emy", 2, 1), ("eX", 2, 0, 4),
]


def phase_table(feats):
    table = []
    for buf, count in enumerate(PIECES):
        width = feats // count
        table += [(buf, k * width, width) for k in range(count)]
    return table


def kernel(
    n_z, layers, halo,
    x_ref, gain_ref, wi_ref, scale_ref, wo_ref, o_ref,
    held, state, xg, edge, p_send, p_recv, mix, mix_in, part_sq, inv_col, sq_send, sq_recv,
    w_send, w_recv, c_recv, local_sem, e_send, e_recv, s_send, s_recv, a_send, a_recv, m_send, m_recv,
):
    rows, feats = x_ref.shape
    total = rows + halo
    blocks, depth = held.shape[1], held.shape[2]
    pools = scale_ref.shape[1]
    chunk = pools // n_z
    last = layers - 1
    table = phase_table(feats)
    phases = len(table)
    lanes = 128
    quarter = feats // 4
    state_chunks = s_recv.shape[0]
    last_buf = len(PIECES) - 1
    sq_tiles = part_sq.shape[1] // lanes
    s = lax.axis_index("sp")
    t = lax.axis_index("tp")
    core = s % 2
    y = (s // 2) % 2
    z = s // 4
    side = z // 2

    def block_of(zz, yy, cc):
        return zz * 4 + yy * 2 + cc

    z_in, z_end = 1 + side, 3 * side
    z_over, z_far = 2 - side, 3 - 3 * side
    is_end = z == z_end
    s_end, s_in = block_of(z_end, y, core), block_of(z_in, y, core)

    y_mate = (block_of(z, 1 - y, core), t)
    c_mate = (block_of(z, y, 1 - core), t)
    x_mate = (s, 1 - t)
    opposite = (block_of(z_over, y, core), t)
    inner = (s_in, t)
    outer = (s_end, t)
    after = (s + 1) % blocks
    after_z = after // 4
    after_holder = (block_of(1 + after_z // 2, (after // 2) % 2, after % 2), t)
    after_slot = jnp.where((after_z == 0) | (after_z == n_z - 1), 1, 0)
    before = [((s_in + blocks - 1) % blocks, t), ((s_end + blocks - 1) % blocks, t)]

    barrier = pltpu.get_barrier_semaphore()

    def greet(peers):
        for peer in peers:
            pl.semaphore_signal(barrier, inc=1, device_id=peer, device_id_type=MESH_ID)

    def send(src, dst, send_sem, recv_sem, to, when=None):
        copy = pltpu.make_async_remote_copy(
            src_ref=src, dst_ref=dst, send_sem=send_sem, recv_sem=recv_sem,
            device_id=to, device_id_type=MESH_ID,
        )
        if when is None:
            copy.start()
        else:
            pl.when(when)(copy.start)

    def departed(ref, sem):
        pltpu.make_async_remote_copy(
            src_ref=ref, dst_ref=ref, send_sem=sem, recv_sem=sem,
            device_id=c_mate, device_id_type=MESH_ID,
        ).wait_send()

    def arrived(ref, sem):
        pltpu.make_async_remote_copy(
            src_ref=ref, dst_ref=ref, send_sem=sem, recv_sem=sem,
            device_id=c_mate, device_id_type=MESH_ID,
        ).wait_recv()

    whole, first, second = pl.ds(0, depth), pl.ds(0, depth // 2), pl.ds(depth // 2, depth // 2)
    volume = {}

    def own(ph):
        buf, start, width = table[ph]
        return (wi_ref if buf % 2 == 0 else wo_ref).at[buf // 2, :, pl.ds(start, width)]

    def slot(ph, block, piece=whole):
        buf, start, width = table[ph]
        return held.at[buf, block, piece, pl.ds(start, width)]

    def send_sem(ph, port, piece):
        buf, _, width = table[ph]
        kind = 1 if port == EM else 0
        share = width * (1 if piece is whole else 0.5) / feats
        volume[buf, kind] = volume.get((buf, kind), 0) + share
        return w_send.at[buf, kind]

    def core_sem(ph, block):
        buf, start, width = table[ph]
        layer = buf // 2
        if buf % 2 == 0:
            return c_recv.at[layer * n_z + block // 4]
        return c_recv.at[layers * n_z + layer + (start // width if buf == last_buf else 0)]

    def send_own(ph, to, port):
        sem = core_sem(ph, s) if port is None else w_recv.at[ph, port]
        send(own(ph), slot(ph, s), send_sem(ph, port, whole), sem, to)

    def forward(ph, block, to, port, piece=whole):
        ref = slot(ph, block, piece)
        sem = core_sem(ph, block) if port is None else w_recv.at[ph, port]
        send(ref, ref, send_sem(ph, port, piece), sem, to)

    def wait_block(ph, block, port, piece=whole):
        arrived(slot(ph, block, piece), w_recv.at[ph, port])

    def drain_weights():
        for (buf, kind), blocks_sent in volume.items():
            assert blocks_sent == int(blocks_sent)
            departed(held.at[buf, pl.ds(0, int(blocks_sent))], w_send.at[buf, kind])
        volume.clear()

    state_rows = rows // state_chunks
    def parts_of(buf):
        return [ph for ph in range(phases) if table[ph][0] == buf]

    def is_out(ph):
        return table[ph][0] % 2 == 1

    def local_of(ph):
        buf, start, width = table[ph]
        return local_sem.at[buf + (start // width if buf == last_buf else 0)]

    def keep_own(ph):
        pltpu.make_async_copy(own(ph), slot(ph, s), local_of(ph)).start()

    def gathered(buf):
        ph = parts_of(buf)[0]
        weight = (wi_ref if buf % 2 == 0 else wo_ref).at[buf // 2]
        pltpu.make_async_copy(weight, held.at[buf, s], local_of(ph)).wait()
        arrived(held.at[buf, pl.ds(0, blocks // 2)], core_sem(ph, s))

    def gathered_piece(ph):
        buf, start, width = table[ph]
        pltpu.make_async_copy(own(ph), slot(ph, s), local_of(ph)).wait()
        arrived(held.at[buf, pl.ds(0, blocks // 2), :, pl.ds(start, width)], core_sem(ph, s))

    def send_edge(when=None):
        send(
            x_ref.at[pl.ds(rows - halo, halo)], edge.at[after_slot],
            e_send.at[0], e_recv.at[after_slot], after_holder, when,
        )

    def send_some_edges(which):
        send_edge(after_slot == which)

    def run(table_of_steps, order):
        for name, *args in order:
            with jax.named_scope("_".join([name] + [str(a) for a in args])):
                table_of_steps[name](*args)

    def end_program():
        greet([inner, y_mate, c_mate, x_mate])
        pl.semaphore_wait(barrier, 5)
        mate = block_of(z_end, 1 - y, core)
        columns = [z_in, z_over, z_far]

        def own_aside(ph):
            if is_out(ph) or not EDGE_BY_MATE[table[ph][0]]:
                send_own(ph, y_mate, M)
            if is_out(ph):
                send_own(ph, c_mate, None)
                keep_own(ph)

        def own_inward(ph):
            send_own(ph, inner, E)

        def mate_inward(ph):
            direct = not EDGE_BY_MATE[table[ph][0]]
            if is_out(ph) or direct:
                wait_block(ph, mate, M)
            if direct:
                forward(ph, mate, inner, EM)
            if is_out(ph):
                forward(ph, mate, c_mate, None)

        def ship_state(k):
            at = pl.ds(k * state_rows, state_rows)
            send(
                x_ref.at[at], state.at[1, pl.ds(halo + k * state_rows, state_rows)],
                s_send.at[0], s_recv.at[k], inner,
            )

        def take_column(which, ph):
            block = block_of(columns[which], y, core)
            wait_block(ph, block, (E, O, F)[which])
            forward(ph, block, y_mate, (EM, OM1, FM)[which])
            forward(ph, block, c_mate, None)

        def take_mate_column(which, ph):
            block = block_of(columns[which], 1 - y, core)
            wait_block(ph, block, (EM, OM1, FM)[which])
            forward(ph, block, c_mate, None)

        def take_mix(layer, j):
            zz = 2 * t + j
            ref, sem = mix_in.at[layer, zz], m_recv.at[layer, zz]
            arrived(ref, sem)
            send(ref, ref, m_send.at[layer], sem, x_mate)

        def take_mate_mix(layer, j):
            zz = 2 * (1 - t) + j
            arrived(mix_in.at[layer, zz], m_recv.at[layer, zz])

        def end_expand(layer, begin, end):
            width = 256
            at = pl.ds(halo, rows)

            @pl.loop(begin * quarter // width, end * quarter // width)
            def _(n):
                cols = pl.ds(pl.multiple_of(n * width, width), width)
                mixed = jnp.concatenate([mix_in[layer, c] for c in range(n_z)], axis=1)
                weight = held[2 * layer + 1, :, :, cols].reshape(pools, width)
                branch = jnp.dot(mixed, weight, preferred_element_type=jnp.float32)
                old = x_ref[:, cols] if layer == 0 else state[1, at, cols]
                new = (old.astype(jnp.float32) + branch).astype(jnp.bfloat16)
                if layer == last:
                    o_ref[:, cols] = new
                else:
                    state[1, at, cols] = new

        part = functools.partial
        run({
            "ey": own_aside, "eown": own_inward, "eM": mate_inward, "st": ship_state,
            "eI": part(take_column, 0), "eO": part(take_column, 1), "eF": part(take_column, 2),
            "eIM": part(take_mate_column, 0), "eOM": part(take_mate_column, 1),
            "eFM": part(take_mate_column, 2), "eall": gathered, "epl": gathered_piece,
            "edge": send_some_edges,
            "emx": take_mix, "emy": take_mate_mix, "eX": end_expand,
        }, END_ORDER)
        with jax.named_scope("drain"):
            drain_weights()
            departed(x_ref, s_send.at[0])
            departed(x_ref.at[pl.ds(0, halo)], e_send.at[0])
            for layer in range(layers):
                departed(mix_in.at[layer, pl.ds(2 * t, 2)], m_send.at[layer])

    def inner_program():
        with jax.named_scope("greet"):
            greet([opposite, y_mate, c_mate, x_mate, outer] + before)
        with jax.named_scope("barrier"):
            pl.semaphore_wait(barrier, 6)
        chunk_z = [z_in, z_end, z_over, z_far]

        def issue(ph):
            send_own(ph, opposite, O)
            send_own(ph, y_mate, M)
            send_own(ph, c_mate, None)
            if is_out(ph):
                send_own(ph, outer, E)
            keep_own(ph)

        def over_pieces(ph):
            share = OVER_BY_MATE[table[ph][0]]
            by_mate = None if share == 0 else whole if share == 1 else first
            direct = None if share == 1 else whole if share == 0 else second
            return by_mate, direct

        def take_end(ph):
            block = block_of(z_end, y, core)
            wait_block(ph, block, E)
            forward(ph, block, opposite, F)
            if EDGE_BY_MATE[table[ph][0]]:
                forward(ph, block, y_mate, EM)
            forward(ph, block, c_mate, None)

        def take_over(ph):
            block = block_of(z_over, y, core)
            wait_block(ph, block, O)
            by_mate, _ = over_pieces(ph)
            if by_mate is not None:
                forward(ph, block, y_mate, OM1, by_mate)
            forward(ph, block, c_mate, None)
            if is_out(ph):
                forward(ph, block, outer, O)

        def take_mate(ph):
            block = block_of(z_in, 1 - y, core)
            wait_block(ph, block, M)
            _, direct = over_pieces(ph)
            if direct is not None:
                forward(ph, block, opposite, OM2, direct)
            forward(ph, block, c_mate, None)

        def take_far(ph):
            block = block_of(z_far, y, core)
            wait_block(ph, block, F)
            forward(ph, block, y_mate, FM)
            forward(ph, block, c_mate, None)
            if is_out(ph):
                forward(ph, block, outer, F)

        def take_mate_end(ph):
            block = block_of(z_end, 1 - y, core)
            wait_block(ph, block, EM)
            forward(ph, block, c_mate, None)

        def take_mate_over(ph):
            block = block_of(z_over, 1 - y, core)
            by_mate, direct = over_pieces(ph)
            if by_mate is not None:
                wait_block(ph, block, OM1, by_mate)
            if direct is not None:
                wait_block(ph, block, OM2, direct)
            forward(ph, block, c_mate, None)

        def take_mate_far(ph):
            block = block_of(z_far, 1 - y, core)
            wait_block(ph, block, FM)
            forward(ph, block, c_mate, None)

        def plane(buf, k):
            if k == 0:
                weight = wi_ref.at[buf // 2]
                pltpu.make_async_copy(weight, held.at[buf, s], local_of(parts_of(buf)[0])).wait()
            block = block_of(chunk_z[k], 0, 0)
            arrived(held.at[buf, pl.ds(block, 2)], core_sem(parts_of(buf)[0], block))

        def first_row(layer):
            return REACH * layer

        def from_row(start):
            return pl.ds(start, total - start)

        def gain_of(layer, start, width):
            at = pl.multiple_of(t * feats + start, lanes)
            return gain_ref[pl.ds(layer, 1), pl.ds(at, width)]

        def pack_squares(g, layer):
            for k in range(sq_tiles):
                block = part_sq[g, pl.ds(k * lanes, lanes)].T
                value = jnp.sum(block, axis=0, keepdims=True)
                sq_send[layer, g, k] = jnp.broadcast_to(value, (8, lanes))
            send(
                sq_send.at[layer, g], sq_recv.at[layer, g],
                a_send.at[layer, g, 1], a_recv.at[layer, g, n_z], x_mate,
            )

        def halved(layer, g):
            return layer == last and g == 1

        def mix_slot(layer, g):
            return 0 if g == 0 else 1 + layer

        def take_edge(g):
            arrived(edge.at[g], e_recv.at[g])
            keep = ((s_in if g == 0 else s_end) > 0).astype(jnp.float32)

            @pl.loop(0, halo // REACH)
            def _(i):
                at = pl.ds(i * REACH, REACH)
                state[g, at] = (edge[g, at].astype(jnp.float32) * keep).astype(jnp.bfloat16)

        def own_state():
            @pl.loop(0, rows // REACH)
            def _(i):
                state[0, pl.ds(halo + i * REACH, REACH)] = x_ref[pl.ds(i * REACH, REACH)]

        def take_state(k):
            arrived(state.at[1, pl.ds(halo + k * state_rows, state_rows)], s_recv.at[k])

        def squares(g, start, stop):
            @pl.loop(start // REACH, stop // REACH)
            def _(i):
                at = pl.ds(i * REACH, REACH)
                sums = jnp.zeros((REACH, lanes), jnp.float32)
                for j in range(feats // lanes):
                    cols = pl.ds(j * lanes, lanes)
                    wide = state[g, at, cols].astype(jnp.float32)
                    sums = sums + wide * wide
                    xg[g, at, cols] = (wide * gain_of(0, j * lanes, lanes)).astype(jnp.bfloat16)
                part_sq[g, at] = sums

        def project(layer, g, k):
            at = from_row(first_row(layer))
            zz = chunk_z[k]
            weight = held[2 * layer, pl.ds(zz * 4, 4)].reshape(chunk, feats)
            value = lax.dot_general(
                xg[g, at], weight, (((1,), (1,)), ((), ())),
                preferred_element_type=jnp.float32,
            )
            p_send[layer, g, zz, at] = value.astype(jnp.bfloat16)
            send(
                p_send.at[layer, g, zz, at], p_recv.at[layer, g, zz, at],
                a_send.at[layer, g, 0], a_recv.at[layer, g, zz], x_mate,
                (zz // 2 != t) if halved(layer, g) else None,
            )

        def inverse(layer, g):
            arrived(sq_recv.at[layer, g], a_recv.at[layer, g, n_z])
            for k in range(sq_tiles):
                mean = (sq_send[layer, g, k] + sq_recv[layer, g, k]) / (2 * feats)
                inv = lax.rsqrt(mean + EPS)
                inv_col[g, pl.ds(k * lanes, lanes)] = jnp.broadcast_to(inv[0:1], (lanes, lanes)).T

        def pool(layer, g, k):
            pool_plane(layer, g, chunk_z[k])

        def pool_half(j):
            pool_plane(last, 1, 2 * t + j)
            ship_mix(last, j)

        def ship_mix(layer, j):
            zz = 2 * t + j
            send(
                mix.at[mix_slot(layer, 1), zz, pl.ds(halo, rows)], mix_in.at[layer, zz],
                m_send.at[layer], m_recv.at[layer, zz], outer,
            )

        def ship_mixes(layer):
            for j in range(2):
                ship_mix(layer, j)

        def pool_plane(layer, g, group):
            start = first_row(layer)
            at = from_row(start)
            arrived(p_recv.at[layer, g, group, at], a_recv.at[layer, g, group])
            row = lax.broadcasted_iota(jnp.int32, (total - start, lanes), 0)
            position = (s_in if g == 0 else s_end) * rows - halo + start + row
            span = jnp.left_shift(jnp.int32(2), group)
            divisor = jnp.maximum(jnp.minimum(position + 1, span), 1).astype(jnp.float32)
            share = 1.0 / divisor
            inv = inv_col[g, at]
            for j in range(chunk // lanes):
                cols = pl.ds(j * lanes, lanes)
                joined = p_send[layer, g, group, at, cols].astype(jnp.float32)
                joined = joined + p_recv[layer, g, group, at, cols].astype(jnp.float32)
                base = (joined * inv).astype(jnp.bfloat16).astype(jnp.float32)
                running = base
                width = 1
                picked = None
                for step in range(GROUPS):
                    running = running + pltpu.roll(running, width, 0)
                    width *= 2
                    picked = running if picked is None else jnp.where(group >= step, running, picked)
                lane = pl.multiple_of(group * chunk + j * lanes, lanes)
                scale = scale_ref[pl.ds(layer, 1), pl.ds(lane, lanes)]
                mix[mix_slot(layer, g), group, at, cols] = ((picked * share - base) * scale).astype(jnp.bfloat16)

        def expand(layer, g, begin, end):
            width = 256
            at = from_row(first_row(layer + 1))
            buf = 2 * layer + 1
            if layer < last and begin == 0:
                part_sq[g] = jnp.zeros(part_sq.shape[1:], jnp.float32)

            @pl.loop(begin * quarter // width, end * quarter // width)
            def _(n):
                col = pl.multiple_of(n * width, width)
                cols = pl.ds(col, width)
                mixed = jnp.concatenate([mix[mix_slot(layer, g), c, at] for c in range(n_z)], axis=1)
                weight = held[buf, :, :, cols].reshape(pools, width)
                branch = jnp.dot(mixed, weight, preferred_element_type=jnp.float32)
                new = (state[g, at, cols].astype(jnp.float32) + branch).astype(jnp.bfloat16)
                if layer == last:
                    o_ref[:, cols] = new
                else:
                    state[g, at, cols] = new
                    wide = new.astype(jnp.float32)
                    xg[g, at, cols] = (wide * gain_of(layer + 1, col, width)).astype(jnp.bfloat16)
                    square = wide * wide
                    sums = square[:, :lanes]
                    for j in range(1, width // lanes):
                        sums = sums + square[:, j * lanes:(j + 1) * lanes]
                    part_sq[g, at] = part_sq[g, at] + sums

            if layer < last and end == 4:
                pack_squares(g, layer + 1)

        def prepare():
            for g in range(2):
                part_sq[g] = jnp.zeros(part_sq.shape[1:], jnp.float32)
            own_state()

        def first_squares(g):
            take_edge(g)
            squares(g, 0, total if g == 0 else halo)
            pack_squares(g, 0)

        def shipped_squares(k):
            take_state(k)
            squares(1, halo + k * state_rows, halo + (k + 1) * state_rows)

        run({
            "issue": issue, "E": take_end, "O": take_over, "M": take_mate, "F": take_far,
            "EM": take_mate_end, "OM": take_mate_over, "FM": take_mate_far,
            "plane": plane, "all": gathered, "bplane": gathered_piece, "edge": send_edge, "init": prepare, "sq": first_squares,
            "st": shipped_squares, "P": project, "Q": pool, "inv": inverse, "H": pool_half,
            "mx": ship_mixes, "X": expand,
        }, INNER_ORDER)
        with jax.named_scope("drain"):
            drain_weights()
            departed(x_ref.at[pl.ds(0, halo)], e_send.at[0])
            for layer in range(layers):
                departed(mix_in.at[layer, pl.ds(2 * t, 2)], m_send.at[layer])
                at = from_row(first_row(layer))
                for g in range(2):
                    departed(sq_send.at[layer, g], a_send.at[layer, g, 1])
                    zz = pl.ds(2 * (1 - t), 2) if halved(layer, g) else pl.ds(0, n_z)
                    departed(p_send.at[layer, g, zz, at], a_send.at[layer, g, 0])

    pl.when(is_end)(end_program)
    pl.when(jnp.logical_not(is_end))(inner_program)


def fused_body(inputs, norm_gain, in_weight, pool_scale, out_weight):
    rows, feats = inputs.shape
    layers = norm_gain.shape[0]
    pools = pool_scale.shape[1]
    blocks = lax.axis_size("sp")
    n_z = blocks // 4
    depth = out_weight.shape[1]
    halo = REACH * layers
    total = rows + halo
    sq_tiles = -(-total // 128)
    chunk = pools // n_z
    phases = len(phase_table(feats))
    state_chunks = len([row for row in END_ORDER if row[0] == "st"])
    bf, f32 = jnp.bfloat16, jnp.float32
    vmem = pl.BlockSpec(memory_space=pltpu.VMEM)
    dma = pltpu.SemaphoreType.DMA
    return pl.pallas_call(
        functools.partial(kernel, n_z, layers, halo),
        out_shape=jax.ShapeDtypeStruct((rows, feats), bf),
        in_specs=[vmem] * 5,
        out_specs=vmem,
        scratch_shapes=[
            pltpu.VMEM((2 * layers, blocks, depth, feats), bf),
            pltpu.VMEM((2, total, feats), bf),
            pltpu.VMEM((2, total, feats), bf),
            pltpu.VMEM((2, halo, feats), bf),
            pltpu.VMEM((layers, 2, n_z, total, chunk), bf),
            pltpu.VMEM((layers, 2, n_z, total, chunk), bf),
            pltpu.VMEM((1 + layers, n_z, total, chunk), bf),
            pltpu.VMEM((layers, n_z, rows, chunk), bf),
            pltpu.VMEM((2, sq_tiles * 128, 128), f32),
            pltpu.VMEM((2, sq_tiles * 128, 128), f32),
            pltpu.VMEM((layers, 2, sq_tiles, 8, 128), f32),
            pltpu.VMEM((layers, 2, sq_tiles, 8, 128), f32),
            dma((2 * layers, 2)),
            dma((phases, 8)),
            dma((layers * n_z + layers - 1 + PIECES[-1],)),
            dma((2 * layers - 1 + PIECES[-1],)),
            dma((1,)),
            dma((2,)),
            dma((1,)),
            dma((state_chunks,)),
            dma((layers, 2, 2)),
            dma((layers, 2, n_z + 1)),
            dma((layers,)),
            dma((layers, n_z)),
        ],
        compiler_params=pltpu.CompilerParams(
            collective_id=0, has_side_effects=True, vmem_limit_bytes=60 * 1024 * 1024
        ),
    )(inputs, norm_gain, jnp.swapaxes(in_weight, 1, 2), pool_scale, out_weight)


def solution(mesh):
    n_sp, n_tp = mesh.shape["sp"], mesh.shape["tp"]
    fused = n_tp == 2 and n_sp == 16
    placed = (P("sp", "tp"), P(), P(None, "tp", "sp"), P(), P(None, "sp", "tp"))
    return jax.shard_map(
        fused_body if fused else plain_body,
        mesh=mesh, in_specs=placed, out_specs=P("sp", "tp"), check_vma=False,
    )
```

```python
import functools

import jax
import jax.numpy as jnp
from jax import lax
from jax.experimental import pallas as pl
from jax.experimental.pallas import tpu as pltpu
from jax.sharding import PartitionSpec as P

EPS = 1e-06
REACH = 16
GROUPS = 4
MESH_ID = pl.DeviceIdType.MESH


def shift_sp(value):
    count = lax.axis_size("sp")
    return lax.ppermute(value, "sp", [(i, i + 1) for i in range(count - 1)])


def window_means(extended, row_count, first_channel, first_pos, pool_total):
    width = extended.shape[1]
    channel = first_channel + lax.broadcasted_iota(jnp.int32, (1, width), 1)
    window_len = jnp.left_shift(jnp.int32(2), channel // (pool_total // GROUPS))
    running = jnp.zeros((row_count, width), jnp.float32)
    for offset in range(REACH):
        shifted = extended[REACH - offset : REACH - offset + row_count]
        running = running + jnp.where(offset < window_len, shifted, 0.0)
    position = first_pos + lax.broadcasted_iota(jnp.int32, (row_count, 1), 0)
    divisor = jnp.minimum(position + 1, window_len).astype(jnp.float32)
    return running / divisor - extended[REACH:]


def plain_body(inputs, norm_gain, in_weight, pool_scale, out_weight):
    rows, feats = inputs.shape
    layers, features = norm_gain.shape
    pools = pool_scale.shape[1]
    part = pools // lax.axis_size("tp")
    t = lax.axis_index("tp")
    s = lax.axis_index("sp")
    current = inputs
    for layer in range(layers):
        in_all = lax.all_gather(in_weight[layer], "sp", axis=1, tiled=True)
        out_all = lax.all_gather(out_weight[layer], "sp", axis=0, tiled=True)
        wide = current.astype(jnp.float32)
        squares = lax.psum(jnp.sum(wide * wide, axis=1), "tp")
        inv_rms = lax.rsqrt(squares / features + EPS)[:, None]
        gain = lax.dynamic_slice_in_dim(norm_gain[layer], t * feats, feats)
        normed = (wide * inv_rms * gain).astype(jnp.bfloat16)
        partial = jnp.dot(normed, in_all, preferred_element_type=jnp.float32)
        pool_in = lax.psum_scatter(
            partial.astype(jnp.bfloat16), "tp", scatter_dimension=1, tiled=True
        )
        edge = shift_sp(pool_in[rows - REACH :])
        extended = jnp.concatenate([edge, pool_in], 0).astype(jnp.float32)
        means = window_means(extended, rows, t * part, s * rows, pools)
        scale = lax.dynamic_slice_in_dim(pool_scale[layer], t * part, part)
        mixed = (means * scale).astype(jnp.bfloat16)
        pooled = lax.all_gather(mixed, "tp", axis=1, tiled=True)
        branch = jnp.dot(pooled, out_all, preferred_element_type=jnp.float32)
        current = (current.astype(jnp.float32) + branch).astype(jnp.bfloat16)
    return current


E, O, M, F, EM, OM1, OM2, FM = range(8)
PIECES = (2, 2, 2, 4, 2, 4)
EDGE_BY_MATE = (True, True, False, False, False, False)
OVER_BY_MATE = (0.5, 0.0, 0.5, 0.5, 0.5, 0.5)
INNER_ORDER = [
    ("init",), ("iy", 0), ("edge",), ("iy", 1), ("im", 0), ("im", 1), ("M", 0), ("E", 0), ("O", 0), ("sq", 0),
    ("M", 1), ("O", 1), ("sqa",), ("E", 1), ("inv", 0, 0), ("EM", 0), ("OM", 0), ("F", 0), ("E", 2), ("ic", 0),
    ("ic", 1), ("ic", 2), ("OM", 1), ("im", 2), ("plane", 0, 0), ("P", 0, 0, 0), ("plane", 0, 2), ("P", 0, 0, 2),
    ("E", 3), ("EM", 1), ("F", 1), ("plane", 0, 1), ("P", 0, 0, 1), ("FM", 0), ("F", 2), ("Q", 0, 0, 0), ("st", 0),
    ("im", 3), ("EM", 2), ("O", 2), ("im", 4), ("im", 5), ("iy", 2), ("iy", 3), ("iy", 4), ("iy", 5), ("ic", 3),
    ("ic", 4), ("ic", 5), ("Q", 0, 0, 2), ("EM", 3), ("F", 3), ("im", 6), ("im", 7), ("st", 1), ("PA", 0), ("FM", 1),
    ("PA", 2), ("O", 3), ("PA", 1), ("plane", 0, 3), ("PA", 3), ("P", 0, 0, 3), ("FM", 2), ("O", 4), ("Q", 0, 0, 1),
    ("st", 2), ("M", 2), ("O", 5), ("O", 6), ("ic", 6), ("ic", 7), ("ic", 8), ("ic", 9), ("ic", 10), ("ic", 11),
    ("ic", 12), ("ic", 13), ("ic", 14), ("M", 3), ("O", 7), ("st", 3), ("sq", 1), ("PB", 3), ("ic", 15), ("OM", 2),
    ("M", 4), ("PB", 2), ("iy", 6), ("iy", 7), ("iy", 8), ("iy", 9), ("iy", 10), ("PB", 0), ("PB", 1),
    ("Q", 0, 0, 3), ("inv", 0, 1), ("M", 5), ("OM", 3), ("Q", 0, 1, 3), ("E", 4), ("plane", 2, 0), ("Q", 0, 1, 2),
    ("FM", 3), ("Q", 0, 1, 0), ("E", 5), ("all", 1), ("X", 0, 0, 0, 1), ("OM", 4), ("X", 0, 0, 1, 2), ("E", 6),
    ("X", 0, 0, 2, 3), ("F", 4), ("OM", 5), ("Q", 0, 1, 1), ("X", 0, 0, 3, 4), ("E", 7), ("P", 1, 0, 0), ("E", 8),
    ("plane", 2, 2), ("P", 1, 0, 2), ("M", 6), ("mx", 0), ("X", 0, 1, 0, 1), ("E", 9), ("F", 5), ("X", 0, 1, 1, 2),
    ("iy", 11), ("F", 6), ("M", 7), ("im", 8), ("im", 9), ("im", 10), ("im", 11), ("inv", 1, 0), ("X", 0, 1, 2, 3),
    ("M", 8), ("X", 0, 1, 3, 4), ("F", 7), ("P", 1, 1, 2), ("M", 9), ("E", 10), ("P", 1, 1, 0), ("F", 8),
    ("Q", 1, 0, 0), ("OM", 6), ("E", 11), ("F", 9), ("M", 10), ("OM", 7), ("Q", 1, 0, 2), ("inv", 1, 1), ("O", 8),
    ("EM", 4), ("FM", 4), ("O", 9), ("Q", 1, 1, 2), ("EM", 5), ("FM", 5), ("O", 10), ("plane", 2, 1), ("P", 1, 1, 1),
    ("E", 12), ("plane", 2, 3), ("P", 1, 1, 3), ("EM", 6), ("P", 1, 0, 3), ("M", 11), ("O", 11), ("P", 1, 0, 1),
    ("FM", 6), ("E", 13), ("Q", 1, 1, 0), ("plane", 4, 0), ("EM", 7), ("FM", 7), ("im", 12), ("im", 13), ("im", 14),
    ("im", 15), ("EM", 8), ("Q", 1, 1, 1), ("FM", 8), ("F", 10), ("EM", 9), ("FM", 9), ("OM", 8), ("OM", 9),
    ("Q", 1, 1, 3), ("mx", 1), ("F", 11), ("EM", 10), ("all", 3), ("X", 1, 1, 0, 2), ("OM", 10), ("X", 1, 1, 2, 4),
    ("F", 12), ("EM", 11), ("Q", 1, 0, 3), ("P", 2, 1, 0), ("OM", 11), ("EM", 12), ("plane", 4, 1), ("P", 2, 1, 1),
    ("F", 13), ("FM", 10), ("plane", 4, 2), ("P", 2, 1, 2), ("EM", 13), ("iy", 12), ("iy", 13), ("iy", 14),
    ("iy", 15), ("Q", 1, 0, 1), ("X", 1, 0, 0, 1), ("O", 12), ("inv", 2, 1), ("FM", 11), ("X", 1, 0, 1, 2),
    ("O", 13), ("X", 1, 0, 2, 3), ("FM", 12), ("plane", 4, 3), ("P", 2, 1, 3), ("O", 14), ("X", 1, 0, 3, 4),
    ("FM", 13), ("P", 2, 0, 2), ("O", 15), ("P", 2, 0, 3), ("M", 12), ("P", 2, 0, 1), ("inv", 2, 0), ("H", 0),
    ("M", 13), ("E", 14), ("P", 2, 0, 0), ("M", 14), ("EM", 14), ("H", 1), ("M", 15), ("E", 15), ("OM", 12),
    ("F", 14), ("OM", 13), ("EM", 15), ("Q", 2, 0, 2), ("bplane", 12), ("OM", 14), ("bplane", 13), ("OM", 15),
    ("F", 15), ("FM", 14), ("Q", 2, 0, 3), ("bplane", 14), ("FM", 15), ("Q", 2, 0, 1), ("bplane", 15),
    ("Q", 2, 0, 0), ("X", 2, 0, 0, 4),
]
END_ORDER = [
    ("edge", 0), ("ey", 0), ("eown", 0), ("eM", 0), ("edge", 1), ("ey", 1), ("eown", 1), ("eM", 1), ("ey", 2),
    ("ey", 3), ("eown", 2), ("eM", 2), ("eown", 3), ("eM", 3), ("st", 0), ("st", 1), ("st", 2), ("st", 3), ("eI", 2),
    ("eIM", 2), ("eF", 2), ("eO", 2), ("eFM", 2), ("eI", 3), ("eOM", 2), ("eF", 3), ("eIM", 3), ("eO", 3),
    ("eFM", 3), ("ey", 4), ("ey", 5), ("eown", 4), ("eown", 5), ("eOM", 3), ("ey", 6), ("eI", 6), ("eO", 6),
    ("ey", 7), ("ey", 8), ("eown", 6), ("eI", 7), ("eown", 7), ("ey", 9), ("ey", 10), ("ey", 11), ("ey", 12),
    ("eown", 8), ("eown", 9), ("eown", 10), ("eown", 11), ("ey", 13), ("ey", 14), ("ey", 15), ("eI", 8), ("eM", 4),
    ("eI", 9), ("eI", 12), ("eM", 5), ("eown", 12), ("eI", 13), ("eM", 6), ("eI", 14), ("eown", 13), ("eIM", 6),
    ("eO", 7), ("eOM", 6), ("eI", 15), ("eM", 7), ("eM", 8), ("eIM", 7), ("emx", 0, 0), ("eM", 9), ("emx", 0, 1),
    ("eM", 10), ("eF", 6), ("emy", 0, 0), ("eF", 7), ("eM", 11), ("eF", 8), ("eM", 12), ("emy", 0, 1), ("eall", 1),
    ("eX", 0, 0, 2), ("eM", 13), ("eF", 9), ("eX", 0, 2, 4), ("eO", 8), ("eO", 9), ("eIM", 8), ("eIM", 9),
    ("eIM", 12), ("eIM", 13), ("eIM", 14), ("eOM", 7), ("eIM", 15), ("emx", 1, 0), ("eFM", 6), ("eFM", 7),
    ("emx", 1, 1), ("eFM", 8), ("eF", 12), ("eFM", 9), ("emy", 1, 0), ("eown", 14), ("eM", 14), ("eown", 15),
    ("eF", 13), ("eM", 15), ("eOM", 8), ("eO", 12), ("eOM", 9), ("emy", 1, 1), ("eO", 13), ("eall", 3),
    ("eX", 1, 0, 1), ("eFM", 12), ("eX", 1, 1, 3), ("eFM", 13), ("eO", 14), ("eX", 1, 3, 4), ("eO", 15), ("eOM", 12),
    ("epl", 12), ("eOM", 13), ("emx", 2, 0), ("epl", 13), ("eOM", 14), ("eOM", 15), ("emx", 2, 1), ("eF", 14),
    ("emy", 2, 0), ("eF", 15), ("emy", 2, 1), ("eX", 2, 0, 1), ("eFM", 14), ("eX", 2, 1, 2), ("eFM", 15),
    ("epl", 14), ("eX", 2, 2, 3), ("epl", 15), ("eX", 2, 3, 4),
]


def phase_table(feats):
    table = []
    for buf, count in enumerate(PIECES):
        width = feats // count
        table += [(buf, k * width, width) for k in range(count)]
    return table


def kernel(
    n_z, layers, halo,
    x_hbm, gain_ref, wi_hbm, scale_ref, wo_hbm, o_ref,
    x_ref, wi_ref, wo_ref, held, state, xg, edge, p_send, p_recv, mix, mix_in, part_sq, inv_col, sq_send, sq_recv,
    w_send, w_recv, c_recv, local_sem, load_sem, e_send, e_recv, s_send, s_recv, a_send, a_recv, m_send, m_recv,
):
    loads = [
        pltpu.make_async_copy(src, dst, load_sem.at[i])
        for i, (src, dst) in enumerate([(wi_hbm, wi_ref), (x_hbm, x_ref), (wo_hbm, wo_ref)])
    ]
    for load in loads:
        load.start()
    rows, feats = x_ref.shape
    total = rows + halo
    blocks, depth = held.shape[1], held.shape[2]
    pools = scale_ref.shape[1]
    chunk = pools // n_z
    last = layers - 1
    table = phase_table(feats)
    phases = len(table)
    lanes = 128
    quarter = feats // 4
    state_chunks = s_recv.shape[0]
    last_buf = len(PIECES) - 1
    sq_tiles = part_sq.shape[1] // lanes
    s = lax.axis_index("sp")
    t = lax.axis_index("tp")
    core = s % 2
    y = (s // 2) % 2
    z = s // 4
    side = z // 2

    def block_of(zz, yy, cc):
        return zz * 4 + yy * 2 + cc

    z_in, z_end = 1 + side, 3 * side
    z_over, z_far = 2 - side, 3 - 3 * side
    is_end = z == z_end
    s_end, s_in = block_of(z_end, y, core), block_of(z_in, y, core)

    y_mate = (block_of(z, 1 - y, core), t)
    c_mate = (block_of(z, y, 1 - core), t)
    x_mate = (s, 1 - t)
    opposite = (block_of(z_over, y, core), t)
    inner = (s_in, t)
    outer = (s_end, t)
    after = (s + 1) % blocks
    after_z = after // 4
    after_holder = (block_of(1 + after_z // 2, (after // 2) % 2, after % 2), t)
    after_slot = jnp.where((after_z == 0) | (after_z == n_z - 1), 1, 0)
    before = [((s_in + blocks - 1) % blocks, t), ((s_end + blocks - 1) % blocks, t)]

    barrier = pltpu.get_barrier_semaphore()

    def greet(peers):
        for peer in peers:
            pl.semaphore_signal(barrier, inc=1, device_id=peer, device_id_type=MESH_ID)

    def send(src, dst, send_sem, recv_sem, to, when=None):
        copy = pltpu.make_async_remote_copy(
            src_ref=src, dst_ref=dst, send_sem=send_sem, recv_sem=recv_sem,
            device_id=to, device_id_type=MESH_ID,
        )
        if when is None:
            copy.start()
        else:
            pl.when(when)(copy.start)

    def departed(ref, sem):
        pltpu.make_async_remote_copy(
            src_ref=ref, dst_ref=ref, send_sem=sem, recv_sem=sem,
            device_id=c_mate, device_id_type=MESH_ID,
        ).wait_send()

    def arrived(ref, sem):
        pltpu.make_async_remote_copy(
            src_ref=ref, dst_ref=ref, send_sem=sem, recv_sem=sem,
            device_id=c_mate, device_id_type=MESH_ID,
        ).wait_recv()

    whole, first, second = pl.ds(0, depth), pl.ds(0, depth // 2), pl.ds(depth // 2, depth // 2)
    volume = {}

    def own(ph):
        buf, start, width = table[ph]
        return (wi_ref if buf % 2 == 0 else wo_ref).at[buf // 2, :, pl.ds(start, width)]

    def slot(ph, block, piece=whole):
        buf, start, width = table[ph]
        return held.at[buf, block, piece, pl.ds(start, width)]

    def send_sem(ph, port, piece):
        buf, _, width = table[ph]
        kind = 1 if port == EM else 0
        share = width * (1 if piece is whole else 0.5) / feats
        volume[buf, kind] = volume.get((buf, kind), 0) + share
        return w_send.at[buf, kind]

    def core_sem(ph, block):
        buf, start, width = table[ph]
        layer = buf // 2
        if buf % 2 == 0:
            return c_recv.at[layer * n_z + block // 4]
        return c_recv.at[layers * n_z + layer + (start // width if buf == last_buf else 0)]

    def send_own(ph, to, port):
        sem = core_sem(ph, s) if port is None else w_recv.at[ph, port]
        send(own(ph), slot(ph, s), send_sem(ph, port, whole), sem, to)

    def forward(ph, block, to, port, piece=whole):
        ref = slot(ph, block, piece)
        sem = core_sem(ph, block) if port is None else w_recv.at[ph, port]
        send(ref, ref, send_sem(ph, port, piece), sem, to)

    def wait_block(ph, block, port, piece=whole):
        arrived(slot(ph, block, piece), w_recv.at[ph, port])

    def drain_weights():
        for (buf, kind), blocks_sent in volume.items():
            assert blocks_sent == int(blocks_sent)
            departed(held.at[buf, pl.ds(0, int(blocks_sent))], w_send.at[buf, kind])
        volume.clear()

    state_rows = rows // state_chunks
    split_row = halo + rows // 2
    def parts_of(buf):
        return [ph for ph in range(phases) if table[ph][0] == buf]

    def is_out(ph):
        return table[ph][0] % 2 == 1

    def local_of(ph):
        buf, start, width = table[ph]
        return local_sem.at[buf + (start // width if buf == last_buf else 0)]

    def keep_own(ph):
        pltpu.make_async_copy(own(ph), slot(ph, s), local_of(ph)).start()

    def gathered(buf):
        ph = parts_of(buf)[0]
        weight = (wi_ref if buf % 2 == 0 else wo_ref).at[buf // 2]
        pltpu.make_async_copy(weight, held.at[buf, s], local_of(ph)).wait()
        arrived(held.at[buf, pl.ds(0, blocks // 2)], core_sem(ph, s))

    def gathered_piece(ph):
        buf, start, width = table[ph]
        pltpu.make_async_copy(own(ph), slot(ph, s), local_of(ph)).wait()
        arrived(held.at[buf, pl.ds(0, blocks // 2), :, pl.ds(start, width)], core_sem(ph, s))

    def half_plane(which, j):
        near = jnp.where(side == 0, z_in - j, z_in + j)
        far = jnp.where(side == 0, z_over + j, z_over - j)
        return jnp.where(which == side, near, far)

    def send_edge(when=None):
        send(
            x_ref.at[pl.ds(rows - halo, halo)], edge.at[after_slot],
            e_send.at[0], e_recv.at[after_slot], after_holder, when,
        )

    def send_some_edges(which):
        send_edge(after_slot == which)

    def run(table_of_steps, order):
        for name, *args in order:
            with jax.named_scope("_".join([name] + [str(a) for a in args])):
                table_of_steps[name](*args)

    def end_program():
        greet([inner, y_mate, c_mate, x_mate])
        pl.semaphore_wait(barrier, 5)
        for load in loads:
            load.wait()
        mate = block_of(z_end, 1 - y, core)
        columns = [z_in, z_over, z_far]

        def own_aside(ph):
            if is_out(ph) or not EDGE_BY_MATE[table[ph][0]]:
                send_own(ph, y_mate, M)
            if is_out(ph):
                send_own(ph, c_mate, None)
                keep_own(ph)

        def own_inward(ph):
            send_own(ph, inner, E)

        def mate_inward(ph):
            direct = not EDGE_BY_MATE[table[ph][0]]
            if is_out(ph) or direct:
                wait_block(ph, mate, M)
            if direct:
                forward(ph, mate, inner, EM)
            if is_out(ph):
                forward(ph, mate, c_mate, None)

        def ship_state(k):
            at = pl.ds(k * state_rows, state_rows)
            send(
                x_ref.at[at], state.at[1, pl.ds(halo + k * state_rows, state_rows)],
                s_send.at[0], s_recv.at[k], inner,
            )

        def take_column(which, ph):
            block = block_of(columns[which], y, core)
            wait_block(ph, block, (E, O, F)[which])
            forward(ph, block, y_mate, (EM, OM1, FM)[which])
            forward(ph, block, c_mate, None)

        def take_mate_column(which, ph):
            block = block_of(columns[which], 1 - y, core)
            wait_block(ph, block, (EM, OM1, FM)[which])
            forward(ph, block, c_mate, None)

        def take_mix(layer, j):
            zz = half_plane(t, j)
            ref, sem = mix_in.at[layer, zz], m_recv.at[layer, zz]
            arrived(ref, sem)
            send(ref, ref, m_send.at[layer], sem, x_mate)

        def take_mate_mix(layer, j):
            zz = half_plane(1 - t, j)
            arrived(mix_in.at[layer, zz], m_recv.at[layer, zz])

        def end_expand(layer, begin, end):
            width = 256
            at = pl.ds(halo, rows)

            @pl.loop(begin * quarter // width, end * quarter // width)
            def _(n):
                cols = pl.ds(pl.multiple_of(n * width, width), width)
                mixed = jnp.concatenate([mix_in[layer, c] for c in range(n_z)], axis=1)
                weight = held[2 * layer + 1, :, :, cols].reshape(pools, width)
                branch = jnp.dot(mixed, weight, preferred_element_type=jnp.float32)
                old = x_ref[:, cols] if layer == 0 else state[1, at, cols]
                new = (old.astype(jnp.float32) + branch).astype(jnp.bfloat16)
                if layer == last:
                    o_ref[:, cols] = new
                else:
                    state[1, at, cols] = new

        part = functools.partial
        run({
            "ey": own_aside, "eown": own_inward, "eM": mate_inward, "st": ship_state,
            "eI": part(take_column, 0), "eO": part(take_column, 1), "eF": part(take_column, 2),
            "eIM": part(take_mate_column, 0), "eOM": part(take_mate_column, 1),
            "eFM": part(take_mate_column, 2), "eall": gathered, "epl": gathered_piece,
            "edge": send_some_edges,
            "emx": take_mix, "emy": take_mate_mix, "eX": end_expand,
        }, END_ORDER)
        with jax.named_scope("drain"):
            drain_weights()
            departed(x_ref, s_send.at[0])
            departed(x_ref.at[pl.ds(0, halo)], e_send.at[0])
            for layer in range(layers):
                departed(mix_in.at[layer, pl.ds(2 * t, 2)], m_send.at[layer])

    def inner_program():
        with jax.named_scope("greet"):
            greet([opposite, y_mate, c_mate, x_mate, outer] + before)
        with jax.named_scope("barrier"):
            pl.semaphore_wait(barrier, 6)
        for load in loads:
            load.wait()
        chunk_z = [z_in, z_end, z_over, z_far]

        def own_across(ph):
            send_own(ph, opposite, O)

        def own_to_mate(ph):
            send_own(ph, y_mate, M)

        def own_near(ph):
            send_own(ph, c_mate, None)
            if is_out(ph):
                send_own(ph, outer, E)
            keep_own(ph)

        def over_pieces(ph):
            share = OVER_BY_MATE[table[ph][0]]
            by_mate = None if share == 0 else whole if share == 1 else first
            direct = None if share == 1 else whole if share == 0 else second
            return by_mate, direct

        def take_end(ph):
            block = block_of(z_end, y, core)
            wait_block(ph, block, E)
            forward(ph, block, opposite, F)
            if EDGE_BY_MATE[table[ph][0]]:
                forward(ph, block, y_mate, EM)
            forward(ph, block, c_mate, None)

        def take_over(ph):
            block = block_of(z_over, y, core)
            wait_block(ph, block, O)
            by_mate, _ = over_pieces(ph)
            if by_mate is not None:
                forward(ph, block, y_mate, OM1, by_mate)
            forward(ph, block, c_mate, None)
            if is_out(ph):
                forward(ph, block, outer, O)

        def take_mate(ph):
            block = block_of(z_in, 1 - y, core)
            wait_block(ph, block, M)
            _, direct = over_pieces(ph)
            if direct is not None:
                forward(ph, block, opposite, OM2, direct)
            forward(ph, block, c_mate, None)

        def take_far(ph):
            block = block_of(z_far, y, core)
            wait_block(ph, block, F)
            forward(ph, block, y_mate, FM)
            forward(ph, block, c_mate, None)
            if is_out(ph):
                forward(ph, block, outer, F)

        def take_mate_end(ph):
            block = block_of(z_end, 1 - y, core)
            wait_block(ph, block, EM)
            forward(ph, block, c_mate, None)

        def take_mate_over(ph):
            block = block_of(z_over, 1 - y, core)
            by_mate, direct = over_pieces(ph)
            if by_mate is not None:
                wait_block(ph, block, OM1, by_mate)
            if direct is not None:
                wait_block(ph, block, OM2, direct)
            forward(ph, block, c_mate, None)

        def take_mate_far(ph):
            block = block_of(z_far, 1 - y, core)
            wait_block(ph, block, FM)
            forward(ph, block, c_mate, None)

        def plane(buf, k):
            if k == 0:
                weight = wi_ref.at[buf // 2]
                pltpu.make_async_copy(weight, held.at[buf, s], local_of(parts_of(buf)[0])).wait()
            block = block_of(chunk_z[k], 0, 0)
            arrived(held.at[buf, pl.ds(block, 2)], core_sem(parts_of(buf)[0], block))

        def first_row(layer):
            return REACH * layer

        def from_row(start):
            return pl.ds(start, total - start)

        def gain_of(layer, start, width):
            at = pl.multiple_of(t * feats + start, lanes)
            return gain_ref[pl.ds(layer, 1), pl.ds(at, width)]

        def pack_squares(g, layer):
            for k in range(sq_tiles):
                block = part_sq[g, pl.ds(k * lanes, lanes)].T
                value = jnp.sum(block, axis=0, keepdims=True)
                sq_send[layer, g, k] = jnp.broadcast_to(value, (8, lanes))
            send(
                sq_send.at[layer, g], sq_recv.at[layer, g],
                a_send.at[layer, g, 1], a_recv.at[layer, g, n_z], x_mate,
            )

        def halved(layer, g):
            return layer == last and g == 1

        def mix_slot(layer, g):
            return 0 if g == 0 else 1 + layer

        def take_edge(g):
            arrived(edge.at[g], e_recv.at[g])
            keep = ((s_in if g == 0 else s_end) > 0).astype(jnp.float32)

            @pl.loop(0, halo // REACH)
            def _(i):
                at = pl.ds(i * REACH, REACH)
                state[g, at] = (edge[g, at].astype(jnp.float32) * keep).astype(jnp.bfloat16)

        def own_state():
            @pl.loop(0, rows // REACH)
            def _(i):
                state[0, pl.ds(halo + i * REACH, REACH)] = x_ref[pl.ds(i * REACH, REACH)]

        def take_state(k):
            arrived(state.at[1, pl.ds(halo + k * state_rows, state_rows)], s_recv.at[k])

        def squares(g, start, stop):
            @pl.loop(start // REACH, stop // REACH)
            def _(i):
                at = pl.ds(i * REACH, REACH)
                sums = jnp.zeros((REACH, lanes), jnp.float32)
                for j in range(feats // lanes):
                    cols = pl.ds(j * lanes, lanes)
                    wide = state[g, at, cols].astype(jnp.float32)
                    sums = sums + wide * wide
                    xg[g, at, cols] = (wide * gain_of(0, j * lanes, lanes)).astype(jnp.bfloat16)
                part_sq[g, at] = sums

        def project(layer, g, k):
            project_rows(layer, g, k, first_row(layer), total, chunk_z[k])

        def project_early(k):
            project_rows(0, 1, k, 0, split_row, n_z + 1 + chunk_z[k])

        def project_late(k):
            project_rows(0, 1, k, split_row, total, chunk_z[k])

        def project_rows(layer, g, k, start, stop, sem):
            at = pl.ds(start, stop - start)
            zz = chunk_z[k]
            weight = held[2 * layer, pl.ds(zz * 4, 4)].reshape(chunk, feats)
            value = lax.dot_general(
                xg[g, at], weight, (((1,), (1,)), ((), ())),
                preferred_element_type=jnp.float32,
            )
            p_send[layer, g, zz, at] = value.astype(jnp.bfloat16)
            send(
                p_send.at[layer, g, zz, at], p_recv.at[layer, g, zz, at],
                a_send.at[layer, g, 0], a_recv.at[layer, g, sem], x_mate,
                (zz // 2 != t) if halved(layer, g) else None,
            )

        def inverse(layer, g):
            arrived(sq_recv.at[layer, g], a_recv.at[layer, g, n_z])
            for k in range(sq_tiles):
                mean = (sq_send[layer, g, k] + sq_recv[layer, g, k]) / (2 * feats)
                inv = lax.rsqrt(mean + EPS)
                inv_col[g, pl.ds(k * lanes, lanes)] = jnp.broadcast_to(inv[0:1], (lanes, lanes)).T

        def pool(layer, g, k):
            pool_plane(layer, g, chunk_z[k])

        def pool_half(j):
            pool_plane(last, 1, half_plane(t, j))
            ship_mix(last, j)

        def ship_mix(layer, j):
            zz = half_plane(t, j)
            send(
                mix.at[mix_slot(layer, 1), zz, pl.ds(halo, rows)], mix_in.at[layer, zz],
                m_send.at[layer], m_recv.at[layer, zz], outer,
            )

        def ship_mixes(layer):
            for j in range(2):
                ship_mix(layer, j)

        def pool_plane(layer, g, group):
            start = first_row(layer)
            at = from_row(start)
            if layer == 0 and g == 1:
                early, late = pl.ds(0, split_row), pl.ds(split_row, total - split_row)
                arrived(p_recv.at[layer, g, group, early], a_recv.at[layer, g, n_z + 1 + group])
                arrived(p_recv.at[layer, g, group, late], a_recv.at[layer, g, group])
            else:
                arrived(p_recv.at[layer, g, group, at], a_recv.at[layer, g, group])
            row = lax.broadcasted_iota(jnp.int32, (total - start, lanes), 0)
            position = (s_in if g == 0 else s_end) * rows - halo + start + row
            span = jnp.left_shift(jnp.int32(2), group)
            divisor = jnp.maximum(jnp.minimum(position + 1, span), 1).astype(jnp.float32)
            share = 1.0 / divisor
            inv = inv_col[g, at]
            for j in range(chunk // lanes):
                cols = pl.ds(j * lanes, lanes)
                joined = p_send[layer, g, group, at, cols].astype(jnp.float32)
                joined = joined + p_recv[layer, g, group, at, cols].astype(jnp.float32)
                base = (joined * inv).astype(jnp.bfloat16).astype(jnp.float32)
                running = base
                width = 1
                picked = None
                for step in range(GROUPS):
                    running = running + pltpu.roll(running, width, 0)
                    width *= 2
                    picked = running if picked is None else jnp.where(group >= step, running, picked)
                lane = pl.multiple_of(group * chunk + j * lanes, lanes)
                scale = scale_ref[pl.ds(layer, 1), pl.ds(lane, lanes)]
                mix[mix_slot(layer, g), group, at, cols] = ((picked * share - base) * scale).astype(jnp.bfloat16)

        def expand(layer, g, begin, end):
            width = 256
            at = from_row(first_row(layer + 1))
            buf = 2 * layer + 1
            if layer < last and begin == 0:
                part_sq[g] = jnp.zeros(part_sq.shape[1:], jnp.float32)

            @pl.loop(begin * quarter // width, end * quarter // width)
            def _(n):
                col = pl.multiple_of(n * width, width)
                cols = pl.ds(col, width)
                mixed = jnp.concatenate([mix[mix_slot(layer, g), c, at] for c in range(n_z)], axis=1)
                weight = held[buf, :, :, cols].reshape(pools, width)
                branch = jnp.dot(mixed, weight, preferred_element_type=jnp.float32)
                new = (state[g, at, cols].astype(jnp.float32) + branch).astype(jnp.bfloat16)
                if layer == last:
                    o_ref[:, cols] = new
                else:
                    state[g, at, cols] = new
                    wide = new.astype(jnp.float32)
                    xg[g, at, cols] = (wide * gain_of(layer + 1, col, width)).astype(jnp.bfloat16)
                    square = wide * wide
                    sums = square[:, :lanes]
                    for j in range(1, width // lanes):
                        sums = sums + square[:, j * lanes:(j + 1) * lanes]
                    part_sq[g, at] = part_sq[g, at] + sums

            if layer < last and end == 4:
                pack_squares(g, layer + 1)

        def prepare():
            for g in range(2):
                part_sq[g] = jnp.zeros(part_sq.shape[1:], jnp.float32)
            own_state()

        def first_squares(g):
            if g == 0:
                take_edge(0)
                squares(0, 0, total)
            pack_squares(g, 0)

        def halo_squares():
            take_edge(1)
            squares(1, 0, halo)

        def shipped_squares(k):
            take_state(k)
            squares(1, halo + k * state_rows, halo + (k + 1) * state_rows)

        run({
            "im": own_across, "iy": own_to_mate, "ic": own_near, "E": take_end, "O": take_over, "M": take_mate, "F": take_far,
            "EM": take_mate_end, "OM": take_mate_over, "FM": take_mate_far,
            "plane": plane, "all": gathered, "bplane": gathered_piece, "edge": send_edge, "init": prepare, "sq": first_squares, "sqa": halo_squares,
            "st": shipped_squares, "P": project, "PA": project_early, "PB": project_late, "Q": pool, "inv": inverse, "H": pool_half,
            "mx": ship_mixes, "X": expand,
        }, INNER_ORDER)
        with jax.named_scope("drain"):
            drain_weights()
            departed(x_ref.at[pl.ds(0, halo)], e_send.at[0])
            for layer in range(layers):
                departed(mix_in.at[layer, pl.ds(2 * t, 2)], m_send.at[layer])
                at = from_row(first_row(layer))
                for g in range(2):
                    departed(sq_send.at[layer, g], a_send.at[layer, g, 1])
                    zz = pl.ds(2 * (1 - t), 2) if halved(layer, g) else pl.ds(0, n_z)
                    departed(p_send.at[layer, g, zz, at], a_send.at[layer, g, 0])

    pl.when(is_end)(end_program)
    pl.when(jnp.logical_not(is_end))(inner_program)


def fused_body(inputs, norm_gain, in_weight, pool_scale, out_weight):
    rows, feats = inputs.shape
    layers = norm_gain.shape[0]
    pools = pool_scale.shape[1]
    blocks = lax.axis_size("sp")
    n_z = blocks // 4
    depth = out_weight.shape[1]
    halo = REACH * layers
    total = rows + halo
    sq_tiles = -(-total // 128)
    chunk = pools // n_z
    phases = len(phase_table(feats))
    state_chunks = len([row for row in END_ORDER if row[0] == "st"])
    bf, f32 = jnp.bfloat16, jnp.float32
    vmem = pl.BlockSpec(memory_space=pltpu.VMEM)
    hbm = pl.BlockSpec(memory_space=pl.ANY)
    dma = pltpu.SemaphoreType.DMA
    return pl.pallas_call(
        functools.partial(kernel, n_z, layers, halo),
        out_shape=jax.ShapeDtypeStruct((rows, feats), bf),
        in_specs=[hbm, vmem, hbm, vmem, hbm],
        out_specs=vmem,
        scratch_shapes=[
            pltpu.VMEM((rows, feats), bf),
            pltpu.VMEM((layers, depth, feats), bf),
            pltpu.VMEM((layers, depth, feats), bf),
            pltpu.VMEM((2 * layers, blocks, depth, feats), bf),
            pltpu.VMEM((2, total, feats), bf),
            pltpu.VMEM((2, total, feats), bf),
            pltpu.VMEM((2, halo, feats), bf),
            pltpu.VMEM((layers, 2, n_z, total, chunk), bf),
            pltpu.VMEM((layers, 2, n_z, total, chunk), bf),
            pltpu.VMEM((1 + layers, n_z, total, chunk), bf),
            pltpu.VMEM((layers, n_z, rows, chunk), bf),
            pltpu.VMEM((2, sq_tiles * 128, 128), f32),
            pltpu.VMEM((2, sq_tiles * 128, 128), f32),
            pltpu.VMEM((layers, 2, sq_tiles, 8, 128), f32),
            pltpu.VMEM((layers, 2, sq_tiles, 8, 128), f32),
            dma((2 * layers, 2)),
            dma((phases, 8)),
            dma((layers * n_z + layers - 1 + PIECES[-1],)),
            dma((2 * layers - 1 + PIECES[-1],)),
            dma((3,)),
            dma((1,)),
            dma((2,)),
            dma((1,)),
            dma((state_chunks,)),
            dma((layers, 2, 2)),
            dma((layers, 2, 2 * n_z + 1)),
            dma((layers,)),
            dma((layers, n_z)),
        ],
        compiler_params=pltpu.CompilerParams(
            collective_id=0, has_side_effects=True, vmem_limit_bytes=60 * 1024 * 1024
        ),
    )(inputs, norm_gain, jnp.swapaxes(in_weight, 1, 2), pool_scale, out_weight)


def solution(mesh):
    n_sp, n_tp = mesh.shape["sp"], mesh.shape["tp"]
    fused = n_tp == 2 and n_sp == 16
    placed = (P("sp", "tp"), P(), P(None, "tp", "sp"), P(), P(None, "sp", "tp"))
    return jax.shard_map(
        fused_body if fused else plain_body,
        mesh=mesh, in_specs=placed, out_specs=P("sp", "tp"), check_vma=False,
    )
```

```python
import functools

import jax
import jax.numpy as jnp
from jax import lax
from jax.experimental import pallas as pl
from jax.experimental.pallas import tpu as pltpu
from jax.sharding import PartitionSpec as P

EPS = 1e-06
REACH = 16
GROUPS = 4
MESH_ID = pl.DeviceIdType.MESH


def shift_sp(value):
    count = lax.axis_size("sp")
    return lax.ppermute(value, "sp", [(i, i + 1) for i in range(count - 1)])


def window_means(extended, row_count, first_channel, first_pos, pool_total):
    width = extended.shape[1]
    channel = first_channel + lax.broadcasted_iota(jnp.int32, (1, width), 1)
    window_len = jnp.left_shift(jnp.int32(2), channel // (pool_total // GROUPS))
    running = jnp.zeros((row_count, width), jnp.float32)
    for offset in range(REACH):
        shifted = extended[REACH - offset : REACH - offset + row_count]
        running = running + jnp.where(offset < window_len, shifted, 0.0)
    position = first_pos + lax.broadcasted_iota(jnp.int32, (row_count, 1), 0)
    divisor = jnp.minimum(position + 1, window_len).astype(jnp.float32)
    return running / divisor - extended[REACH:]


def plain_body(inputs, norm_gain, in_weight, pool_scale, out_weight):
    rows, feats = inputs.shape
    layers, features = norm_gain.shape
    pools = pool_scale.shape[1]
    part = pools // lax.axis_size("tp")
    t = lax.axis_index("tp")
    s = lax.axis_index("sp")
    current = inputs
    for layer in range(layers):
        in_all = lax.all_gather(in_weight[layer], "sp", axis=1, tiled=True)
        out_all = lax.all_gather(out_weight[layer], "sp", axis=0, tiled=True)
        wide = current.astype(jnp.float32)
        squares = lax.psum(jnp.sum(wide * wide, axis=1), "tp")
        inv_rms = lax.rsqrt(squares / features + EPS)[:, None]
        gain = lax.dynamic_slice_in_dim(norm_gain[layer], t * feats, feats)
        normed = (wide * inv_rms * gain).astype(jnp.bfloat16)
        partial = jnp.dot(normed, in_all, preferred_element_type=jnp.float32)
        pool_in = lax.psum_scatter(
            partial.astype(jnp.bfloat16), "tp", scatter_dimension=1, tiled=True
        )
        edge = shift_sp(pool_in[rows - REACH :])
        extended = jnp.concatenate([edge, pool_in], 0).astype(jnp.float32)
        means = window_means(extended, rows, t * part, s * rows, pools)
        scale = lax.dynamic_slice_in_dim(pool_scale[layer], t * part, part)
        mixed = (means * scale).astype(jnp.bfloat16)
        pooled = lax.all_gather(mixed, "tp", axis=1, tiled=True)
        branch = jnp.dot(pooled, out_all, preferred_element_type=jnp.float32)
        current = (current.astype(jnp.float32) + branch).astype(jnp.bfloat16)
    return current


E, O, M, F, EM, OM1, OM2, FM = range(8)
PIECES = (2, 2, 2, 4, 2, 4)
EDGE_BY_MATE = (True, False, False, False, False, False)
OVER_BY_MATE = (0.5, 0.5, 0.5, 0.5, 0.5, 0)
INNER_ORDER = [
    ("im", 0), ("iy", 0), ("edge",), ("im", 1), ("im", 2), ("init",), ("iy", 1), ("iy", 2), ("ic", 0), ("ic", 1),
    ("ic", 2), ("O", 0), ("M", 0), ("E", 0), ("O", 1), ("E", 1), ("sq", 0), ("M", 1), ("O", 2), ("E", 2),
    ("plane", 0, 0), ("P", 0, 0, 0), ("inv", 0, 0), ("M", 2), ("OM", 0), ("E", 3), ("F", 0), ("EM", 0),
    ("Q", 0, 0, 0), ("sqa",), ("F", 1), ("OM", 1), ("EM", 1), ("plane", 0, 2), ("P", 0, 0, 2), ("iy", 3), ("iy", 4),
    ("iy", 5), ("plane", 0, 1), ("P", 0, 0, 1), ("F", 2), ("st", 0), ("OM", 2), ("im", 3), ("FM", 0), ("im", 4),
    ("im", 5), ("im", 6), ("im", 7), ("im", 8), ("im", 9), ("F", 3), ("Q", 0, 0, 2), ("FM", 1), ("st", 1), ("PA", 0),
    ("plane", 0, 3), ("PA", 3), ("O", 3), ("PA", 1), ("M", 3), ("P", 0, 0, 3), ("Q", 0, 0, 1), ("PA", 2), ("O", 4),
    ("M", 4), ("im", 10), ("im", 11), ("st", 2), ("O", 5), ("M", 5), ("O", 6), ("ic", 3), ("ic", 4), ("ic", 5),
    ("ic", 6), ("O", 7), ("ic", 7), ("ic", 8), ("ic", 9), ("FM", 2), ("O", 8), ("plane", 2, 0), ("st", 3), ("sq", 1),
    ("PB", 3), ("O", 9), ("Q", 0, 0, 3), ("PB", 2), ("PB", 0), ("FM", 3), ("PB", 1), ("EM", 2), ("inv", 0, 1),
    ("OM", 3), ("Q", 0, 1, 3), ("iy", 6), ("iy", 7), ("iy", 8), ("iy", 9), ("iy", 10), ("OM", 4), ("EM", 3),
    ("Q", 0, 1, 2), ("O", 10), ("all", 1), ("X", 0, 0, 0, 1), ("Q", 0, 1, 0), ("X", 0, 0, 1, 2), ("E", 4),
    ("X", 0, 0, 2, 4), ("O", 11), ("P", 1, 0, 0), ("M", 6), ("OM", 5), ("ic", 10), ("ic", 11), ("ic", 12),
    ("Q", 0, 1, 1), ("E", 5), ("mx", 0), ("X", 0, 1, 0, 1), ("M", 7), ("X", 0, 1, 1, 2), ("im", 12), ("im", 13),
    ("im", 14), ("plane", 2, 2), ("P", 1, 0, 2), ("F", 4), ("M", 8), ("inv", 1, 0), ("X", 0, 1, 2, 3), ("EM", 4),
    ("OM", 6), ("X", 0, 1, 3, 4), ("M", 9), ("P", 1, 1, 2), ("Q", 1, 0, 0), ("P", 1, 1, 0), ("EM", 5), ("F", 5),
    ("iy", 11), ("M", 10), ("OM", 7), ("E", 6), ("plane", 2, 1), ("P", 1, 1, 1), ("O", 12), ("Q", 1, 0, 2),
    ("inv", 1, 1), ("P", 1, 0, 1), ("E", 7), ("O", 13), ("E", 8), ("O", 14), ("E", 9), ("Q", 1, 1, 2), ("OM", 8),
    ("FM", 4), ("OM", 9), ("OM", 10), ("E", 10), ("Q", 1, 1, 0), ("FM", 5), ("F", 6), ("plane", 2, 3),
    ("P", 1, 1, 3), ("F", 7), ("E", 11), ("P", 1, 0, 3), ("M", 11), ("Q", 1, 1, 1), ("F", 8), ("EM", 6), ("FM", 6),
    ("plane", 4, 0), ("F", 9), ("ic", 13), ("ic", 14), ("ic", 15), ("EM", 7), ("FM", 7), ("im", 15), ("Q", 1, 0, 1),
    ("EM", 8), ("FM", 8), ("F", 10), ("EM", 9), ("FM", 9), ("Q", 1, 1, 3), ("mx", 1), ("all", 3), ("X", 1, 1, 0, 1),
    ("F", 11), ("X", 1, 1, 1, 2), ("EM", 10), ("X", 1, 1, 2, 3), ("OM", 11), ("X", 1, 1, 3, 4), ("FM", 10),
    ("Q", 1, 0, 3), ("X", 1, 0, 0, 1), ("EM", 11), ("O", 15), ("plane", 4, 2), ("P", 2, 1, 0), ("P", 2, 1, 2),
    ("E", 12), ("plane", 4, 1), ("FM", 11), ("inv", 2, 1), ("P", 2, 1, 1), ("X", 1, 0, 1, 2), ("E", 13),
    ("plane", 4, 3), ("P", 2, 1, 3), ("X", 1, 0, 2, 3), ("EM", 12), ("X", 1, 0, 3, 4), ("F", 12), ("P", 2, 0, 2),
    ("E", 14), ("P", 2, 0, 3), ("F", 13), ("EM", 13), ("P", 2, 0, 1), ("H", 0), ("P", 2, 0, 0), ("EM", 14),
    ("FM", 12), ("iy", 12), ("iy", 13), ("iy", 14), ("iy", 15), ("inv", 2, 0), ("H", 1), ("F", 14), ("E", 15),
    ("FM", 13), ("EM", 15), ("M", 12), ("Q", 2, 0, 2), ("F", 15), ("M", 13), ("M", 14), ("Q", 2, 0, 3), ("OM", 12),
    ("M", 15), ("OM", 13), ("bplane", 12), ("FM", 14), ("bplane", 13), ("OM", 14), ("Q", 2, 0, 1), ("FM", 15),
    ("bplane", 14), ("OM", 15), ("bplane", 15), ("Q", 2, 0, 0), ("X", 2, 0, 0, 4),
]
END_ORDER = [
    ("edge", 0), ("ey", 0), ("ey", 1), ("ey", 2), ("ey", 3), ("eown", 0), ("eown", 1), ("eown", 2), ("eown", 3),
    ("eM", 1), ("eM", 0), ("edge", 1), ("ey", 4), ("ey", 5), ("st", 0), ("st", 1), ("st", 2), ("st", 3), ("eM", 2),
    ("eI", 2), ("eM", 3), ("eown", 4), ("eown", 5), ("eM", 4), ("eM", 5), ("eO", 2), ("eIM", 2), ("eOM", 2),
    ("eF", 2), ("ey", 6), ("eown", 6), ("eF", 3), ("eFM", 2), ("ey", 7), ("ey", 8), ("eown", 7), ("ey", 9),
    ("ey", 10), ("ey", 11), ("eown", 8), ("eown", 9), ("eown", 10), ("eown", 11), ("eM", 6), ("eO", 3), ("eFM", 3),
    ("eM", 7), ("eO", 6), ("eM", 8), ("eM", 9), ("eI", 3), ("ey", 12), ("ey", 13), ("ey", 14), ("ey", 15), ("eI", 6),
    ("eM", 10), ("eO", 7), ("eI", 7), ("eM", 11), ("eI", 8), ("eI", 9), ("eOM", 3), ("eO", 8), ("eOM", 6), ("eO", 9),
    ("eIM", 3), ("eI", 12), ("eown", 12), ("eown", 13), ("eM", 12), ("eown", 14), ("eM", 13), ("emx", 0, 0),
    ("eM", 14), ("eown", 15), ("eM", 15), ("emx", 0, 1), ("eIM", 6), ("emy", 0, 0), ("eO", 12), ("eOM", 7),
    ("eO", 13), ("eIM", 7), ("emy", 0, 1), ("eall", 1), ("eX", 0, 0, 2), ("eIM", 8), ("eO", 14), ("eX", 0, 2, 4),
    ("eIM", 9), ("eOM", 8), ("eF", 6), ("eOM", 9), ("eIM", 12), ("eF", 7), ("eOM", 12), ("eF", 8), ("eOM", 13),
    ("eF", 9), ("eOM", 14), ("eI", 13), ("eFM", 6), ("eI", 14), ("eFM", 7), ("eI", 15), ("eFM", 8), ("eFM", 9),
    ("emx", 1, 0), ("eIM", 13), ("eIM", 14), ("emx", 1, 1), ("eIM", 15), ("eO", 15), ("emy", 1, 0), ("eF", 12),
    ("emy", 1, 1), ("eall", 3), ("eX", 1, 0, 1), ("eOM", 15), ("eX", 1, 1, 2), ("eF", 13), ("eX", 1, 2, 4),
    ("eFM", 12), ("emx", 2, 0), ("epl", 12), ("eFM", 13), ("epl", 13), ("emx", 2, 1), ("eF", 14), ("emy", 2, 0),
    ("eF", 15), ("emy", 2, 1), ("eX", 2, 0, 1), ("eFM", 14), ("eX", 2, 1, 2), ("eFM", 15), ("epl", 14),
    ("eX", 2, 2, 3), ("epl", 15), ("eX", 2, 3, 4),
]


def phase_table(feats):
    table = []
    for buf, count in enumerate(PIECES):
        width = feats // count
        table += [(buf, k * width, width) for k in range(count)]
    return table


def kernel(
    n_z, layers, halo,
    x_hbm, gain_ref, wi_hbm, scale_ref, wo_hbm, o_hbm,
    x_ref, wi_ref, wo_ref, o_ref, held, state, xg, edge, p_send, p_recv, mix, mix_in, part_sq, inv_col, sq_send, sq_recv,
    w_send, w_recv, c_recv, local_sem, load_sem, out_sem, e_send, e_recv, s_send, s_recv, a_send, a_recv, early_recv, m_send, m_recv,
):
    loads = [
        pltpu.make_async_copy(src, dst, load_sem.at[i])
        for i, (src, dst) in enumerate([(wi_hbm, wi_ref), (x_hbm, x_ref), (wo_hbm, wo_ref)])
    ]
    for load in loads:
        load.start()
    rows, feats = x_ref.shape
    total = rows + halo
    blocks, depth = held.shape[1], held.shape[2]
    pools = scale_ref.shape[1]
    chunk = pools // n_z
    last = layers - 1
    table = phase_table(feats)
    phases = len(table)
    lanes = 128
    quarter = feats // 4
    state_chunks = s_recv.shape[0]
    last_buf = len(PIECES) - 1
    sq_tiles = part_sq.shape[1] // lanes
    s = lax.axis_index("sp")
    t = lax.axis_index("tp")
    core = s % 2
    y = (s // 2) % 2
    z = s // 4
    side = z // 2

    def block_of(zz, yy, cc):
        return zz * 4 + yy * 2 + cc

    z_in, z_end = 1 + side, 3 * side
    z_over, z_far = 2 - side, 3 - 3 * side
    is_end = z == z_end
    s_end, s_in = block_of(z_end, y, core), block_of(z_in, y, core)

    y_mate = (block_of(z, 1 - y, core), t)
    c_mate = (block_of(z, y, 1 - core), t)
    x_mate = (s, 1 - t)
    opposite = (block_of(z_over, y, core), t)
    inner = (s_in, t)
    outer = (s_end, t)
    after = (s + 1) % blocks
    after_z = after // 4
    after_holder = (block_of(1 + after_z // 2, (after // 2) % 2, after % 2), t)
    after_slot = jnp.where((after_z == 0) | (after_z == n_z - 1), 1, 0)
    before = [((s_in + blocks - 1) % blocks, t), ((s_end + blocks - 1) % blocks, t)]

    barrier = pltpu.get_barrier_semaphore()

    def greet(peers):
        for peer in peers:
            pl.semaphore_signal(barrier, inc=1, device_id=peer, device_id_type=MESH_ID)

    def send(src, dst, send_sem, recv_sem, to, when=None):
        copy = pltpu.make_async_remote_copy(
            src_ref=src, dst_ref=dst, send_sem=send_sem, recv_sem=recv_sem,
            device_id=to, device_id_type=MESH_ID,
        )
        if when is None:
            copy.start()
        else:
            pl.when(when)(copy.start)

    def departed(ref, sem):
        pltpu.make_async_remote_copy(
            src_ref=ref, dst_ref=ref, send_sem=sem, recv_sem=sem,
            device_id=c_mate, device_id_type=MESH_ID,
        ).wait_send()

    def arrived(ref, sem):
        pltpu.make_async_remote_copy(
            src_ref=ref, dst_ref=ref, send_sem=sem, recv_sem=sem,
            device_id=c_mate, device_id_type=MESH_ID,
        ).wait_recv()

    whole, first, second = pl.ds(0, depth), pl.ds(0, depth // 2), pl.ds(depth // 2, depth // 2)
    volume = {}

    def put_out(cols):
        pltpu.make_async_copy(o_ref.at[:, cols], o_hbm.at[:, cols], out_sem.at[0]).start()

    def wait_out():
        pltpu.make_async_copy(o_ref, o_hbm, out_sem.at[0]).wait()

    def own(ph):
        buf, start, width = table[ph]
        return (wi_ref if buf % 2 == 0 else wo_ref).at[buf // 2, :, pl.ds(start, width)]

    def slot(ph, block, piece=whole):
        buf, start, width = table[ph]
        return held.at[buf, block, piece, pl.ds(start, width)]

    def send_sem(ph, port, piece):
        buf, _, width = table[ph]
        kind = 1 if port == EM else 0
        share = width * (1 if piece is whole else 0.5) / feats
        volume[buf, kind] = volume.get((buf, kind), 0) + share
        return w_send.at[buf, kind]

    def core_sem(ph, block):
        buf, start, width = table[ph]
        layer = buf // 2
        if buf % 2 == 0:
            return c_recv.at[layer * n_z + block // 4]
        return c_recv.at[layers * n_z + layer + (start // width if buf == last_buf else 0)]

    def send_own(ph, to, port):
        sem = core_sem(ph, s) if port is None else w_recv.at[ph, port]
        send(own(ph), slot(ph, s), send_sem(ph, port, whole), sem, to)

    def forward(ph, block, to, port, piece=whole):
        ref = slot(ph, block, piece)
        sem = core_sem(ph, block) if port is None else w_recv.at[ph, port]
        send(ref, ref, send_sem(ph, port, piece), sem, to)

    def wait_block(ph, block, port, piece=whole):
        arrived(slot(ph, block, piece), w_recv.at[ph, port])

    def drain_weights():
        for (buf, kind), blocks_sent in volume.items():
            assert blocks_sent == int(blocks_sent)
            departed(held.at[buf, pl.ds(0, int(blocks_sent))], w_send.at[buf, kind])
        volume.clear()

    state_rows = rows // state_chunks
    split_row = halo + rows // 2
    def parts_of(buf):
        return [ph for ph in range(phases) if table[ph][0] == buf]

    def is_out(ph):
        return table[ph][0] % 2 == 1

    def local_of(ph):
        buf, start, width = table[ph]
        return local_sem.at[buf + (start // width if buf == last_buf else 0)]

    def keep_own(ph):
        pltpu.make_async_copy(own(ph), slot(ph, s), local_of(ph)).start()

    def gathered(buf):
        ph = parts_of(buf)[0]
        weight = (wi_ref if buf % 2 == 0 else wo_ref).at[buf // 2]
        pltpu.make_async_copy(weight, held.at[buf, s], local_of(ph)).wait()
        arrived(held.at[buf, pl.ds(0, blocks // 2)], core_sem(ph, s))

    def gathered_piece(ph):
        buf, start, width = table[ph]
        pltpu.make_async_copy(own(ph), slot(ph, s), local_of(ph)).wait()
        arrived(held.at[buf, pl.ds(0, blocks // 2), :, pl.ds(start, width)], core_sem(ph, s))

    def half_plane(which, j):
        near = jnp.where(side == 0, z_in - j, z_in + j)
        far = jnp.where(side == 0, z_over + j, z_over - j)
        return jnp.where(which == side, near, far)

    def send_edge(when=None):
        send(
            x_ref.at[pl.ds(rows - halo, halo)], edge.at[after_slot],
            e_send.at[0], e_recv.at[after_slot], after_holder, when,
        )

    def send_some_edges(which):
        send_edge(after_slot == which)

    def run(table_of_steps, order):
        for name, *args in order:
            with jax.named_scope("_".join([name] + [str(a) for a in args])):
                table_of_steps[name](*args)

    def end_program():
        greet([inner, y_mate, c_mate, x_mate])
        pl.semaphore_wait(barrier, 5)
        for load in loads:
            load.wait()
        mate = block_of(z_end, 1 - y, core)
        columns = [z_in, z_over, z_far]

        def own_aside(ph):
            if is_out(ph) or not EDGE_BY_MATE[table[ph][0]]:
                send_own(ph, y_mate, M)
            if is_out(ph):
                send_own(ph, c_mate, None)
                keep_own(ph)

        def own_inward(ph):
            send_own(ph, inner, E)

        def mate_inward(ph):
            direct = not EDGE_BY_MATE[table[ph][0]]
            if is_out(ph) or direct:
                wait_block(ph, mate, M)
            if direct:
                forward(ph, mate, inner, EM)
            if is_out(ph):
                forward(ph, mate, c_mate, None)

        def ship_state(k):
            at = pl.ds(k * state_rows, state_rows)
            send(
                x_ref.at[at], state.at[1, pl.ds(halo + k * state_rows, state_rows)],
                s_send.at[0], s_recv.at[k], inner,
            )

        def take_column(which, ph):
            block = block_of(columns[which], y, core)
            wait_block(ph, block, (E, O, F)[which])
            forward(ph, block, y_mate, (EM, OM1, FM)[which])
            forward(ph, block, c_mate, None)

        def take_mate_column(which, ph):
            block = block_of(columns[which], 1 - y, core)
            wait_block(ph, block, (EM, OM1, FM)[which])
            forward(ph, block, c_mate, None)

        def take_mix(layer, j):
            zz = half_plane(t, j)
            ref, sem = mix_in.at[layer, zz], m_recv.at[layer, zz]
            arrived(ref, sem)
            send(ref, ref, m_send.at[layer], sem, x_mate)

        def take_mate_mix(layer, j):
            zz = half_plane(1 - t, j)
            arrived(mix_in.at[layer, zz], m_recv.at[layer, zz])

        def end_expand(layer, begin, end):
            width = 256
            at = pl.ds(halo, rows)

            @pl.loop(begin * quarter // width, end * quarter // width)
            def _(n):
                cols = pl.ds(pl.multiple_of(n * width, width), width)
                mixed = jnp.concatenate([mix_in[layer, c] for c in range(n_z)], axis=1)
                weight = held[2 * layer + 1, :, :, cols].reshape(pools, width)
                branch = jnp.dot(mixed, weight, preferred_element_type=jnp.float32)
                old = x_ref[:, cols] if layer == 0 else state[1, at, cols]
                new = (old.astype(jnp.float32) + branch).astype(jnp.bfloat16)
                if layer == last:
                    o_ref[:, cols] = new
                    put_out(cols)
                else:
                    state[1, at, cols] = new

        part = functools.partial
        run({
            "ey": own_aside, "eown": own_inward, "eM": mate_inward, "st": ship_state,
            "eI": part(take_column, 0), "eO": part(take_column, 1), "eF": part(take_column, 2),
            "eIM": part(take_mate_column, 0), "eOM": part(take_mate_column, 1),
            "eFM": part(take_mate_column, 2), "eall": gathered, "epl": gathered_piece,
            "edge": send_some_edges,
            "emx": take_mix, "emy": take_mate_mix, "eX": end_expand,
        }, END_ORDER)
        with jax.named_scope("drain"):
            drain_weights()
            wait_out()
            departed(x_ref, s_send.at[0])
            departed(x_ref.at[pl.ds(0, halo)], e_send.at[0])
            for layer in range(layers):
                departed(mix_in.at[layer, pl.ds(2 * t, 2)], m_send.at[layer])

    def inner_program():
        with jax.named_scope("greet"):
            greet([opposite, y_mate, c_mate, x_mate, outer] + before)
        with jax.named_scope("barrier"):
            pl.semaphore_wait(barrier, 6)
        for load in loads:
            load.wait()
        chunk_z = [z_in, z_end, z_over, z_far]

        def own_across(ph):
            send_own(ph, opposite, O)

        def own_to_mate(ph):
            send_own(ph, y_mate, M)

        def own_near(ph):
            send_own(ph, c_mate, None)
            if is_out(ph):
                send_own(ph, outer, E)
            keep_own(ph)

        def over_pieces(ph):
            share = OVER_BY_MATE[table[ph][0]]
            by_mate = None if share == 0 else whole if share == 1 else first
            direct = None if share == 1 else whole if share == 0 else second
            return by_mate, direct

        def take_end(ph):
            block = block_of(z_end, y, core)
            wait_block(ph, block, E)
            forward(ph, block, opposite, F)
            if EDGE_BY_MATE[table[ph][0]]:
                forward(ph, block, y_mate, EM)
            forward(ph, block, c_mate, None)

        def take_over(ph):
            block = block_of(z_over, y, core)
            wait_block(ph, block, O)
            by_mate, _ = over_pieces(ph)
            if by_mate is not None:
                forward(ph, block, y_mate, OM1, by_mate)
            forward(ph, block, c_mate, None)
            if is_out(ph):
                forward(ph, block, outer, O)

        def take_mate(ph):
            block = block_of(z_in, 1 - y, core)
            wait_block(ph, block, M)
            _, direct = over_pieces(ph)
            if direct is not None:
                forward(ph, block, opposite, OM2, direct)
            forward(ph, block, c_mate, None)

        def take_far(ph):
            block = block_of(z_far, y, core)
            wait_block(ph, block, F)
            forward(ph, block, y_mate, FM)
            forward(ph, block, c_mate, None)
            if is_out(ph):
                forward(ph, block, outer, F)

        def take_mate_end(ph):
            block = block_of(z_end, 1 - y, core)
            wait_block(ph, block, EM)
            forward(ph, block, c_mate, None)

        def take_mate_over(ph):
            block = block_of(z_over, 1 - y, core)
            by_mate, direct = over_pieces(ph)
            if by_mate is not None:
                wait_block(ph, block, OM1, by_mate)
            if direct is not None:
                wait_block(ph, block, OM2, direct)
            forward(ph, block, c_mate, None)

        def take_mate_far(ph):
            block = block_of(z_far, 1 - y, core)
            wait_block(ph, block, FM)
            forward(ph, block, c_mate, None)

        def plane(buf, k):
            if k == 0:
                weight = wi_ref.at[buf // 2]
                pltpu.make_async_copy(weight, held.at[buf, s], local_of(parts_of(buf)[0])).wait()
            block = block_of(chunk_z[k], 0, 0)
            arrived(held.at[buf, pl.ds(block, 2)], core_sem(parts_of(buf)[0], block))

        def first_row(layer):
            return REACH * layer

        def from_row(start):
            return pl.ds(start, total - start)

        def gain_of(layer, start, width):
            at = pl.multiple_of(t * feats + start, lanes)
            return gain_ref[pl.ds(layer, 1), pl.ds(at, width)]

        def pack_squares(g, layer):
            for k in range(sq_tiles):
                block = part_sq[g, pl.ds(k * lanes, lanes)].T
                value = jnp.sum(block, axis=0, keepdims=True)
                sq_send[layer, g, k] = jnp.broadcast_to(value, (8, lanes))
            send(
                sq_send.at[layer, g], sq_recv.at[layer, g],
                a_send.at[layer, g, 1], a_recv.at[layer, g, n_z], x_mate,
            )

        def halved(layer, g):
            return layer == last and g == 1

        def mix_slot(layer, g):
            return 0 if g == 0 else 1 + layer

        def take_edge(g):
            arrived(edge.at[g], e_recv.at[g])
            keep = ((s_in if g == 0 else s_end) > 0).astype(jnp.float32)

            @pl.loop(0, halo // REACH)
            def _(i):
                at = pl.ds(i * REACH, REACH)
                state[g, at] = (edge[g, at].astype(jnp.float32) * keep).astype(jnp.bfloat16)

        def own_state():
            @pl.loop(0, rows // REACH)
            def _(i):
                state[0, pl.ds(halo + i * REACH, REACH)] = x_ref[pl.ds(i * REACH, REACH)]

        def take_state(k):
            arrived(state.at[1, pl.ds(halo + k * state_rows, state_rows)], s_recv.at[k])

        def squares(g, start, stop):
            @pl.loop(start // REACH, stop // REACH)
            def _(i):
                at = pl.ds(i * REACH, REACH)
                sums = jnp.zeros((REACH, lanes), jnp.float32)
                for j in range(feats // lanes):
                    cols = pl.ds(j * lanes, lanes)
                    wide = state[g, at, cols].astype(jnp.float32)
                    sums = sums + wide * wide
                    xg[g, at, cols] = (wide * gain_of(0, j * lanes, lanes)).astype(jnp.bfloat16)
                part_sq[g, at] = sums

        def project(layer, g, k):
            project_rows(layer, g, k, first_row(layer), total, a_recv.at[layer, g, chunk_z[k]])

        def project_early(k):
            project_rows(0, 1, k, 0, split_row, early_recv.at[chunk_z[k]])

        def project_late(k):
            project_rows(0, 1, k, split_row, total, a_recv.at[0, 1, chunk_z[k]])

        def project_rows(layer, g, k, start, stop, sem):
            at = pl.ds(start, stop - start)
            zz = chunk_z[k]
            weight = held[2 * layer, pl.ds(zz * 4, 4)].reshape(chunk, feats)
            value = lax.dot_general(
                xg[g, at], weight, (((1,), (1,)), ((), ())),
                preferred_element_type=jnp.float32,
            )
            p_send[layer, g, zz, at] = value.astype(jnp.bfloat16)
            send(
                p_send.at[layer, g, zz, at], p_recv.at[layer, g, zz, at],
                a_send.at[layer, g, 0], sem, x_mate,
                (zz // 2 != t) if halved(layer, g) else None,
            )

        def inverse(layer, g):
            arrived(sq_recv.at[layer, g], a_recv.at[layer, g, n_z])
            for k in range(sq_tiles):
                mean = (sq_send[layer, g, k] + sq_recv[layer, g, k]) / (2 * feats)
                inv = lax.rsqrt(mean + EPS)
                inv_col[g, pl.ds(k * lanes, lanes)] = jnp.broadcast_to(inv[0:1], (lanes, lanes)).T

        def pool(layer, g, k):
            pool_plane(layer, g, chunk_z[k])

        def pool_half(j):
            pool_plane(last, 1, half_plane(t, j))
            ship_mix(last, j)

        def ship_mix(layer, j):
            zz = half_plane(t, j)
            send(
                mix.at[mix_slot(layer, 1), zz, pl.ds(halo, rows)], mix_in.at[layer, zz],
                m_send.at[layer], m_recv.at[layer, zz], outer,
            )

        def ship_mixes(layer):
            for j in range(2):
                ship_mix(layer, j)

        def pool_plane(layer, g, group):
            start = first_row(layer)
            at = from_row(start)
            if layer == 0 and g == 1:
                early, late = pl.ds(0, split_row), pl.ds(split_row, total - split_row)
                arrived(p_recv.at[layer, g, group, early], early_recv.at[group])
                arrived(p_recv.at[layer, g, group, late], a_recv.at[layer, g, group])
            else:
                arrived(p_recv.at[layer, g, group, at], a_recv.at[layer, g, group])
            row = lax.broadcasted_iota(jnp.int32, (total - start, lanes), 0)
            position = (s_in if g == 0 else s_end) * rows - halo + start + row
            span = jnp.left_shift(jnp.int32(2), group)
            divisor = jnp.maximum(jnp.minimum(position + 1, span), 1).astype(jnp.float32)
            share = 1.0 / divisor
            inv = inv_col[g, at]
            for j in range(chunk // lanes):
                cols = pl.ds(j * lanes, lanes)
                joined = p_send[layer, g, group, at, cols].astype(jnp.float32)
                joined = joined + p_recv[layer, g, group, at, cols].astype(jnp.float32)
                base = (joined * inv).astype(jnp.bfloat16).astype(jnp.float32)
                running = base
                width = 1
                picked = None
                for step in range(GROUPS):
                    running = running + pltpu.roll(running, width, 0)
                    width *= 2
                    picked = running if picked is None else jnp.where(group >= step, running, picked)
                lane = pl.multiple_of(group * chunk + j * lanes, lanes)
                scale = scale_ref[pl.ds(layer, 1), pl.ds(lane, lanes)]
                mix[mix_slot(layer, g), group, at, cols] = ((picked * share - base) * scale).astype(jnp.bfloat16)

        def expand(layer, g, begin, end):
            width = 256
            at = from_row(first_row(layer + 1))
            buf = 2 * layer + 1
            if layer < last and begin == 0:
                part_sq[g] = jnp.zeros(part_sq.shape[1:], jnp.float32)

            @pl.loop(begin * quarter // width, end * quarter // width)
            def _(n):
                col = pl.multiple_of(n * width, width)
                cols = pl.ds(col, width)
                mixed = jnp.concatenate([mix[mix_slot(layer, g), c, at] for c in range(n_z)], axis=1)
                weight = held[buf, :, :, cols].reshape(pools, width)
                branch = jnp.dot(mixed, weight, preferred_element_type=jnp.float32)
                new = (state[g, at, cols].astype(jnp.float32) + branch).astype(jnp.bfloat16)
                if layer == last:
                    o_ref[:, cols] = new
                    put_out(cols)
                else:
                    state[g, at, cols] = new
                    wide = new.astype(jnp.float32)
                    xg[g, at, cols] = (wide * gain_of(layer + 1, col, width)).astype(jnp.bfloat16)
                    square = wide * wide
                    sums = square[:, :lanes]
                    for j in range(1, width // lanes):
                        sums = sums + square[:, j * lanes:(j + 1) * lanes]
                    part_sq[g, at] = part_sq[g, at] + sums

            if layer < last and end == 4:
                pack_squares(g, layer + 1)

        def prepare():
            for g in range(2):
                part_sq[g] = jnp.zeros(part_sq.shape[1:], jnp.float32)
            own_state()

        def first_squares(g):
            if g == 0:
                take_edge(0)
                squares(0, 0, total)
            pack_squares(g, 0)

        def halo_squares():
            take_edge(1)
            squares(1, 0, halo)

        def shipped_squares(k):
            take_state(k)
            squares(1, halo + k * state_rows, halo + (k + 1) * state_rows)

        run({
            "im": own_across, "iy": own_to_mate, "ic": own_near, "E": take_end, "O": take_over, "M": take_mate, "F": take_far,
            "EM": take_mate_end, "OM": take_mate_over, "FM": take_mate_far,
            "plane": plane, "all": gathered, "bplane": gathered_piece, "edge": send_edge, "init": prepare, "sq": first_squares, "sqa": halo_squares,
            "st": shipped_squares, "P": project, "PA": project_early, "PB": project_late, "Q": pool, "inv": inverse, "H": pool_half,
            "mx": ship_mixes, "X": expand,
        }, INNER_ORDER)
        with jax.named_scope("drain"):
            drain_weights()
            wait_out()
            departed(x_ref.at[pl.ds(0, halo)], e_send.at[0])
            for layer in range(layers):
                departed(mix_in.at[layer, pl.ds(2 * t, 2)], m_send.at[layer])
                at = from_row(first_row(layer))
                for g in range(2):
                    departed(sq_send.at[layer, g], a_send.at[layer, g, 1])
                    zz = pl.ds(2 * (1 - t), 2) if halved(layer, g) else pl.ds(0, n_z)
                    departed(p_send.at[layer, g, zz, at], a_send.at[layer, g, 0])

    pl.when(is_end)(end_program)
    pl.when(jnp.logical_not(is_end))(inner_program)


def fused_body(inputs, norm_gain, in_weight, pool_scale, out_weight):
    rows, feats = inputs.shape
    layers = norm_gain.shape[0]
    pools = pool_scale.shape[1]
    blocks = lax.axis_size("sp")
    n_z = blocks // 4
    depth = out_weight.shape[1]
    halo = REACH * layers
    total = rows + halo
    sq_tiles = -(-total // 128)
    chunk = pools // n_z
    phases = len(phase_table(feats))
    state_chunks = len([row for row in END_ORDER if row[0] == "st"])
    bf, f32 = jnp.bfloat16, jnp.float32
    vmem = pl.BlockSpec(memory_space=pltpu.VMEM)
    hbm = pl.BlockSpec(memory_space=pl.ANY)
    dma = pltpu.SemaphoreType.DMA
    return pl.pallas_call(
        functools.partial(kernel, n_z, layers, halo),
        out_shape=jax.ShapeDtypeStruct((rows, feats), bf),
        in_specs=[hbm, vmem, hbm, vmem, hbm],
        out_specs=hbm,
        scratch_shapes=[
            pltpu.VMEM((rows, feats), bf),
            pltpu.VMEM((layers, depth, feats), bf),
            pltpu.VMEM((layers, depth, feats), bf),
            pltpu.VMEM((rows, feats), bf),
            pltpu.VMEM((2 * layers, blocks, depth, feats), bf),
            pltpu.VMEM((2, total, feats), bf),
            pltpu.VMEM((2, total, feats), bf),
            pltpu.VMEM((2, halo, feats), bf),
            pltpu.VMEM((layers, 2, n_z, total, chunk), bf),
            pltpu.VMEM((layers, 2, n_z, total, chunk), bf),
            pltpu.VMEM((1 + layers, n_z, total, chunk), bf),
            pltpu.VMEM((layers, n_z, rows, chunk), bf),
            pltpu.VMEM((2, sq_tiles * 128, 128), f32),
            pltpu.VMEM((2, sq_tiles * 128, 128), f32),
            pltpu.VMEM((layers, 2, sq_tiles, 8, 128), f32),
            pltpu.VMEM((layers, 2, sq_tiles, 8, 128), f32),
            dma((2 * layers, 2)),
            dma((phases, 8)),
            dma((layers * n_z + layers - 1 + PIECES[-1],)),
            dma((2 * layers - 1 + PIECES[-1],)),
            dma((3,)),
            dma((1,)),
            dma((1,)),
            dma((2,)),
            dma((1,)),
            dma((state_chunks,)),
            dma((layers, 2, 2)),
            dma((layers, 2, n_z + 1)),
            dma((n_z,)),
            dma((layers,)),
            dma((layers, n_z)),
        ],
        compiler_params=pltpu.CompilerParams(
            collective_id=0, has_side_effects=True, vmem_limit_bytes=60 * 1024 * 1024
        ),
    )(inputs, norm_gain, jnp.swapaxes(in_weight, 1, 2), pool_scale, out_weight)


def solution(mesh):
    n_sp, n_tp = mesh.shape["sp"], mesh.shape["tp"]
    fused = n_tp == 2 and n_sp == 16
    placed = (P("sp", "tp"), P(), P(None, "tp", "sp"), P(), P(None, "sp", "tp"))
    return jax.shard_map(
        fused_body if fused else plain_body,
        mesh=mesh, in_specs=placed, out_specs=P("sp", "tp"), check_vma=False,
    )
```

```python
import functools

import jax
import jax.numpy as jnp
from jax import lax
from jax.experimental import pallas as pl
from jax.experimental.pallas import tpu as pltpu
from jax.sharding import PartitionSpec as P

EPS = 1e-06
REACH = 16
GROUPS = 4
MESH_ID = pl.DeviceIdType.MESH


def shift_sp(value):
    count = lax.axis_size("sp")
    return lax.ppermute(value, "sp", [(i, i + 1) for i in range(count - 1)])


def window_means(extended, row_count, first_channel, first_pos, pool_total):
    width = extended.shape[1]
    channel = first_channel + lax.broadcasted_iota(jnp.int32, (1, width), 1)
    window_len = jnp.left_shift(jnp.int32(2), channel // (pool_total // GROUPS))
    running = jnp.zeros((row_count, width), jnp.float32)
    for offset in range(REACH):
        shifted = extended[REACH - offset : REACH - offset + row_count]
        running = running + jnp.where(offset < window_len, shifted, 0.0)
    position = first_pos + lax.broadcasted_iota(jnp.int32, (row_count, 1), 0)
    divisor = jnp.minimum(position + 1, window_len).astype(jnp.float32)
    return running / divisor - extended[REACH:]


def plain_body(inputs, norm_gain, in_weight, pool_scale, out_weight):
    rows, feats = inputs.shape
    layers, features = norm_gain.shape
    pools = pool_scale.shape[1]
    part = pools // lax.axis_size("tp")
    t = lax.axis_index("tp")
    s = lax.axis_index("sp")
    current = inputs
    for layer in range(layers):
        in_all = lax.all_gather(in_weight[layer], "sp", axis=1, tiled=True)
        out_all = lax.all_gather(out_weight[layer], "sp", axis=0, tiled=True)
        wide = current.astype(jnp.float32)
        squares = lax.psum(jnp.sum(wide * wide, axis=1), "tp")
        inv_rms = lax.rsqrt(squares / features + EPS)[:, None]
        gain = lax.dynamic_slice_in_dim(norm_gain[layer], t * feats, feats)
        normed = (wide * inv_rms * gain).astype(jnp.bfloat16)
        partial = jnp.dot(normed, in_all, preferred_element_type=jnp.float32)
        pool_in = lax.psum_scatter(
            partial.astype(jnp.bfloat16), "tp", scatter_dimension=1, tiled=True
        )
        edge = shift_sp(pool_in[rows - REACH :])
        extended = jnp.concatenate([edge, pool_in], 0).astype(jnp.float32)
        means = window_means(extended, rows, t * part, s * rows, pools)
        scale = lax.dynamic_slice_in_dim(pool_scale[layer], t * part, part)
        mixed = (means * scale).astype(jnp.bfloat16)
        pooled = lax.all_gather(mixed, "tp", axis=1, tiled=True)
        branch = jnp.dot(pooled, out_all, preferred_element_type=jnp.float32)
        current = (current.astype(jnp.float32) + branch).astype(jnp.bfloat16)
    return current


E, O, M, F, EM, OM1, OM2, FM = range(8)
PIECES = (2, 2, 2, 4, 2, 4)
EDGE_BY_MATE = (True, False, False, False, False, False)
OVER_BY_MATE = (0.5, 0.5, 0.5, 0.5, 0.5, 0)
INNER_ORDER = [
    ("im", 0), ("iy", 0), ("edge",), ("im", 1), ("im", 2), ("init",), ("iy", 1), ("iy", 2), ("ic", 0), ("ic", 1),
    ("ic", 2), ("O", 0), ("M", 0), ("E", 0), ("O", 1), ("E", 1), ("sq", 0), ("M", 1), ("O", 2), ("E", 2),
    ("plane", 0, 0), ("P", 0, 0, 0), ("inv", 0, 0), ("M", 2), ("OM", 0), ("E", 3), ("F", 0), ("EM", 0),
    ("Q", 0, 0, 0), ("sqa",), ("F", 1), ("OM", 1), ("EM", 1), ("plane", 0, 2), ("P", 0, 0, 2), ("iy", 3), ("iy", 4),
    ("iy", 5), ("plane", 0, 1), ("P", 0, 0, 1), ("F", 2), ("st", 0), ("OM", 2), ("im", 3), ("FM", 0), ("im", 4),
    ("im", 5), ("im", 6), ("im", 7), ("im", 8), ("im", 9), ("F", 3), ("Q", 0, 0, 2), ("FM", 1), ("st", 1), ("PA", 0),
    ("plane", 0, 3), ("PA", 3), ("O", 3), ("PA", 1), ("M", 3), ("P", 0, 0, 3), ("Q", 0, 0, 1), ("PA", 2), ("O", 4),
    ("M", 4), ("im", 10), ("im", 11), ("st", 2), ("O", 5), ("M", 5), ("O", 6), ("ic", 3), ("ic", 4), ("ic", 5),
    ("ic", 6), ("O", 7), ("ic", 7), ("ic", 8), ("ic", 9), ("FM", 2), ("O", 8), ("plane", 2, 0), ("st", 3), ("sq", 1),
    ("PB", 3), ("O", 9), ("Q", 0, 0, 3), ("PB", 2), ("PB", 0), ("FM", 3), ("PB", 1), ("EM", 2), ("inv", 0, 1),
    ("OM", 3), ("Q", 0, 1, 3), ("iy", 6), ("iy", 7), ("iy", 8), ("iy", 9), ("iy", 10), ("OM", 4), ("EM", 3),
    ("Q", 0, 1, 2), ("O", 10), ("all", 1), ("X", 0, 0, 0, 1), ("Q", 0, 1, 0), ("X", 0, 0, 1, 2), ("E", 4),
    ("X", 0, 0, 2, 4), ("O", 11), ("P", 1, 0, 0), ("M", 6), ("OM", 5), ("ic", 10), ("ic", 11), ("ic", 12),
    ("Q", 0, 1, 1), ("E", 5), ("mx", 0), ("X", 0, 1, 0, 1), ("M", 7), ("X", 0, 1, 1, 2), ("im", 12), ("im", 13),
    ("im", 14), ("plane", 2, 2), ("P", 1, 0, 2), ("F", 4), ("M", 8), ("inv", 1, 0), ("X", 0, 1, 2, 3), ("EM", 4),
    ("OM", 6), ("X", 0, 1, 3, 4), ("M", 9), ("P", 1, 1, 2), ("Q", 1, 0, 0), ("P", 1, 1, 0), ("EM", 5), ("F", 5),
    ("iy", 11), ("M", 10), ("OM", 7), ("E", 6), ("plane", 2, 1), ("P", 1, 1, 1), ("O", 12), ("Q", 1, 0, 2),
    ("inv", 1, 1), ("P", 1, 0, 1), ("E", 7), ("O", 13), ("E", 8), ("O", 14), ("E", 9), ("Q", 1, 1, 2), ("OM", 8),
    ("FM", 4), ("OM", 9), ("OM", 10), ("E", 10), ("Q", 1, 1, 0), ("FM", 5), ("F", 6), ("plane", 2, 3),
    ("P", 1, 1, 3), ("F", 7), ("E", 11), ("P", 1, 0, 3), ("M", 11), ("Q", 1, 1, 1), ("F", 8), ("EM", 6), ("FM", 6),
    ("plane", 4, 0), ("F", 9), ("ic", 13), ("ic", 14), ("ic", 15), ("EM", 7), ("FM", 7), ("im", 15), ("Q", 1, 0, 1),
    ("EM", 8), ("FM", 8), ("F", 10), ("EM", 9), ("FM", 9), ("Q", 1, 1, 3), ("mx", 1), ("all", 3), ("X", 1, 1, 0, 1),
    ("F", 11), ("X", 1, 1, 1, 2), ("EM", 10), ("X", 1, 1, 2, 3), ("OM", 11), ("X", 1, 1, 3, 4), ("FM", 10),
    ("Q", 1, 0, 3), ("X", 1, 0, 0, 1), ("EM", 11), ("O", 15), ("plane", 4, 2), ("P", 2, 1, 0), ("P", 2, 1, 2),
    ("E", 12), ("plane", 4, 1), ("FM", 11), ("inv", 2, 1), ("P", 2, 1, 1), ("X", 1, 0, 1, 2), ("E", 13),
    ("plane", 4, 3), ("P", 2, 1, 3), ("X", 1, 0, 2, 3), ("EM", 12), ("X", 1, 0, 3, 4), ("F", 12), ("P", 2, 0, 2),
    ("E", 14), ("P", 2, 0, 3), ("F", 13), ("EM", 13), ("P", 2, 0, 1), ("H", 0), ("P", 2, 0, 0), ("EM", 14),
    ("FM", 12), ("iy", 12), ("iy", 13), ("iy", 14), ("iy", 15), ("inv", 2, 0), ("H", 1), ("F", 14), ("E", 15),
    ("FM", 13), ("EM", 15), ("M", 12), ("Q", 2, 0, 2), ("F", 15), ("M", 13), ("M", 14), ("Q", 2, 0, 3), ("OM", 12),
    ("M", 15), ("OM", 13), ("bplane", 12), ("FM", 14), ("bplane", 13), ("OM", 14), ("Q", 2, 0, 1), ("FM", 15),
    ("bplane", 14), ("OM", 15), ("bplane", 15), ("Q", 2, 0, 0), ("X", 2, 0, 0, 4),
]
END_ORDER = [
    ("edge", 0), ("ey", 0), ("ey", 1), ("ey", 2), ("ey", 3), ("eown", 0), ("eown", 1), ("eown", 2), ("eown", 3),
    ("eM", 1), ("eM", 0), ("edge", 1), ("ey", 4), ("ey", 5), ("st", 0), ("st", 1), ("st", 2), ("st", 3), ("eM", 2),
    ("eI", 2), ("eM", 3), ("eown", 4), ("eown", 5), ("eM", 4), ("eM", 5), ("eO", 2), ("eIM", 2), ("eOM", 2),
    ("eF", 2), ("ey", 6), ("eown", 6), ("eF", 3), ("eFM", 2), ("ey", 7), ("ey", 8), ("eown", 7), ("ey", 9),
    ("ey", 10), ("ey", 11), ("eown", 8), ("eown", 9), ("eown", 10), ("eown", 11), ("eM", 6), ("eO", 3), ("eFM", 3),
    ("eM", 7), ("eO", 6), ("eM", 8), ("eM", 9), ("eI", 3), ("ey", 12), ("ey", 13), ("ey", 14), ("ey", 15), ("eI", 6),
    ("eM", 10), ("eO", 7), ("eI", 7), ("eM", 11), ("eI", 8), ("eI", 9), ("eOM", 3), ("eO", 8), ("eOM", 6), ("eO", 9),
    ("eIM", 3), ("eI", 12), ("eown", 12), ("eown", 13), ("eM", 12), ("eown", 14), ("eM", 13), ("emx", 0, 0),
    ("eM", 14), ("eown", 15), ("eM", 15), ("emx", 0, 1), ("eIM", 6), ("emy", 0, 0), ("eO", 12), ("eOM", 7),
    ("eO", 13), ("eIM", 7), ("emy", 0, 1), ("eall", 1), ("eX", 0, 0, 2), ("eIM", 8), ("eO", 14), ("eX", 0, 2, 4),
    ("eIM", 9), ("eOM", 8), ("eF", 6), ("eOM", 9), ("eIM", 12), ("eF", 7), ("eOM", 12), ("eF", 8), ("eOM", 13),
    ("eF", 9), ("eOM", 14), ("eI", 13), ("eFM", 6), ("eI", 14), ("eFM", 7), ("eI", 15), ("eFM", 8), ("eFM", 9),
    ("emx", 1, 0), ("eIM", 13), ("eIM", 14), ("emx", 1, 1), ("eIM", 15), ("eO", 15), ("emy", 1, 0), ("eF", 12),
    ("emy", 1, 1), ("eall", 3), ("eX", 1, 0, 1), ("eOM", 15), ("eX", 1, 1, 2), ("eF", 13), ("eX", 1, 2, 4),
    ("eFM", 12), ("emx", 2, 0), ("epl", 12), ("eFM", 13), ("epl", 13), ("emx", 2, 1), ("eF", 14), ("emy", 2, 0),
    ("eF", 15), ("emy", 2, 1), ("eX", 2, 0, 1), ("eFM", 14), ("eX", 2, 1, 2), ("eFM", 15), ("epl", 14),
    ("eX", 2, 2, 3), ("epl", 15), ("eX", 2, 3, 4),
]


def phase_table(feats):
    table = []
    for buf, count in enumerate(PIECES):
        width = feats // count
        table += [(buf, k * width, width) for k in range(count)]
    return table


def kernel(
    n_z, layers, halo,
    x_hbm, gain_ref, wi_hbm, scale_ref, wo_hbm, o_hbm,
    x_ref, wi_ref, wo_ref, o_ref, held, state, xg, edge, p_send, p_recv, mix, mix_in, part_sq, inv_col, sq_send, sq_recv,
    w_send, w_recv, c_recv, local_sem, load_sem, out_sem, e_send, e_recv, s_send, s_recv, a_send, a_recv, early_recv, m_send, m_recv,
):
    loads = [
        pltpu.make_async_copy(src, dst, load_sem.at[i])
        for i, (src, dst) in enumerate([(wi_hbm, wi_ref), (x_hbm, x_ref), (wo_hbm, wo_ref)])
    ]
    for load in loads:
        load.start()
    rows, feats = x_ref.shape
    total = rows + halo
    blocks, depth = held.shape[1], held.shape[2]
    pools = scale_ref.shape[1]
    chunk = pools // n_z
    last = layers - 1
    table = phase_table(feats)
    phases = len(table)
    lanes = 128
    quarter = feats // 4
    state_chunks = s_recv.shape[0]
    last_buf = len(PIECES) - 1
    sq_tiles = part_sq.shape[1] // lanes
    s = lax.axis_index("sp")
    t = lax.axis_index("tp")
    core = s % 2
    y = (s // 2) % 2
    z = s // 4
    side = z // 2

    def block_of(zz, yy, cc):
        return zz * 4 + yy * 2 + cc

    z_in, z_end = 1 + side, 3 * side
    z_over, z_far = 2 - side, 3 - 3 * side
    is_end = z == z_end
    s_end, s_in = block_of(z_end, y, core), block_of(z_in, y, core)

    y_mate = (block_of(z, 1 - y, core), t)
    c_mate = (block_of(z, y, 1 - core), t)
    x_mate = (s, 1 - t)
    opposite = (block_of(z_over, y, core), t)
    inner = (s_in, t)
    outer = (s_end, t)
    after = (s + 1) % blocks
    after_z = after // 4
    after_holder = (block_of(1 + after_z // 2, (after // 2) % 2, after % 2), t)
    after_slot = jnp.where((after_z == 0) | (after_z == n_z - 1), 1, 0)
    before = [((s_in + blocks - 1) % blocks, t), ((s_end + blocks - 1) % blocks, t)]

    barrier = pltpu.get_barrier_semaphore()

    def greet(peers):
        for peer in peers:
            pl.semaphore_signal(barrier, inc=1, device_id=peer, device_id_type=MESH_ID)

    def send(src, dst, send_sem, recv_sem, to, when=None):
        copy = pltpu.make_async_remote_copy(
            src_ref=src, dst_ref=dst, send_sem=send_sem, recv_sem=recv_sem,
            device_id=to, device_id_type=MESH_ID,
        )
        if when is None:
            copy.start()
        else:
            pl.when(when)(copy.start)

    def departed(ref, sem):
        pltpu.make_async_remote_copy(
            src_ref=ref, dst_ref=ref, send_sem=sem, recv_sem=sem,
            device_id=c_mate, device_id_type=MESH_ID,
        ).wait_send()

    def arrived(ref, sem):
        pltpu.make_async_remote_copy(
            src_ref=ref, dst_ref=ref, send_sem=sem, recv_sem=sem,
            device_id=c_mate, device_id_type=MESH_ID,
        ).wait_recv()

    whole, first, second = pl.ds(0, depth), pl.ds(0, depth // 2), pl.ds(depth // 2, depth // 2)
    volume = {}

    def put_out(cols):
        pltpu.make_async_copy(o_ref.at[:, cols], o_hbm.at[:, cols], out_sem.at[0]).start()

    def wait_out():
        pltpu.make_async_copy(o_ref, o_hbm, out_sem.at[0]).wait()

    def own(ph):
        buf, start, width = table[ph]
        return (wi_ref if buf % 2 == 0 else wo_ref).at[buf // 2, :, pl.ds(start, width)]

    def slot(ph, block, piece=whole):
        buf, start, width = table[ph]
        return held.at[buf, block, piece, pl.ds(start, width)]

    def send_sem(ph, port, piece):
        buf, _, width = table[ph]
        kind = 1 if port == EM else 0
        share = width * (1 if piece is whole else 0.5) / feats
        volume[buf, kind] = volume.get((buf, kind), 0) + share
        return w_send.at[buf, kind]

    def core_sem(ph, block):
        buf, start, width = table[ph]
        layer = buf // 2
        if buf % 2 == 0:
            return c_recv.at[layer * n_z + block // 4]
        return c_recv.at[layers * n_z + layer + (start // width if buf == last_buf else 0)]

    def send_own(ph, to, port):
        sem = core_sem(ph, s) if port is None else w_recv.at[ph, port]
        send(own(ph), slot(ph, s), send_sem(ph, port, whole), sem, to)

    def forward(ph, block, to, port, piece=whole):
        ref = slot(ph, block, piece)
        sem = core_sem(ph, block) if port is None else w_recv.at[ph, port]
        send(ref, ref, send_sem(ph, port, piece), sem, to)

    def wait_block(ph, block, port, piece=whole):
        arrived(slot(ph, block, piece), w_recv.at[ph, port])

    def drain_weights():
        for (buf, kind), blocks_sent in volume.items():
            assert blocks_sent == int(blocks_sent)
            departed(held.at[buf, pl.ds(0, int(blocks_sent))], w_send.at[buf, kind])
        volume.clear()

    state_rows = rows // state_chunks
    split_row = halo + rows // 2
    def parts_of(buf):
        return [ph for ph in range(phases) if table[ph][0] == buf]

    def is_out(ph):
        return table[ph][0] % 2 == 1

    def local_of(ph):
        buf, start, width = table[ph]
        return local_sem.at[buf + (start // width if buf == last_buf else 0)]

    def keep_own(ph):
        pltpu.make_async_copy(own(ph), slot(ph, s), local_of(ph)).start()

    def gathered(buf):
        ph = parts_of(buf)[0]
        weight = (wi_ref if buf % 2 == 0 else wo_ref).at[buf // 2]
        pltpu.make_async_copy(weight, held.at[buf, s], local_of(ph)).wait()
        arrived(held.at[buf, pl.ds(0, blocks // 2)], core_sem(ph, s))

    def gathered_piece(ph):
        buf, start, width = table[ph]
        pltpu.make_async_copy(own(ph), slot(ph, s), local_of(ph)).wait()
        arrived(held.at[buf, pl.ds(0, blocks // 2), :, pl.ds(start, width)], core_sem(ph, s))

    def half_plane(which, j):
        near = jnp.where(side == 0, z_in - j, z_in + j)
        far = jnp.where(side == 0, z_over + j, z_over - j)
        return jnp.where(which == side, near, far)

    def send_edge(when=None):
        send(
            x_ref.at[pl.ds(rows - halo, halo)], edge.at[after_slot],
            e_send.at[0], e_recv.at[after_slot], after_holder, when,
        )

    def send_some_edges(which):
        send_edge(after_slot == which)

    def run(table_of_steps, order):
        for name, *args in order:
            with jax.named_scope("_".join([name] + [str(a) for a in args])):
                table_of_steps[name](*args)

    def end_program():
        greet([inner, y_mate, c_mate, x_mate])
        pl.semaphore_wait(barrier, 5)
        for load in loads:
            load.wait()
        mate = block_of(z_end, 1 - y, core)
        columns = [z_in, z_over, z_far]

        def own_aside(ph):
            if is_out(ph) or not EDGE_BY_MATE[table[ph][0]]:
                send_own(ph, y_mate, M)
            if is_out(ph):
                send_own(ph, c_mate, None)
                keep_own(ph)

        def own_inward(ph):
            send_own(ph, inner, E)

        def mate_inward(ph):
            direct = not EDGE_BY_MATE[table[ph][0]]
            if is_out(ph) or direct:
                wait_block(ph, mate, M)
            if direct:
                forward(ph, mate, inner, EM)
            if is_out(ph):
                forward(ph, mate, c_mate, None)

        def ship_state(k):
            at = pl.ds(k * state_rows, state_rows)
            send(
                x_ref.at[at], state.at[1, pl.ds(halo + k * state_rows, state_rows)],
                s_send.at[0], s_recv.at[k], inner,
            )

        def take_column(which, ph):
            block = block_of(columns[which], y, core)
            wait_block(ph, block, (E, O, F)[which])
            forward(ph, block, y_mate, (EM, OM1, FM)[which])
            forward(ph, block, c_mate, None)

        def take_mate_column(which, ph):
            block = block_of(columns[which], 1 - y, core)
            wait_block(ph, block, (EM, OM1, FM)[which])
            forward(ph, block, c_mate, None)

        def take_mix(layer, j):
            zz = half_plane(t, j)
            ref, sem = mix_in.at[layer, zz], m_recv.at[layer, zz]
            arrived(ref, sem)
            send(ref, ref, m_send.at[layer], sem, x_mate)

        def take_mate_mix(layer, j):
            zz = half_plane(1 - t, j)
            arrived(mix_in.at[layer, zz], m_recv.at[layer, zz])

        def end_expand(layer, begin, end):
            width = 512
            at = pl.ds(halo, rows)

            @pl.loop(begin * quarter // width, end * quarter // width)
            def _(n):
                cols = pl.ds(pl.multiple_of(n * width, width), width)
                mixed = jnp.concatenate([mix_in[layer, c] for c in range(n_z)], axis=1)
                weight = held[2 * layer + 1, :, :, cols].reshape(pools, width)
                branch = jnp.dot(mixed, weight, preferred_element_type=jnp.float32)
                old = x_ref[:, cols] if layer == 0 else state[1, at, cols]
                new = (old.astype(jnp.float32) + branch).astype(jnp.bfloat16)
                if layer == last:
                    o_ref[:, cols] = new
                    put_out(cols)
                else:
                    state[1, at, cols] = new

        part = functools.partial
        run({
            "ey": own_aside, "eown": own_inward, "eM": mate_inward, "st": ship_state,
            "eI": part(take_column, 0), "eO": part(take_column, 1), "eF": part(take_column, 2),
            "eIM": part(take_mate_column, 0), "eOM": part(take_mate_column, 1),
            "eFM": part(take_mate_column, 2), "eall": gathered, "epl": gathered_piece,
            "edge": send_some_edges,
            "emx": take_mix, "emy": take_mate_mix, "eX": end_expand,
        }, END_ORDER)
        with jax.named_scope("drain"):
            drain_weights()
            wait_out()
            departed(x_ref, s_send.at[0])
            departed(x_ref.at[pl.ds(0, halo)], e_send.at[0])
            for layer in range(layers):
                departed(mix_in.at[layer, pl.ds(2 * t, 2)], m_send.at[layer])

    def inner_program():
        with jax.named_scope("greet"):
            greet([opposite, y_mate, c_mate, x_mate, outer] + before)
        with jax.named_scope("barrier"):
            pl.semaphore_wait(barrier, 6)
        for load in loads:
            load.wait()
        chunk_z = [z_in, z_end, z_over, z_far]

        def own_across(ph):
            send_own(ph, opposite, O)

        def own_to_mate(ph):
            send_own(ph, y_mate, M)

        def own_near(ph):
            send_own(ph, c_mate, None)
            if is_out(ph):
                send_own(ph, outer, E)
            keep_own(ph)

        def over_pieces(ph):
            share = OVER_BY_MATE[table[ph][0]]
            by_mate = None if share == 0 else whole if share == 1 else first
            direct = None if share == 1 else whole if share == 0 else second
            return by_mate, direct

        def take_end(ph):
            block = block_of(z_end, y, core)
            wait_block(ph, block, E)
            forward(ph, block, opposite, F)
            if EDGE_BY_MATE[table[ph][0]]:
                forward(ph, block, y_mate, EM)
            forward(ph, block, c_mate, None)

        def take_over(ph):
            block = block_of(z_over, y, core)
            wait_block(ph, block, O)
            by_mate, _ = over_pieces(ph)
            if by_mate is not None:
                forward(ph, block, y_mate, OM1, by_mate)
            forward(ph, block, c_mate, None)
            if is_out(ph):
                forward(ph, block, outer, O)

        def take_mate(ph):
            block = block_of(z_in, 1 - y, core)
            wait_block(ph, block, M)
            _, direct = over_pieces(ph)
            if direct is not None:
                forward(ph, block, opposite, OM2, direct)
            forward(ph, block, c_mate, None)

        def take_far(ph):
            block = block_of(z_far, y, core)
            wait_block(ph, block, F)
            forward(ph, block, y_mate, FM)
            forward(ph, block, c_mate, None)
            if is_out(ph):
                forward(ph, block, outer, F)

        def take_mate_end(ph):
            block = block_of(z_end, 1 - y, core)
            wait_block(ph, block, EM)
            forward(ph, block, c_mate, None)

        def take_mate_over(ph):
            block = block_of(z_over, 1 - y, core)
            by_mate, direct = over_pieces(ph)
            if by_mate is not None:
                wait_block(ph, block, OM1, by_mate)
            if direct is not None:
                wait_block(ph, block, OM2, direct)
            forward(ph, block, c_mate, None)

        def take_mate_far(ph):
            block = block_of(z_far, 1 - y, core)
            wait_block(ph, block, FM)
            forward(ph, block, c_mate, None)

        def plane(buf, k):
            if k == 0:
                weight = wi_ref.at[buf // 2]
                pltpu.make_async_copy(weight, held.at[buf, s], local_of(parts_of(buf)[0])).wait()
            block = block_of(chunk_z[k], 0, 0)
            arrived(held.at[buf, pl.ds(block, 2)], core_sem(parts_of(buf)[0], block))

        def first_row(layer):
            return REACH * layer

        def from_row(start):
            return pl.ds(start, total - start)

        def gain_of(layer, start, width):
            at = pl.multiple_of(t * feats + start, lanes)
            return gain_ref[pl.ds(layer, 1), pl.ds(at, width)]

        def pack_squares(g, layer):
            for k in range(sq_tiles):
                block = part_sq[g, pl.ds(k * lanes, lanes)].T
                value = jnp.sum(block, axis=0, keepdims=True)
                sq_send[layer, g, k] = jnp.broadcast_to(value, (8, lanes))
            send(
                sq_send.at[layer, g], sq_recv.at[layer, g],
                a_send.at[layer, g, 1], a_recv.at[layer, g, n_z], x_mate,
            )

        def halved(layer, g):
            return layer == last and g == 1

        def mix_slot(layer, g):
            return 0 if g == 0 else 1 + layer

        def take_edge(g):
            arrived(edge.at[g], e_recv.at[g])
            keep = ((s_in if g == 0 else s_end) > 0).astype(jnp.float32)

            @pl.loop(0, halo // REACH)
            def _(i):
                at = pl.ds(i * REACH, REACH)
                state[g, at] = (edge[g, at].astype(jnp.float32) * keep).astype(jnp.bfloat16)

        def own_state():
            @pl.loop(0, rows // REACH)
            def _(i):
                state[0, pl.ds(halo + i * REACH, REACH)] = x_ref[pl.ds(i * REACH, REACH)]

        def take_state(k):
            arrived(state.at[1, pl.ds(halo + k * state_rows, state_rows)], s_recv.at[k])

        def squares(g, start, stop):
            @pl.loop(start // REACH, stop // REACH)
            def _(i):
                at = pl.ds(i * REACH, REACH)
                sums = jnp.zeros((REACH, lanes), jnp.float32)
                for j in range(feats // lanes):
                    cols = pl.ds(j * lanes, lanes)
                    wide = state[g, at, cols].astype(jnp.float32)
                    sums = sums + wide * wide
                    xg[g, at, cols] = (wide * gain_of(0, j * lanes, lanes)).astype(jnp.bfloat16)
                part_sq[g, at] = sums

        def project(layer, g, k):
            project_rows(layer, g, k, first_row(layer), total, a_recv.at[layer, g, chunk_z[k]])

        def project_early(k):
            project_rows(0, 1, k, 0, split_row, early_recv.at[chunk_z[k]])

        def project_late(k):
            project_rows(0, 1, k, split_row, total, a_recv.at[0, 1, chunk_z[k]])

        def project_rows(layer, g, k, start, stop, sem):
            at = pl.ds(start, stop - start)
            zz = chunk_z[k]
            weight = held[2 * layer, pl.ds(zz * 4, 4)].reshape(chunk, feats)
            value = lax.dot_general(
                xg[g, at], weight, (((1,), (1,)), ((), ())),
                preferred_element_type=jnp.float32,
            )
            p_send[layer, g, zz, at] = value.astype(jnp.bfloat16)
            send(
                p_send.at[layer, g, zz, at], p_recv.at[layer, g, zz, at],
                a_send.at[layer, g, 0], sem, x_mate,
                (zz // 2 != t) if halved(layer, g) else None,
            )

        def inverse(layer, g):
            arrived(sq_recv.at[layer, g], a_recv.at[layer, g, n_z])
            for k in range(sq_tiles):
                mean = (sq_send[layer, g, k] + sq_recv[layer, g, k]) / (2 * feats)
                inv = lax.rsqrt(mean + EPS)
                inv_col[g, pl.ds(k * lanes, lanes)] = jnp.broadcast_to(inv[0:1], (lanes, lanes)).T

        def pool(layer, g, k):
            pool_plane(layer, g, chunk_z[k])

        def pool_half(j):
            pool_plane(last, 1, half_plane(t, j))
            ship_mix(last, j)

        def ship_mix(layer, j):
            zz = half_plane(t, j)
            send(
                mix.at[mix_slot(layer, 1), zz, pl.ds(halo, rows)], mix_in.at[layer, zz],
                m_send.at[layer], m_recv.at[layer, zz], outer,
            )

        def ship_mixes(layer):
            for j in range(2):
                ship_mix(layer, j)

        def pool_plane(layer, g, group):
            start = first_row(layer)
            at = from_row(start)
            if layer == 0 and g == 1:
                early, late = pl.ds(0, split_row), pl.ds(split_row, total - split_row)
                arrived(p_recv.at[layer, g, group, early], early_recv.at[group])
                arrived(p_recv.at[layer, g, group, late], a_recv.at[layer, g, group])
            else:
                arrived(p_recv.at[layer, g, group, at], a_recv.at[layer, g, group])
            row = lax.broadcasted_iota(jnp.int32, (total - start, lanes), 0)
            position = (s_in if g == 0 else s_end) * rows - halo + start + row
            span = jnp.left_shift(jnp.int32(2), group)
            divisor = jnp.maximum(jnp.minimum(position + 1, span), 1).astype(jnp.float32)
            share = 1.0 / divisor
            inv = inv_col[g, at]
            for j in range(chunk // lanes):
                cols = pl.ds(j * lanes, lanes)
                joined = p_send[layer, g, group, at, cols].astype(jnp.float32)
                joined = joined + p_recv[layer, g, group, at, cols].astype(jnp.float32)
                base = (joined * inv).astype(jnp.bfloat16).astype(jnp.float32)
                running = base
                width = 1
                picked = None
                for step in range(GROUPS):
                    running = running + pltpu.roll(running, width, 0)
                    width *= 2
                    picked = running if picked is None else jnp.where(group >= step, running, picked)
                lane = pl.multiple_of(group * chunk + j * lanes, lanes)
                scale = scale_ref[pl.ds(layer, 1), pl.ds(lane, lanes)]
                mix[mix_slot(layer, g), group, at, cols] = ((picked * share - base) * scale).astype(jnp.bfloat16)

        def expand(layer, g, begin, end):
            width = 512
            at = from_row(first_row(layer + 1))
            buf = 2 * layer + 1
            if layer < last and begin == 0:
                part_sq[g] = jnp.zeros(part_sq.shape[1:], jnp.float32)

            @pl.loop(begin * quarter // width, end * quarter // width)
            def _(n):
                col = pl.multiple_of(n * width, width)
                cols = pl.ds(col, width)
                mixed = jnp.concatenate([mix[mix_slot(layer, g), c, at] for c in range(n_z)], axis=1)
                weight = held[buf, :, :, cols].reshape(pools, width)
                branch = jnp.dot(mixed, weight, preferred_element_type=jnp.float32)
                new = (state[g, at, cols].astype(jnp.float32) + branch).astype(jnp.bfloat16)
                if layer == last:
                    o_ref[:, cols] = new
                    put_out(cols)
                else:
                    state[g, at, cols] = new
                    wide = new.astype(jnp.float32)
                    xg[g, at, cols] = (wide * gain_of(layer + 1, col, width)).astype(jnp.bfloat16)
                    square = wide * wide
                    sums = square[:, :lanes]
                    for j in range(1, width // lanes):
                        sums = sums + square[:, j * lanes:(j + 1) * lanes]
                    part_sq[g, at] = part_sq[g, at] + sums

            if layer < last and end == 4:
                pack_squares(g, layer + 1)

        def prepare():
            for g in range(2):
                part_sq[g] = jnp.zeros(part_sq.shape[1:], jnp.float32)
            own_state()

        def first_squares(g):
            if g == 0:
                take_edge(0)
                squares(0, 0, total)
            pack_squares(g, 0)

        def halo_squares():
            take_edge(1)
            squares(1, 0, halo)

        def shipped_squares(k):
            take_state(k)
            squares(1, halo + k * state_rows, halo + (k + 1) * state_rows)

        run({
            "im": own_across, "iy": own_to_mate, "ic": own_near, "E": take_end, "O": take_over, "M": take_mate, "F": take_far,
            "EM": take_mate_end, "OM": take_mate_over, "FM": take_mate_far,
            "plane": plane, "all": gathered, "bplane": gathered_piece, "edge": send_edge, "init": prepare, "sq": first_squares, "sqa": halo_squares,
            "st": shipped_squares, "P": project, "PA": project_early, "PB": project_late, "Q": pool, "inv": inverse, "H": pool_half,
            "mx": ship_mixes, "X": expand,
        }, INNER_ORDER)
        with jax.named_scope("drain"):
            drain_weights()
            wait_out()
            departed(x_ref.at[pl.ds(0, halo)], e_send.at[0])
            for layer in range(layers):
                departed(mix_in.at[layer, pl.ds(2 * t, 2)], m_send.at[layer])
                at = from_row(first_row(layer))
                for g in range(2):
                    departed(sq_send.at[layer, g], a_send.at[layer, g, 1])
                    zz = pl.ds(2 * (1 - t), 2) if halved(layer, g) else pl.ds(0, n_z)
                    departed(p_send.at[layer, g, zz, at], a_send.at[layer, g, 0])

    pl.when(is_end)(end_program)
    pl.when(jnp.logical_not(is_end))(inner_program)


def fused_body(inputs, norm_gain, in_weight, pool_scale, out_weight):
    rows, feats = inputs.shape
    layers = norm_gain.shape[0]
    pools = pool_scale.shape[1]
    blocks = lax.axis_size("sp")
    n_z = blocks // 4
    depth = out_weight.shape[1]
    halo = REACH * layers
    total = rows + halo
    sq_tiles = -(-total // 128)
    chunk = pools // n_z
    phases = len(phase_table(feats))
    state_chunks = len([row for row in END_ORDER if row[0] == "st"])
    bf, f32 = jnp.bfloat16, jnp.float32
    vmem = pl.BlockSpec(memory_space=pltpu.VMEM)
    hbm = pl.BlockSpec(memory_space=pl.ANY)
    dma = pltpu.SemaphoreType.DMA
    return pl.pallas_call(
        functools.partial(kernel, n_z, layers, halo),
        out_shape=jax.ShapeDtypeStruct((rows, feats), bf),
        in_specs=[hbm, vmem, hbm, vmem, hbm],
        out_specs=hbm,
        scratch_shapes=[
            pltpu.VMEM((rows, feats), bf),
            pltpu.VMEM((layers, depth, feats), bf),
            pltpu.VMEM((layers, depth, feats), bf),
            pltpu.VMEM((rows, feats), bf),
            pltpu.VMEM((2 * layers, blocks, depth, feats), bf),
            pltpu.VMEM((2, total, feats), bf),
            pltpu.VMEM((2, total, feats), bf),
            pltpu.VMEM((2, halo, feats), bf),
            pltpu.VMEM((layers, 2, n_z, total, chunk), bf),
            pltpu.VMEM((layers, 2, n_z, total, chunk), bf),
            pltpu.VMEM((1 + layers, n_z, total, chunk), bf),
            pltpu.VMEM((layers, n_z, rows, chunk), bf),
            pltpu.VMEM((2, sq_tiles * 128, 128), f32),
            pltpu.VMEM((2, sq_tiles * 128, 128), f32),
            pltpu.VMEM((layers, 2, sq_tiles, 8, 128), f32),
            pltpu.VMEM((layers, 2, sq_tiles, 8, 128), f32),
            dma((2 * layers, 2)),
            dma((phases, 8)),
            dma((layers * n_z + layers - 1 + PIECES[-1],)),
            dma((2 * layers - 1 + PIECES[-1],)),
            dma((3,)),
            dma((1,)),
            dma((1,)),
            dma((2,)),
            dma((1,)),
            dma((state_chunks,)),
            dma((layers, 2, 2)),
            dma((layers, 2, n_z + 1)),
            dma((n_z,)),
            dma((layers,)),
            dma((layers, n_z)),
        ],
        compiler_params=pltpu.CompilerParams(
            collective_id=0, has_side_effects=True, vmem_limit_bytes=60 * 1024 * 1024
        ),
    )(inputs, norm_gain, jnp.swapaxes(in_weight, 1, 2), pool_scale, out_weight)


def solution(mesh):
    n_sp, n_tp = mesh.shape["sp"], mesh.shape["tp"]
    fused = n_tp == 2 and n_sp == 16
    placed = (P("sp", "tp"), P(), P(None, "tp", "sp"), P(), P(None, "sp", "tp"))
    return jax.shard_map(
        fused_body if fused else plain_body,
        mesh=mesh, in_specs=placed, out_specs=P("sp", "tp"), check_vma=False,
    )
```
